32 devices in a mesh: sp: 8 (over z, x), dp: 4 (over y, core).
Axes of the slice: x: 2, y: 2, z: 4, core: 2. Of those that a mesh axis runs over, the one named last changes fastest.
Arguments:
- queries: bfloat16 [4, 1024, 16, 128], P('dp', 'sp'), may hold values from -6 to 6
- key_rows: bfloat16 [4, 1024, 4, 128], P('dp', 'sp'), may hold values from -6 to 6
- values: bfloat16 [4, 1024, 4, 128], P('dp', 'sp'), may hold values from -6 to 6
- query_gain: float32 [128], replicated, may hold values from 0.4 to 5
- key_gain: float32 [128], replicated, may hold values from 0.4 to 5
- out_weight: bfloat16 [2048, 2048], P('sp', 'dp'), may hold values from -0.125 to 0.125
- residual: bfloat16 [4, 1024, 2048], P('dp', 'sp'), may hold values from -6 to 6
- norm_gain: float32 [2048], replicated, may hold values from 0.1 to 1.9
- expert_gate: bfloat16 [8, 2048, 1792], P('sp'), may hold values from -0.125 to 0.125
- expert_up: bfloat16 [8, 2048, 1792], P('sp'), may hold values from -0.125 to 0.125
- expert_down: bfloat16 [8, 1792, 2048], P('sp'), may hold values from -0.125 to 0.125
- routes: int32 [4, 1024, 2], P('dp', 'sp'), may hold values from 0 to 7, all different within a row; in each aligned block of 64 rows (0 to 63, 64 to 127, ..., all dimensions but the last counted through in order) at most 32 rows name the same one
- route_weight: float32 [4, 1024, 2], P('dp', 'sp'), may hold values from 0.25 to 1
Outputs:
- layer_out: bfloat16 [4, 1024, 2048], P('dp', 'sp')
The draws below stay inside these ranges and needn't reach their ends.
Inputs may be any that keep to these rules, and one draw needn't show every extreme that they name: `routes`: in each aligned block of 64 rows of one device, no expert is named by more than 32 entries, a bound that some block reaches; the two experts of a row differ.
All inputs are finite; a program needn't handle non-finite values.
Results may differ from the reference program's by a relative error of at most 0.0095.
The reference program's roundings to bfloat16 on the way count: a program that leaves them out, or rounds other values in their place, can miss the bound.
Values may be sent and summed in bfloat16 or wider, within the bound.
A program may use at most 128 MiB of HBM per device.

```python
import math
import jax
import jax.numpy as jnp
import numpy as np
from jax import lax

D = 2048
HEADS = 16
KV_HEADS = 4
HEAD_DIM = 128
EXPERT_FF = 1792
GRID_W = 64
SEQS = 4
LENGTH = 1024
EXPERTS = 8
HALF = 64
CAP = 32


def shared_keys(key):
    drawn = jax.random.normal(jax.random.fold_in(key, 11), (SEQS, LENGTH, KV_HEADS, HEAD_DIM), jnp.float32)
    return jnp.clip(drawn, -6.0, 6.0)


def draw_key_rows(key, part):
    return shared_keys(key).astype(jnp.bfloat16)


def draw_queries(key, part):
    drawn = jax.random.normal(jax.random.fold_in(key, 12), (SEQS, LENGTH, HEADS, HEAD_DIM), jnp.float32)
    drawn = jnp.clip(drawn, -6.0, 6.0)
    return drawn.astype(jnp.bfloat16)


def gain_draw(key, salt):
    drawn = jax.random.normal(jax.random.fold_in(key, salt), (HEAD_DIM,), jnp.float32)
    return 1.0 + 0.18 * jnp.clip(drawn, -3.0, 3.0)


def draw_query_gain(key, part):
    return gain_draw(key, 21)


def draw_key_gain(key, part):
    return gain_draw(key, 22)


def block_levels(stream_key, extent, pieces, low, top_value):
    def one(dim, parts):
        heights = jax.random.uniform(jax.random.fold_in(jax.random.fold_in(stream_key, 6), dim), (parts,), jnp.float32, low / len(pieces), top_value / len(pieces))
        return jnp.repeat(jnp.exp(heights), extent[dim] // parts).reshape((-1,) + (1,) * (len(extent) - dim - 1))

    level = one(*pieces[0])
    for cut in pieces[1:]:
        level = level * one(*cut)
    return level


def shared_out(rng, own, number, rows, number_of, top, reach, skew):
    sequence = jax.random.permutation(rng, number_of)
    packed, ordinary = portions_of(number_of, rows * top, reach, skew, True), portions_of(number_of, rows * top, reach, skew, False)
    places = jnp.arange(number_of)

    def named(tallies, rotation):
        used = int((tallies > 0).sum())
        fixed = max(1, used // 4)
        passed = fixed + (places - fixed + rotation * (used - fixed)) % max(1, number_of - fixed)
        return jnp.zeros((number_of,), jnp.int32).at[sequence[jnp.where(places < fixed, places, passed)]].set(jnp.asarray(tallies, jnp.int32))

    tallies = jnp.where(number % 4 == 0, named(packed, number // 4), named(ordinary, number - number // 4 - 1))
    mixed = jax.random.permutation(jax.random.fold_in(own, 3), number_of)
    donor, sink = mixed[0:number_of // 2 * 2:2], mixed[1:number_of // 2 * 2:2]
    margin = jnp.minimum(tallies[donor] - 1, reach - tallies[sink]) // 2
    margin = jnp.where((donor == sequence[0]) | (sink == sequence[0]) | (tallies[sink] == 0), 0, jnp.maximum(margin, 0))
    passed = jax.random.randint(jax.random.fold_in(own, 4), (number_of // 2,), 0, 1 << 20) % (margin + 1)
    tallies = tallies.at[donor].add(-passed).at[sink].add(passed)
    items = jnp.searchsorted(jnp.cumsum(tallies), jnp.arange(rows * top), side="right").astype(jnp.int32)
    listing = items.reshape(top, rows).T
    listing = listing[jax.random.permutation(jax.random.fold_in(own, 1), rows)]
    rotation = jax.random.randint(jax.random.fold_in(own, 2), (rows, 1), 0, top)
    return jnp.take_along_axis(listing, (jnp.arange(top)[None, :] + rotation) % top, axis=1)


def portions_of(amount, total, most, slope, full):
    weights = [(1 << 20) // math.isqrt(grade ** slope) + 1 for grade in range(1, amount + 1)]
    largest = most if full else min(most, max(-(-total // amount), total * weights[0] // sum(weights)))
    least = 1 if total - largest >= amount - 1 else 0
    counts, spare = [largest] + [least] * (amount - 1), total - largest - least * (amount - 1)
    while spare > 0:
        movable = [i for i in range(1, amount) if counts[i] < largest] or [i for i in range(1, amount) if counts[i] < most]
        mass, budget = sum([weights[i] for i in movable]), spare
        for i in movable:
            addition = min(most - counts[i], max(1, budget * weights[i] // mass), spare)
            counts[i] = counts[i] + addition
            spare = spare - addition
    return np.array(counts)


def gaussian(own_key, dims, deviation, bound, pieces=(), kind=jnp.bfloat16):
    array = jax.random.normal(own_key, dims, jnp.float32) * deviation
    if len(pieces) > 0:
        array = block_levels(own_key, dims, pieces, -0.22, 0.18) * array
    return jnp.clip(array, min=-bound, max=bound).astype(kind)


def setup_inputs(seed: int = 0) -> dict:
    streams_of = jax.random.split(jax.random.key(seed), 14)
    queries = draw_queries(jax.random.fold_in(streams_of[13], 71), 0)
    key_rows = draw_key_rows(jax.random.fold_in(streams_of[13], 71), 0)
    values = gaussian(streams_of[2], (SEQS, LENGTH, KV_HEADS, HEAD_DIM), 1.0, 6.0, ((0, 4), (1, 8)))
    query_gain = draw_query_gain(jax.random.fold_in(streams_of[13], 71), 0)
    key_gain = draw_key_gain(jax.random.fold_in(streams_of[13], 71), 0)
    out_weight = gaussian(streams_of[5], (HEADS * HEAD_DIM, D), (HEADS * HEAD_DIM) ** -0.5, 0.125, ((0, 8), (1, 4)))
    residual = gaussian(streams_of[6], (SEQS, LENGTH, D), 1.0, 6.0, ((0, 4), (1, 8)))
    norm_gain = jnp.clip(1.0 + 0.18 * jax.random.normal(streams_of[7], (D,), jnp.float32), 0.1, 1.9)
    expert_gate = gaussian(streams_of[8], (EXPERTS, D, EXPERT_FF), D ** -0.5, 0.125, ((0, 8),))
    expert_up = gaussian(streams_of[9], (EXPERTS, D, EXPERT_FF), D ** -0.5, 0.125, ((0, 8),))
    expert_down = gaussian(streams_of[10], (EXPERTS, EXPERT_FF, D), EXPERT_FF ** -0.5, 0.125, ((0, 8),))
    routes_keys = jax.random.split(jax.random.fold_in(streams_of[11], 1), SEQS * LENGTH // HALF)
    routes_turns = jax.random.permutation(jax.random.fold_in(streams_of[11], 3), SEQS * LENGTH // HALF)
    routes = jax.vmap(lambda own, number: shared_out(jax.random.fold_in(streams_of[11], 2), own, number, HALF, EXPERTS, 2, CAP, 2))(routes_keys, routes_turns).reshape((SEQS, LENGTH, 2))
    route_weight = jnp.clip(0.25 + 0.75 * jax.random.uniform(streams_of[12], (SEQS, LENGTH, 2), jnp.float32) ** block_levels(streams_of[12], (SEQS, LENGTH, 2), ((0, 4), (1, 8)), -0.2, 0.2), 0.25, 1.0)
    return {"queries": queries, "key_rows": key_rows, "values": values, "query_gain": query_gain, "key_gain": key_gain, "out_weight": out_weight, "residual": residual, "norm_gain": norm_gain, "expert_gate": expert_gate, "expert_up": expert_up, "expert_down": expert_down, "routes": routes, "route_weight": route_weight}


EPS = 1e-06
THETA = 10000.0

def rotate_half(vector, position):
    half_size = vector.shape[-1] // 2
    inverse = THETA ** (-jnp.arange(half_size, dtype=jnp.float32) / half_size)
    angles = position[:, None] * inverse[None, :]
    cosine = jnp.cos(angles)[:, None, :]
    sine_part = jnp.sin(angles)[:, None, :]
    first_part = vector[..., :half_size]
    second_part = vector[..., half_size:]
    return jnp.concatenate([first_part * cosine - second_part * sine_part, first_part * sine_part + second_part * cosine], axis=-1)

def normalize_rotate(vector, gain, positions):
    as_float = vector.astype(jnp.float32)
    scaled = as_float * lax.rsqrt(lax.optimization_barrier(jnp.mean(as_float * as_float, axis=-1, keepdims=True)) + EPS) * gain
    grid_row = (positions // GRID_W).astype(jnp.float32)
    column = (positions % GRID_W).astype(jnp.float32)
    quarter = scaled.shape[-1] // 2
    turned = jnp.concatenate([rotate_half(scaled[..., :quarter], grid_row), rotate_half(scaled[..., quarter:], column)], axis=-1)
    return turned.astype(jnp.bfloat16)

def softmax_rows(scores):
    row_max = lax.optimization_barrier(jnp.max(scores, axis=-1, keepdims=True))
    exponent = jnp.exp(scores - row_max)
    return (exponent / lax.optimization_barrier(jnp.sum(exponent, axis=-1, keepdims=True))).astype(jnp.bfloat16)

def attend_sequence(rot_query, rot_key, value_rows):
    length = rot_query.shape[0]
    group_size = HEADS // KV_HEADS
    block_size = min(512, length)
    key_float = rot_key.astype(jnp.float32)
    value_float = value_rows.astype(jnp.float32)
    grouped = rot_query.reshape(length // block_size, block_size, KV_HEADS, group_size, HEAD_DIM)

    def one_block(query_block):
        scores = jnp.einsum('qhgd,khd->hgqk', query_block.astype(jnp.float32), key_float) * HEAD_DIM ** (-0.5)
        weights = softmax_rows(scores)
        return jnp.einsum('hgqk,khd->qhgd', weights.astype(jnp.float32), value_float).astype(jnp.bfloat16)
    outputs = lax.map(one_block, grouped)
    return outputs.reshape(length, HEADS * HEAD_DIM)

def reference(queries, key_rows, values, query_gain, key_gain, out_weight, residual, norm_gain, expert_gate, expert_up, expert_down, routes, route_weight):
    positions = jnp.arange(LENGTH, dtype=jnp.int32)

    def one_sequence(inputs):
        query_seq, key_seq, value_seq, residual_seq = inputs
        rot_query = normalize_rotate(query_seq, query_gain, positions)
        rot_key = normalize_rotate(key_seq, key_gain, positions)
        attended = attend_sequence(rot_query, rot_key, value_seq)
        return residual_seq.astype(jnp.float32) + jnp.dot(attended, out_weight, preferred_element_type=jnp.float32)
    mixed_sum = lax.map(one_sequence, (queries, key_rows, values, residual))
    flat_mixed = mixed_sum.reshape(-1, D)
    normed = (flat_mixed * lax.rsqrt(lax.optimization_barrier(jnp.mean(flat_mixed * flat_mixed, axis=-1, keepdims=True)) + EPS) * norm_gain).astype(jnp.bfloat16)
    tokens = flat_mixed.shape[0]
    blocks = tokens // HALF
    chosen = routes.reshape(blocks, HALF * 2)
    onehot = (chosen[..., None] == jnp.arange(EXPERTS, dtype=jnp.int32)).astype(jnp.int32)
    slot_rank = lax.optimization_barrier(jnp.sum(jnp.cumsum(onehot, axis=1) * onehot, axis=-1)) - 1
    slot_index = jnp.arange(blocks, dtype=jnp.int32)[:, None] * CAP + slot_rank
    per_expert = blocks * CAP
    target = (chosen * per_expert + slot_index).reshape(-1).astype(jnp.int32)
    source_row = jnp.repeat(jnp.arange(tokens, dtype=jnp.int32), 2)
    row_table = jnp.full((EXPERTS * per_expert,), tokens, jnp.int32).at[target].set(source_row)
    padded = jnp.concatenate([normed, jnp.zeros((1, D), jnp.bfloat16)], axis=0)

    def one_expert(inputs):
        row_ids, gate_weight, up_weight, down_weight = inputs
        selected = padded[row_ids]
        gate_part = jnp.dot(selected, gate_weight, preferred_element_type=jnp.float32)
        up_part = jnp.dot(selected, up_weight, preferred_element_type=jnp.float32)
        hidden = (jax.nn.silu(gate_part) * up_part).astype(jnp.bfloat16)
        return jnp.dot(hidden, down_weight, preferred_element_type=jnp.float32).astype(jnp.bfloat16)
    outputs = lax.map(one_expert, (row_table.reshape(EXPERTS, per_expert), expert_gate, expert_up, expert_down))
    picked = outputs.reshape(-1, D)[target].astype(jnp.float32).reshape(tokens, 2, D)
    weights = route_weight.reshape(tokens, 2, 1)
    result = flat_mixed + lax.optimization_barrier(jnp.sum(picked * weights, axis=1))
    return result.reshape(SEQS, LENGTH, D).astype(jnp.bfloat16)
```

```python
import functools
import math

import jax
import jax.numpy as jnp
from jax import lax
from jax.experimental import pallas as pl
from jax.experimental.pallas import tpu as pltpu
from jax.sharding import PartitionSpec as P

GRID_W = 64
EPS = 1e-06
THETA = 10000.0
MESH = pl.DeviceIdType.MESH
VMEM = pl.BlockSpec(memory_space=pltpu.VMEM)
ANY = pl.BlockSpec(memory_space=pl.ANY)
F32 = jnp.float32
BF16 = jnp.bfloat16


def rotation_tables(start, rows, width):
    quarter = width // 4
    lane = lax.broadcasted_iota(jnp.int32, (rows, width), 1)
    position = start + lax.broadcasted_iota(jnp.int32, (rows, width), 0)
    place = jnp.where(lane < 2 * quarter, position // GRID_W, position % GRID_W)
    part = lane % (2 * quarter)
    power = (part % quarter).astype(F32) * (-math.log(THETA) / quarter)
    angles = place.astype(F32) * jnp.exp(power)
    sign = jnp.where(part < quarter, -1.0, 1.0).astype(F32)
    return jnp.cos(angles), jnp.sin(angles) * sign


def turn(rows, gain, cosine, sine):
    width = rows.shape[-1]
    quarter = width // 4
    a = rows.astype(F32)
    a = a * lax.rsqrt(jnp.mean(a * a, axis=-1, keepdims=True) + EPS) * gain
    lane = lax.broadcasted_iota(jnp.int32, a.shape, 1) % (2 * quarter)
    partner = jnp.where(
        lane < quarter, pltpu.roll(a, width - quarter, 1), pltpu.roll(a, quarter, 1)
    )
    return (a * cosine + partner * sine).astype(BF16)


class Line:
    def __init__(self, depth, width, block, send, recv):
        self.depth, self.width, self.block = depth, width, block
        self.send, self.recv = send, recv
        me = lax.axis_index("sp")
        self.z, self.x = me // width, me % width
        self.ends = []

    def copy(self, unit, plane, way, target):
        return pltpu.make_async_remote_copy(
            src_ref=self.block(unit, plane * self.width + self.x),
            dst_ref=self.block(unit, plane * self.width + self.x),
            send_sem=self.send.at[unit, plane, way],
            recv_sem=self.recv.at[unit, plane],
            device_id={"sp": target * self.width + self.x},
            device_id_type=MESH,
        )

    def start(self, condition, unit, plane, way, target):
        @pl.when(condition)
        def _():
            self.copy(unit, plane, way, target).start()

        self.ends.append((condition, unit, plane, way, target))

    def up(self, condition, unit, plane):
        self.start(condition & (self.z < self.depth - 1), unit, plane, 0, self.z + 1)

    def down(self, condition, unit, plane):
        self.start(condition & (self.z > 0), unit, plane, 1, self.z - 1)

    def arrive(self, condition, unit, plane):
        @pl.when(condition)
        def _():
            self.copy(unit, plane, 0, plane).wait_recv()

    def step(self, t, unit, condition=True, then=None):
        below = (self.z - t >= 0) & condition
        above = (self.z + t < self.depth) & condition
        self.arrive(below, unit, self.z - t)
        self.up(below, unit, self.z - t)
        if then is not None:
            then(below, unit, self.z - t)
        self.arrive(above, unit, self.z + t)
        self.down(above, unit, self.z + t)
        if then is not None:
            then(above, unit, self.z + t)

    def drain(self):
        for condition, unit, plane, way, target in self.ends:

            @pl.when(condition)
            def _():
                self.copy(unit, plane, way, target).wait_send()


def slot_choice(table, base, slots, capacity):
    rows = table.shape[0]
    slot = lax.broadcasted_iota(jnp.int32, (rows, slots), 1)
    expert = (slot // capacity + base).astype(F32)
    first = table[:, 0:1] == expert
    second = table[:, 1:2] == expert
    named = jnp.where(first | second, 1.0, 0.0).astype(BF16)
    earlier = lax.broadcasted_iota(jnp.int32, (rows, rows), 1) < lax.broadcasted_iota(
        jnp.int32, (rows, rows), 0
    )
    rank = jnp.dot(
        jnp.where(earlier, 1.0, 0.0).astype(BF16), named, preferred_element_type=F32
    )
    here = rank == (slot % capacity).astype(F32)
    return (
        jnp.where(first & here, 1.0, 0.0).astype(BF16),
        jnp.where(second & here, 1.0, 0.0).astype(BF16),
    )


def attention_part(
    n,
    dp,
    start_loads,
    q_ref,
    k_ref,
    v_ref,
    qg_ref,
    kg_ref,
    w_ref,
    res_ref,
    ng_ref,
    routes_ref,
    gates_ref,
    mixed_ref,
    normed_ref,
    own_table,
    table,
    q_in,
    k_in,
    v_in,
    wide,
    stage,
    q_stage,
    q_all,
    kv,
    w_full,
    swap,
    att,
    proj,
    back,
    res_in,
    gains,
    norm_in,
    in_sem,
    kvx_send,
    kvx_recv,
    kvz_send,
    kvz_recv,
    qx_send,
    qx_recv,
    wx_send,
    wx_recv,
    wz_send,
    wz_recv,
    ax_send,
    ax_recv,
    t_sem,
    y_send,
    y_recv,
    pair_send,
    pair_recv,
    fwd_send,
    fwd_recv,
    back_send,
    back_recv,
):
    me = lax.axis_index("sp")
    mine = lax.axis_index("dp")
    rows, heads, width = q_ref.shape
    kv_heads = k_ref.shape[1]
    group = heads // kv_heads
    model = heads * width
    across = stage.shape[0]
    depth = n // across
    local_kv = kv_heads // across
    local = heads // across
    z, x = me // across, me % across
    always = me >= 0
    ny = dp // 2
    core = mine % 2
    row_y = mine // 2
    partner = row_y * 2 + 1 - core
    w_rows, w_cols = w_ref.shape

    def span(start, size):
        return pl.ds(pl.multiple_of(start * size, size), size)

    fetches = [
        pltpu.make_async_copy(src, dst, in_sem.at[i])
        for i, (src, dst) in enumerate(
            (
                (k_ref, k_in),
                (v_ref, v_in),
                (kg_ref, gains.at[0]),
                (q_ref, q_in),
                (qg_ref, gains.at[1]),
                (w_ref, w_full.at[span(me, w_rows)]),
                (res_ref, res_in),
                (ng_ref, norm_in),
            )
        )
    ]
    for fetch in fetches:
        fetch.start()
    barrier = pltpu.get_barrier_semaphore()
    for d in range(1, n):
        pl.semaphore_signal(
            barrier, inc=1, device_id={"sp": lax.rem(me + d, n)}, device_id_type=MESH
        )
    for d in range(1, dp):
        pl.semaphore_signal(
            barrier, inc=1, device_id={"dp": lax.rem(mine + d, dp)}, device_id_type=MESH
        )

    cosine, sine = rotation_tables(me * rows, rows, width)
    my_rows = span(me, rows)
    for fetch in fetches[:3]:
        fetch.wait()
    for part, source in ((0, k_in), (1, v_in)):
        wide[:, 0:kv_heads, :] = source[...].astype(F32)
        for g in range(kv_heads):
            lines = wide[:, g, :]
            slot = 2 * (g % local_kv) + part
            if part == 0:
                lines = turn(lines, gains[0], cosine, sine)
            stage[g // local_kv, slot] = lines.astype(BF16)
    for c in range(2 * local_kv):
        kv[c, my_rows, :] = stage[x, c]
    pl.semaphore_wait(barrier, n - 1 + dp - 1)

    def remote(src, dst, send, recv, **device):
        return pltpu.make_async_remote_copy(
            src_ref=src,
            dst_ref=dst,
            send_sem=send,
            recv_sem=recv,
            device_id=device,
            device_id_type=MESH,
        )

    def beside(k):
        return z * across + lax.rem(x + k, across)

    def kv_block(g, sp):
        return kv.at[pl.ds(2 * g, 2), span(sp, rows), :]

    kv_units = [(k, g) for k in range(across) for g in range(local_kv)]

    def kv_unit(u, sp):
        k, g = kv_units[u]
        return kv_block(g, sp - sp % across + lax.rem(sp % across + k, across))

    halves = 2
    w_units = [(j, k) for j in range(halves) for k in range(2)]
    part_rows, part_cols = w_rows // 2, w_cols // halves

    def w_unit(u, sp):
        j, k = w_units[u]
        start = pl.multiple_of(sp * w_rows + k * part_rows, part_rows)
        return w_full.at[pl.ds(start, part_rows), pl.ds(j * part_cols, part_cols)]

    kv_line = Line(depth, across, kv_unit, kvz_send, kvz_recv)
    w_line = Line(depth, across, w_unit, wz_send, wz_recv)
    kvx, qx, ax, wx = {}, {}, {}, []
    for g in range(local_kv):
        for k in range(1, across):
            kvx[k, g] = remote(
                stage.at[lax.rem(x + k, across), pl.ds(2 * g, 2)],
                kv_block(g, me),
                kvx_send.at[k, g],
                kvx_recv.at[across - k, g],
                sp=beside(k),
            )
            kvx[k, g].start()
        kv_line.up(always, g, z)
        kv_line.down(always, g, z)

    start_loads()
    fetches[3].wait()
    fetches[4].wait()
    for h in range(0, heads, 8):
        wide[:, h : h + 8, :] = q_in[:, h : h + 8, :].astype(F32)
    for k in list(range(1, across)) + [0]:
        first = lax.rem(x + k, across) * local

        def turn_head(i, carry):
            lines = turn(wide[:, pl.ds(first + i, 1), :].reshape(rows, width), gains[1], cosine, sine)
            if k == 0:
                q_all[i, 0:rows] = lines
            else:
                q_stage[k - 1, i] = lines
            return carry

        lax.fori_loop(0, local, turn_head, 0)
        if k > 0:
            qx[k] = remote(
                q_stage.at[k - 1],
                q_all.at[:, pl.ds((across - k) * rows, rows), :],
                qx_send.at[k],
                qx_recv.at[across - k],
                sp=beside(k),
            )
            qx[k].start()
        if k == across - 1:
            for u in range(local_kv, len(kv_units)):
                kk, g = kv_units[u]
                remote(
                    stage.at[0, pl.ds(2 * g, 2)],
                    kv_block(g, beside(kk)),
                    kvx_send.at[kk, g],
                    kvx_recv.at[kk, g],
                    sp=me,
                ).wait_recv()
                kv_line.up(always, u, z)
                kv_line.down(always, u, z)
    fetches[5].wait()

    def w_across(condition, u, plane):
        for k in range(1, across):

            def copy():
                return remote(
                    w_unit(u, plane * across + x),
                    w_unit(u, plane * across + x),
                    wx_send.at[u, plane, k],
                    wx_recv.at[u, plane, across - k],
                    sp=beside(k),
                )

            @pl.when(condition)
            def _():
                copy().start()

            wx.append((condition, copy))

    def w_begin(t):
        for u in range(len(w_units)):
            w_line.up(z == t, u, z)
            w_line.down(depth - 1 - z == t, u, z)

    w_begin(0)
    lanes = jnp.concatenate(
        [
            routes_ref[...].astype(F32),
            gates_ref[...],
            jnp.zeros((width - 4, rows), F32),
        ],
        axis=0,
    )
    own_table[...] = lanes.T
    table_copy = remote(
        own_table, table, t_sem.at[0], t_sem.at[1], sp=lax.rem(me + n // 2, n)
    )
    table_copy.start()
    for u in range(len(w_units)):
        w_across(always, u, z)
    for t in range(1, depth):
        for u in range(len(kv_units)):
            kv_line.step(t, u)
        w_begin(t)
    middle = (z > 0) & (z < depth - 1)
    for u in range(len(w_units)):
        w_line.step(1, u, middle, w_across)
    for k in range(1, across):
        remote(
            q_stage.at[0],
            q_all.at[:, pl.ds(k * rows, rows), :],
            qx_send.at[k],
            qx_recv.at[k],
            sp=me,
        ).wait_recv()

    scale = width ** (-0.5)
    wide_group = group * width

    def att_cols(k, g):
        side = lax.rem(x + k, across)
        start = (side * local_kv + g) * wide_group
        return pl.ds(pl.multiple_of(start, wide_group), wide_group)

    y_copies, pair_copies, fwd_copies = {}, {}, {}

    def spread_att(u):
        k, g = kv_units[u]
        block = att.at[mine, :, att_cols(k, g)]
        for j in range(1, ny):
            target = lax.rem(row_y + j, ny) * 2 + core
            copy = remote(block, block, y_send.at[j, u], y_recv.at[j, u], dp=target)
            copy.start()
            y_copies[j, u] = copy
        copy = remote(block, block, pair_send.at[u], pair_recv.at[u], dp=partner)
        copy.start()
        pair_copies[u] = copy

    def forward(u):
        for j in range(1, ny):
            source = lax.rem(row_y + ny - j, ny) * 2 + core
            y_copies[j, u].wait_recv()
            block = att.at[source, :, att_cols(*kv_units[u])]
            copy = remote(block, block, fwd_send.at[j, u], fwd_recv.at[j, u], dp=partner)
            copy.start()
            fwd_copies[j, u] = copy

    for g in range(local_kv):

        def one_head(i, carry):
            h = g * group + i
            scores = (
                lax.dot_general(
                    q_all[h], kv[2 * g], (((1,), (1,)), ((), ())), preferred_element_type=F32
                )
                * scale
            )
            exponent = jnp.exp(scores - jnp.max(scores, axis=-1, keepdims=True))
            weights = (exponent / jnp.sum(exponent, axis=-1, keepdims=True)).astype(BF16)
            out = jnp.dot(weights, kv[2 * g + 1], preferred_element_type=F32).astype(BF16)
            cols = pl.ds(pl.multiple_of((x * local + h) * width, width), width)
            att[mine, :, cols] = out[0:rows]
            cols = pl.ds(pl.multiple_of(h * width, width), width)
            for k in range(1, across):
                swap[k - 1, :, cols] = out[k * rows : (k + 1) * rows]
            return carry

        lax.fori_loop(0, group, one_head, 0)
        for k in range(1, across):
            ax[k, g] = remote(
                swap.at[k - 1, :, pl.ds(g * wide_group, wide_group)],
                att.at[mine, :, att_cols(0, g)],
                ax_send.at[k, g],
                ax_recv.at[across - k, g],
                sp=beside(k),
            )
            ax[k, g].start()
        spread_att(g)
        if g == 0:
            for u in range(len(w_units)):
                w_line.step(1, u, jnp.logical_not(middle), w_across)
    for t in range(2, depth - 1):
        for u in range(len(w_units)):
            w_line.step(t, u, True, w_across)
    for u in range(local_kv, len(kv_units)):
        k, g = kv_units[u]
        remote(
            swap.at[0, :, pl.ds(g * wide_group, wide_group)],
            att.at[mine, :, att_cols(k, g)],
            ax_send.at[k, g],
            ax_recv.at[k, g],
            sp=me,
        ).wait_recv()
        spread_att(u)
    for u in range(len(kv_units)):
        forward(u)
    for u in range(len(w_units)):
        w_line.step(depth - 1, u, True, w_across)
    for u in range(len(kv_units)):
        pair_copies[u].wait_recv()
        for j in range(1, ny):
            fwd_copies[j, u].wait_recv()

    back_copies = {}
    for j in range(halves):
        for u, (jj, _) in enumerate(w_units):
            if jj != j:
                continue
            for plane in range(depth):
                for k in range(1, across):
                    remote(
                        w_unit(u, plane * across + x),
                        w_unit(u, plane * across + lax.rem(x + k, across)),
                        wx_send.at[u, plane, k],
                        wx_recv.at[u, plane, k],
                        sp=me,
                    ).wait_recv()
        cols = slice(j * part_cols, (j + 1) * part_cols)
        result = jnp.dot(
            att[...].reshape(dp * rows, model), w_full[:, cols], preferred_element_type=F32
        ).astype(BF16)
        for s in range(dp):
            proj[s, :, cols] = result[s * rows : (s + 1) * rows]
        back[mine, :, cols] = proj[mine, :, cols]
        order = sorted(range(1, dp), key=lambda d: d % 2)
        for d in order:
            target = lax.rem(mine + d, dp)
            copy = remote(
                proj.at[target, :, cols],
                back.at[mine, :, cols],
                back_send.at[d, j],
                back_recv.at[d, j],
                dp=target,
            )
            copy.start()
            back_copies[d, j] = copy

    kv_line.drain()
    w_line.drain()
    for condition, copy in wx:

        @pl.when(condition)
        def _():
            copy().wait_send()

    for copies in (kvx, qx, ax):
        for copy in copies.values():
            copy.wait_send()
    table_copy.wait()
    fetches[6].wait()
    fetches[7].wait()
    for copies in (y_copies, pair_copies, fwd_copies):
        for copy in copies.values():
            copy.wait_send()
    for copy in back_copies.values():
        copy.wait()
    square = jnp.zeros((rows, 1), F32)
    for s in range(dp):
        cols = slice(s * w_cols, (s + 1) * w_cols)
        part = res_in[:, cols].astype(F32) + back[s].astype(F32)
        mixed_ref[:, cols] = part
        square = square + jnp.sum(part * part, axis=-1, keepdims=True)
    factor = lax.rsqrt(square / model + EPS)
    for s in range(dp):
        cols = slice(s * w_cols, (s + 1) * w_cols)
        normed_ref[:, cols] = (mixed_ref[:, cols] * factor * norm_in[:, cols]).astype(BF16)


def expert_part(
    n,
    capacity,
    normed_ref,
    mixed_ref,
    own_ref,
    other_ref,
    loads,
    out_ref,
    gate,
    up,
    down,
    relay,
    sent,
    recv,
    hidden,
    res,
    ret,
    part,
    home,
    hold,
    relay_sem,
    home_sem,
    go_send,
    go_recv,
    ret_send,
    ret_recv,
):
    me = lax.axis_index("sp")
    half = n // 2
    base = me // half * half
    mine = me % half
    partner = lax.rem(me + half, n)
    rows, model = normed_ref.shape
    few = rows // 2
    slots = half * capacity
    ff = gate.shape[1]

    def peer(k):
        return base + lax.rem(mine + k, half)

    relays = []
    for b in range(2):
        copy = pltpu.make_async_remote_copy(
            src_ref=normed_ref.at[pl.ds(b * few, few)],
            dst_ref=relay.at[b],
            send_sem=relay_sem.at[0, b],
            recv_sem=relay_sem.at[1, b],
            device_id={"sp": partner},
            device_id_type=MESH,
        )
        copy.start()
        relays.append(copy)

    def block(index):
        return pl.ds(pl.multiple_of(index * capacity, capacity), capacity)

    go, back, homes = {}, {}, []

    def choices(r):
        table = own_ref if r < 2 else other_ref
        return slot_choice(table[(r % 2) * few : (r % 2 + 1) * few], base, slots, capacity)

    def dispatch(r):
        first, second = choices(r)
        choice = first + second
        lines = normed_ref[(r % 2) * few : (r % 2 + 1) * few] if r < 2 else relay[r % 2]
        for t in range(model // 512):
            cols = slice(t * 512, (t + 1) * 512)
            sent[r, :, cols] = lax.dot_general(
                choice, lines[:, cols], (((0,), (0,)), ((), ())), preferred_element_type=F32
            ).astype(BF16)
        recv[r, block(mine)] = sent[r, block(mine)]
        for k in range(1, half):
            copy = pltpu.make_async_remote_copy(
                src_ref=sent.at[r, block(lax.rem(mine + k, half))],
                dst_ref=recv.at[r, block(mine)],
                send_sem=go_send.at[r, k],
                recv_sem=go_recv.at[r, k],
                device_id={"sp": peer(k)},
                device_id_type=MESH,
            )
            copy.start()
            go[r, k] = copy

    tile = 256

    def serve(r):
        for k in range(1, half):
            go[r, k].wait_recv()

        def up_tile(t, carry):
            cols = pl.ds(pl.multiple_of(t * tile, tile), tile)
            gate_part = jnp.dot(recv[r], gate[:, cols], preferred_element_type=F32)
            up_part = jnp.dot(recv[r], up[:, cols], preferred_element_type=F32)
            hidden[:, cols] = (gate_part / (1.0 + jnp.exp(-gate_part)) * up_part).astype(BF16)
            return carry

        lax.fori_loop(0, ff // tile, up_tile, 0)
        if r == 0:
            loads[2].wait()

        def down_tile(t, carry):
            cols = pl.ds(pl.multiple_of(t * tile, tile), tile)
            res[r, :, cols] = jnp.dot(
                hidden[...], down[:, cols], preferred_element_type=F32
            ).astype(BF16)
            return carry

        lax.fori_loop(0, model // tile, down_tile, 0)
        ret[r, block(mine)] = res[r, block(mine)]
        for k in range(1, half):
            copy = pltpu.make_async_remote_copy(
                src_ref=res.at[r, block(lax.rem(mine + k, half))],
                dst_ref=ret.at[r, block(mine)],
                send_sem=ret_send.at[r, k],
                recv_sem=ret_recv.at[r, k],
                device_id={"sp": peer(k)},
                device_id_type=MESH,
            )
            copy.start()
            back[r, k] = copy

    def combine(r, store):
        first, second = choices(r)
        table = own_ref if r < 2 else other_ref
        lines = slice((r % 2) * few, (r % 2 + 1) * few)
        for k in range(1, half):
            back[r, k].wait_recv()
        for t in range(model // 512):
            cols = slice(t * 512, (t + 1) * 512)
            served = ret[r, :, cols]
            store(
                lines,
                cols,
                jnp.dot(first, served, preferred_element_type=F32) * table[lines, 2:3]
                + jnp.dot(second, served, preferred_element_type=F32) * table[lines, 3:4],
            )

    def store_part(lines, cols, value):
        part[lines, cols] = value.astype(BF16)

    def send_home(b):
        combine(2 + b, store_part)
        copy = pltpu.make_async_remote_copy(
            src_ref=part.at[pl.ds(b * few, few)],
            dst_ref=home.at[b],
            send_sem=home_sem.at[0, b],
            recv_sem=home_sem.at[1, b],
            device_id={"sp": partner},
            device_id_type=MESH,
        )
        copy.start()
        homes.append(copy)

    def store_own(lines, cols, value):
        hold[lines, cols] = mixed_ref[lines, cols] + value

    dispatch(0)
    dispatch(1)
    loads[0].wait()
    loads[1].wait()
    serve(0)
    relays[0].wait_recv()
    dispatch(2)
    serve(1)
    relays[1].wait_recv()
    dispatch(3)
    serve(2)
    serve(3)
    send_home(0)
    send_home(1)
    combine(0, store_own)
    combine(1, store_own)
    for b in range(2):
        homes[b].wait_recv()
        lines = slice(b * few, (b + 1) * few)
        out_ref[lines] = (hold[lines] + home[b].astype(F32)).astype(BF16)
    for b in range(2):
        relays[b].wait_send()
        homes[b].wait_send()
    for r in range(4):
        for k in range(1, half):
            go[r, k].wait_send()
            back[r, k].wait_send()


def layer_kernel(n, dp, capacity, *refs):
    inputs, refs = refs[:10], refs[10:]
    weights, out_ref, refs = refs[:3], refs[3], refs[4:]
    middle, refs = refs[:4], refs[4:]
    attention, refs = refs[:38], refs[38:]
    load_sem, stores, experts = refs[0], refs[1:4], refs[4:]
    loads = [
        pltpu.make_async_copy(src.at[0], dst, load_sem.at[i])
        for i, (src, dst) in enumerate(zip(weights, stores))
    ]

    def start_loads():
        for load in loads:
            load.start()

    attention_part(n, dp, start_loads, *inputs, *middle, *attention)
    mixed, normed, own, other = middle
    expert_part(n, capacity, normed, mixed, own, other, loads, out_ref, *stores, *experts)


def on_device(
    n,
    dp,
    queries,
    key_rows,
    values,
    query_gain,
    key_gain,
    out_weight,
    residual,
    norm_gain,
    expert_gate,
    expert_up,
    expert_down,
    routes,
    route_weight,
):
    _, rows, heads, width = queries.shape
    kv_heads = key_rows.shape[2]
    model = heads * width
    length = rows * n
    experts = expert_gate.shape[0] * n
    capacity = max(2, 4 * (rows // 2) // experts)
    slots = n // 2 * capacity
    across = max(x for x in range(1, n + 1) if n % x == 0 and x * x <= n)
    depth = n // across
    local_kv, local = kv_heads // across, heads // across
    units = across * local_kv
    w_rows, w_cols = out_weight.shape
    dma = pltpu.SemaphoreType.DMA
    ny = dp // 2
    ff = expert_gate.shape[2]
    few = rows // 2
    attention_scratch = [
        pltpu.VMEM((rows, heads, width), BF16),
        pltpu.VMEM((rows, kv_heads, width), BF16),
        pltpu.VMEM((rows, kv_heads, width), BF16),
        pltpu.VMEM((rows, heads, width), F32),
        pltpu.VMEM((across, 2 * local_kv, rows, width), BF16),
        pltpu.VMEM((across - 1, local, rows, width), BF16),
        pltpu.VMEM((local, across * rows, width), BF16),
        pltpu.VMEM((2 * local_kv, length, width), BF16),
        pltpu.VMEM((w_rows * n, w_cols), BF16),
        pltpu.VMEM((across - 1, rows, local * width), BF16),
        pltpu.VMEM((dp, rows, model), BF16),
        pltpu.VMEM((dp, rows, w_cols), BF16),
        pltpu.VMEM((dp, rows, w_cols), BF16),
        pltpu.VMEM((rows, model), BF16),
        pltpu.VMEM((2, 1, width), F32),
        pltpu.VMEM((1, model), F32),
        dma((8,)),
        dma((across, local_kv)),
        dma((across, local_kv)),
        dma((units, depth, 2)),
        dma((units, depth)),
        dma((across,)),
        dma((across,)),
        dma((4, depth, across)),
        dma((4, depth, across)),
        dma((4, depth, 2)),
        dma((4, depth)),
        dma((across, local_kv)),
        dma((across, local_kv)),
        dma((2,)),
        dma((ny, units)),
        dma((ny, units)),
        dma((units,)),
        dma((units,)),
        dma((ny, units)),
        dma((ny, units)),
        dma((dp, 2)),
        dma((dp, 2)),
    ]
    result = pl.pallas_call(
        functools.partial(layer_kernel, n, dp, capacity),
        out_shape=jax.ShapeDtypeStruct((rows, model), BF16),
        in_specs=[ANY] * 8 + [VMEM] * 2 + [ANY] * 3,
        out_specs=VMEM,
        scratch_shapes=[
            pltpu.VMEM((rows, model), F32),
            pltpu.VMEM((rows, model), BF16),
            pltpu.VMEM((rows, width), F32),
            pltpu.VMEM((rows, width), F32),
            *attention_scratch,
            dma((3,)),
            pltpu.VMEM((model, ff), BF16),
            pltpu.VMEM((model, ff), BF16),
            pltpu.VMEM((ff, model), BF16),
            pltpu.VMEM((2, few, model), BF16),
            pltpu.VMEM((4, slots, model), BF16),
            pltpu.VMEM((4, slots, model), BF16),
            pltpu.VMEM((slots, ff), BF16),
            pltpu.VMEM((4, slots, model), BF16),
            pltpu.VMEM((4, slots, model), BF16),
            pltpu.VMEM((rows, model), BF16),
            pltpu.VMEM((2, few, model), BF16),
            pltpu.VMEM((rows, model), F32),
            dma((2, 2)),
            dma((2, 2)),
            dma((4, n)),
            dma((4, n)),
            dma((4, n)),
            dma((4, n)),
        ],
        compiler_params=pltpu.CompilerParams(
            collective_id=0, has_side_effects=True, vmem_limit_bytes=56 * 1024 * 1024
        ),
        name="layer",
    )(
        queries[0],
        key_rows[0],
        values[0],
        query_gain[None],
        key_gain[None],
        out_weight,
        residual[0],
        norm_gain[None],
        routes[0].T,
        route_weight[0].T,
        expert_gate,
        expert_up,
        expert_down,
    )
    return result[None]


def solution(mesh):
    in_specs = (
        P("dp", "sp", None, None),
        P("dp", "sp", None, None),
        P("dp", "sp", None, None),
        P(),
        P(),
        P("sp", "dp"),
        P("dp", "sp", None),
        P(),
        P("sp", None, None),
        P("sp", None, None),
        P("sp", None, None),
        P("dp", "sp", None),
        P("dp", "sp", None),
    )
    out_specs = P("dp", "sp", None)
    return jax.shard_map(
        functools.partial(on_device, mesh.shape["sp"], mesh.shape["dp"]),
        mesh=mesh,
        in_specs=in_specs,
        out_specs=out_specs,
        check_vma=False,
    )
```

```python
import functools
import math

import jax
import jax.numpy as jnp
from jax import lax
from jax.experimental import pallas as pl
from jax.experimental.pallas import tpu as pltpu
from jax.sharding import PartitionSpec as P

GRID_W = 64
EPS = 1e-06
CHUNKS = 4
TILE = 256
THETA = 10000.0
MESH = pl.DeviceIdType.MESH
VMEM = pl.BlockSpec(memory_space=pltpu.VMEM)
ANY = pl.BlockSpec(memory_space=pl.ANY)
F32 = jnp.float32
BF16 = jnp.bfloat16


def rotation_tables(start, rows, width):
    quarter = width // 4
    lane = lax.broadcasted_iota(jnp.int32, (rows, width), 1)
    position = start + lax.broadcasted_iota(jnp.int32, (rows, width), 0)
    place = jnp.where(lane < 2 * quarter, position // GRID_W, position % GRID_W)
    part = lane % (2 * quarter)
    power = (part % quarter).astype(F32) * (-math.log(THETA) / quarter)
    angles = place.astype(F32) * jnp.exp(power)
    sign = jnp.where(part < quarter, -1.0, 1.0).astype(F32)
    return jnp.cos(angles), jnp.sin(angles) * sign


def turn(rows, gain, cosine, sine):
    width = rows.shape[-1]
    quarter = width // 4
    a = rows.astype(F32)
    a = a * lax.rsqrt(jnp.mean(a * a, axis=-1, keepdims=True) + EPS) * gain
    lane = lax.broadcasted_iota(jnp.int32, a.shape, 1) % (2 * quarter)
    partner = jnp.where(
        lane < quarter, pltpu.roll(a, width - quarter, 1), pltpu.roll(a, quarter, 1)
    )
    return (a * cosine + partner * sine).astype(BF16)


class Line:
    def __init__(self, depth, width, block, send, recv):
        self.depth, self.width, self.block = depth, width, block
        self.send, self.recv = send, recv
        me = lax.axis_index("sp")
        self.z, self.x = me // width, me % width
        self.ends = []

    def copy(self, unit, plane, way, target):
        return pltpu.make_async_remote_copy(
            src_ref=self.block(unit, plane * self.width + self.x),
            dst_ref=self.block(unit, plane * self.width + self.x),
            send_sem=self.send.at[unit, plane, way],
            recv_sem=self.recv.at[unit, plane],
            device_id={"sp": target * self.width + self.x},
            device_id_type=MESH,
        )

    def start(self, condition, unit, plane, way, target):
        @pl.when(condition)
        def _():
            self.copy(unit, plane, way, target).start()

        self.ends.append((condition, unit, plane, way, target))

    def up(self, condition, unit, plane):
        self.start(condition & (self.z < self.depth - 1), unit, plane, 0, self.z + 1)

    def down(self, condition, unit, plane):
        self.start(condition & (self.z > 0), unit, plane, 1, self.z - 1)

    def arrive(self, condition, unit, plane):
        @pl.when(condition)
        def _():
            self.copy(unit, plane, 0, plane).wait_recv()

    def step(self, t, unit, condition=True, then=None):
        below = (self.z - t >= 0) & condition
        above = (self.z + t < self.depth) & condition
        self.arrive(below, unit, self.z - t)
        self.up(below, unit, self.z - t)
        if then is not None:
            then(below, unit, self.z - t)
        self.arrive(above, unit, self.z + t)
        self.down(above, unit, self.z + t)
        if then is not None:
            then(above, unit, self.z + t)

    def drain(self):
        for condition, unit, plane, way, target in self.ends:

            @pl.when(condition)
            def _():
                self.copy(unit, plane, way, target).wait_send()


def selection(table, first_expert, column, columns, capacity):
    rows = table.shape[1]
    few = rows // 2
    slots = columns * 2 * capacity
    slot = lax.broadcasted_iota(jnp.int32, (slots, rows), 0)
    row = lax.broadcasted_iota(jnp.int32, (slots, rows), 1)
    side = (column + slot // (2 * capacity)) % columns
    expert = (first_expert + side).astype(F32)
    same = (slot // capacity) % 2 == row // few
    first = (table[0:1, :] == expert) & same
    second = (table[1:2, :] == expert) & same
    named = jnp.where(first | second, 1.0, 0.0).astype(BF16)
    before = lax.broadcasted_iota(jnp.int32, (rows, rows), 0)
    after = lax.broadcasted_iota(jnp.int32, (rows, rows), 1)
    earlier = jnp.where(before < after, 1.0, 0.0).astype(BF16)
    rank = jnp.dot(named, earlier, preferred_element_type=F32)
    here = rank == (slot % capacity).astype(F32)
    choice = jnp.where((first | second) & here, 1.0, 0.0)
    weight = jnp.where(first & here, table[2:3, :], 0.0)
    weight = weight + jnp.where(second & here, table[3:4, :], 0.0)
    weight = weight.T
    high = weight.astype(BF16)
    low = (weight - high.astype(F32)).astype(BF16)
    return choice.astype(BF16), high, low


def attention_part(
    n,
    dp,
    start_loads,
    q_ref,
    k_ref,
    v_ref,
    qg_ref,
    kg_ref,
    w_ref,
    res_ref,
    ng_ref,
    mixed_ref,
    normed_ref,
    prepare,
    q_in,
    k_in,
    v_in,
    wide,
    stage,
    q_stage,
    q_all,
    kv,
    w_full,
    swap,
    att,
    proj,
    back,
    res_in,
    gains,
    norm_in,
    in_sem,
    kvx_send,
    kvx_recv,
    kvz_send,
    kvz_recv,
    qx_send,
    qx_recv,
    wx_send,
    wx_recv,
    wz_send,
    wz_recv,
    ax_send,
    ax_recv,
    y_send,
    y_recv,
    pair_send,
    pair_recv,
    fwd_send,
    fwd_recv,
    back_send,
    back_recv,
):
    me = lax.axis_index("sp")
    mine = lax.axis_index("dp")
    rows, heads, width = q_ref.shape
    kv_heads = k_ref.shape[1]
    group = heads // kv_heads
    model = heads * width
    across = stage.shape[0]
    depth = n // across
    local_kv = kv_heads // across
    local = heads // across
    z, x = me // across, me % across
    always = me >= 0
    ny = dp // 2
    core = mine % 2
    row_y = mine // 2
    partner = row_y * 2 + 1 - core
    w_rows, w_cols = w_ref.shape

    def span(start, size):
        return pl.ds(pl.multiple_of(start * size, size), size)

    fetches = [
        pltpu.make_async_copy(src, dst, in_sem.at[i])
        for i, (src, dst) in enumerate(
            (
                (k_ref, k_in),
                (v_ref, v_in),
                (kg_ref, gains.at[0]),
                (q_ref, q_in),
                (qg_ref, gains.at[1]),
                (w_ref, w_full.at[span(me, w_rows)]),
                (res_ref, res_in),
                (ng_ref, norm_in),
            )
        )
    ]
    for fetch in fetches:
        fetch.start()
    barrier = pltpu.get_barrier_semaphore()
    for d in range(1, n):
        pl.semaphore_signal(
            barrier, inc=1, device_id={"sp": lax.rem(me + d, n)}, device_id_type=MESH
        )
    for d in range(1, dp):
        pl.semaphore_signal(
            barrier, inc=1, device_id={"dp": lax.rem(mine + d, dp)}, device_id_type=MESH
        )

    cosine, sine = rotation_tables(me * rows, rows, width)
    my_rows = span(me, rows)
    for fetch in fetches[:3]:
        fetch.wait()
    for part, source in ((0, k_in), (1, v_in)):
        wide[:, 0:kv_heads, :] = source[...].astype(F32)
        for g in range(kv_heads):
            lines = wide[:, g, :]
            slot = 2 * (g % local_kv) + part
            if part == 0:
                lines = turn(lines, gains[0], cosine, sine)
            stage[g // local_kv, slot] = lines.astype(BF16)
    for c in range(2 * local_kv):
        kv[c, my_rows, :] = stage[x, c]
    pl.semaphore_wait(barrier, n - 1 + dp - 1)

    def remote(src, dst, send, recv, **device):
        return pltpu.make_async_remote_copy(
            src_ref=src,
            dst_ref=dst,
            send_sem=send,
            recv_sem=recv,
            device_id=device,
            device_id_type=MESH,
        )

    def beside(k):
        return z * across + lax.rem(x + k, across)

    def kv_block(g, sp):
        return kv.at[pl.ds(2 * g, 2), span(sp, rows), :]

    kv_units = [(k, g) for k in range(across) for g in range(local_kv)]

    def kv_unit(u, sp):
        k, g = kv_units[u]
        return kv_block(g, sp - sp % across + lax.rem(sp % across + k, across))

    halves = 2
    w_units = [(j, k) for j in range(halves) for k in range(2)]
    part_rows, part_cols = w_rows // 2, w_cols // halves

    def w_unit(u, sp):
        j, k = w_units[u]
        start = pl.multiple_of(sp * w_rows + k * part_rows, part_rows)
        return w_full.at[pl.ds(start, part_rows), pl.ds(j * part_cols, part_cols)]

    kv_line = Line(depth, across, kv_unit, kvz_send, kvz_recv)
    w_line = Line(depth, across, w_unit, wz_send, wz_recv)
    kvx, qx, ax, wx = {}, {}, {}, []
    for g in range(local_kv):
        for k in range(1, across):
            kvx[k, g] = remote(
                stage.at[lax.rem(x + k, across), pl.ds(2 * g, 2)],
                kv_block(g, me),
                kvx_send.at[k, g],
                kvx_recv.at[across - k, g],
                sp=beside(k),
            )
            kvx[k, g].start()
        kv_line.up(always, g, z)
        kv_line.down(always, g, z)

    start_loads()
    fetches[3].wait()
    fetches[4].wait()
    for h in range(0, heads, 8):
        wide[:, h : h + 8, :] = q_in[:, h : h + 8, :].astype(F32)
    for k in list(range(1, across)) + [0]:
        first = lax.rem(x + k, across) * local

        def turn_head(i, carry):
            lines = turn(wide[:, pl.ds(first + i, 1), :].reshape(rows, width), gains[1], cosine, sine)
            if k == 0:
                q_all[i, 0:rows] = lines
            else:
                q_stage[k - 1, i] = lines
            return carry

        lax.fori_loop(0, local, turn_head, 0)
        if k > 0:
            qx[k] = remote(
                q_stage.at[k - 1],
                q_all.at[:, pl.ds((across - k) * rows, rows), :],
                qx_send.at[k],
                qx_recv.at[across - k],
                sp=beside(k),
            )
            qx[k].start()
        if k == across - 1:
            for u in range(local_kv, len(kv_units)):
                kk, g = kv_units[u]
                remote(
                    stage.at[0, pl.ds(2 * g, 2)],
                    kv_block(g, beside(kk)),
                    kvx_send.at[kk, g],
                    kvx_recv.at[kk, g],
                    sp=me,
                ).wait_recv()
                kv_line.up(always, u, z)
                kv_line.down(always, u, z)
    fetches[5].wait()

    def w_across(condition, u, plane):
        for k in range(1, across):

            def copy():
                return remote(
                    w_unit(u, plane * across + x),
                    w_unit(u, plane * across + x),
                    wx_send.at[u, plane, k],
                    wx_recv.at[u, plane, across - k],
                    sp=beside(k),
                )

            @pl.when(condition)
            def _():
                copy().start()

            wx.append((condition, copy))

    def w_begin(t):
        for u in range(len(w_units)):
            w_line.up(z == t, u, z)
            w_line.down(depth - 1 - z == t, u, z)

    w_begin(0)
    prepare(0)
    for u in range(len(w_units)):
        w_across(always, u, z)
    for t in range(1, depth):
        for u in range(len(kv_units)):
            kv_line.step(t, u)
        w_begin(t)
    middle = (z > 0) & (z < depth - 1)
    for u in range(len(w_units)):
        w_line.step(1, u, middle, w_across)
    prepare(1)
    for k in range(1, across):
        remote(
            q_stage.at[0],
            q_all.at[:, pl.ds(k * rows, rows), :],
            qx_send.at[k],
            qx_recv.at[k],
            sp=me,
        ).wait_recv()

    scale = width ** (-0.5)
    wide_group = group * width

    def att_cols(k, g):
        side = lax.rem(x + k, across)
        start = (side * local_kv + g) * wide_group
        return pl.ds(pl.multiple_of(start, wide_group), wide_group)

    y_copies, pair_copies, fwd_copies = {}, {}, {}

    def spread_att(u):
        k, g = kv_units[u]
        block = att.at[mine, :, att_cols(k, g)]
        for j in range(1, ny):
            target = lax.rem(row_y + j, ny) * 2 + core
            copy = remote(block, block, y_send.at[j, u], y_recv.at[j, u], dp=target)
            copy.start()
            y_copies[j, u] = copy
        copy = remote(block, block, pair_send.at[u], pair_recv.at[u], dp=partner)
        copy.start()
        pair_copies[u] = copy

    def forward(u):
        for j in range(1, ny):
            source = lax.rem(row_y + ny - j, ny) * 2 + core
            y_copies[j, u].wait_recv()
            block = att.at[source, :, att_cols(*kv_units[u])]
            copy = remote(block, block, fwd_send.at[j, u], fwd_recv.at[j, u], dp=partner)
            copy.start()
            fwd_copies[j, u] = copy

    for g in range(local_kv):

        def one_head(i, carry):
            h = g * group + i
            scores = (
                lax.dot_general(
                    q_all[h], kv[2 * g], (((1,), (1,)), ((), ())), preferred_element_type=F32
                )
                * scale
            )
            exponent = jnp.exp(scores - jnp.max(scores, axis=-1, keepdims=True))
            weights = (exponent / jnp.sum(exponent, axis=-1, keepdims=True)).astype(BF16)
            out = jnp.dot(weights, kv[2 * g + 1], preferred_element_type=F32).astype(BF16)
            cols = pl.ds(pl.multiple_of((x * local + h) * width, width), width)
            att[mine, :, cols] = out[0:rows]
            cols = pl.ds(pl.multiple_of(h * width, width), width)
            for k in range(1, across):
                swap[k - 1, :, cols] = out[k * rows : (k + 1) * rows]
            return carry

        lax.fori_loop(0, group, one_head, 0)
        for k in range(1, across):
            ax[k, g] = remote(
                swap.at[k - 1, :, pl.ds(g * wide_group, wide_group)],
                att.at[mine, :, att_cols(0, g)],
                ax_send.at[k, g],
                ax_recv.at[across - k, g],
                sp=beside(k),
            )
            ax[k, g].start()
        spread_att(g)
        if g == 0:
            for u in range(len(w_units)):
                w_line.step(1, u, jnp.logical_not(middle), w_across)
    for t in range(2, depth - 1):
        for u in range(len(w_units)):
            w_line.step(t, u, True, w_across)
    for u in range(local_kv, len(kv_units)):
        k, g = kv_units[u]
        remote(
            swap.at[0, :, pl.ds(g * wide_group, wide_group)],
            att.at[mine, :, att_cols(k, g)],
            ax_send.at[k, g],
            ax_recv.at[k, g],
            sp=me,
        ).wait_recv()
        spread_att(u)
    for u in range(len(kv_units)):
        forward(u)
    for u in range(len(w_units)):
        w_line.step(depth - 1, u, True, w_across)
    for u in range(len(kv_units)):
        pair_copies[u].wait_recv()
        for j in range(1, ny):
            fwd_copies[j, u].wait_recv()

    back_copies = {}
    for j in range(halves):
        for u, (jj, _) in enumerate(w_units):
            if jj != j:
                continue
            for plane in range(depth):
                for k in range(1, across):
                    remote(
                        w_unit(u, plane * across + x),
                        w_unit(u, plane * across + lax.rem(x + k, across)),
                        wx_send.at[u, plane, k],
                        wx_recv.at[u, plane, k],
                        sp=me,
                    ).wait_recv()
        cols = slice(j * part_cols, (j + 1) * part_cols)
        result = jnp.dot(
            att[...].reshape(dp * rows, model), w_full[:, cols], preferred_element_type=F32
        ).astype(BF16)
        for s in range(dp):
            proj[s, :, cols] = result[s * rows : (s + 1) * rows]
        back[mine, :, cols] = proj[mine, :, cols]
        order = sorted(range(1, dp), key=lambda d: d % 2)
        for d in order:
            target = lax.rem(mine + d, dp)
            copy = remote(
                proj.at[target, :, cols],
                back.at[mine, :, cols],
                back_send.at[d, j],
                back_recv.at[d, j],
                dp=target,
            )
            copy.start()
            back_copies[d, j] = copy

    kv_line.drain()
    w_line.drain()
    for condition, copy in wx:

        @pl.when(condition)
        def _():
            copy().wait_send()

    for copies in (kvx, qx, ax):
        for copy in copies.values():
            copy.wait_send()
    fetches[6].wait()
    fetches[7].wait()
    for copies in (y_copies, pair_copies, fwd_copies):
        for copy in copies.values():
            copy.wait_send()
    for copy in back_copies.values():
        copy.wait()
    square = jnp.zeros((rows, 1), F32)
    for s in range(dp):
        cols = slice(s * w_cols, (s + 1) * w_cols)
        part = res_in[:, cols].astype(F32) + back[s].astype(F32)
        mixed_ref[:, cols] = part
        square = square + jnp.sum(part * part, axis=-1, keepdims=True)
    factor = lax.rsqrt(square / model + EPS)
    for s in range(dp):
        cols = slice(s * w_cols, (s + 1) * w_cols)
        normed_ref[:, cols] = (mixed_ref[:, cols] * factor * norm_in[:, cols]).astype(BF16)


class Experts:
    def __init__(self, n, capacity, routes, gates, middle, loads, out, *refs):
        (
            self.gate,
            self.up,
            self.down,
            self.tables,
            self.pick,
            self.high,
            self.low,
            self.column,
            self.asked,
            self.served,
            self.answer,
            self.given,
            self.acc,
            self.hidden,
            self.partial,
            self.incoming,
            self.hold,
            self.result,
            self.table_sem,
            self.column_send,
            self.column_recv,
            self.ask_send,
            self.ask_recv,
            self.give_send,
            self.give_recv,
            self.part_send,
            self.part_recv,
            self.out_sem,
        ) = refs
        self.mixed, self.normed = middle
        self.routes, self.gates = routes, gates
        self.loads, self.out = loads, out
        me = lax.axis_index("sp")
        self.columns = max(x for x in range(1, n + 1) if n % x == 0 and x * x <= n)
        self.depth = n // self.columns
        self.z, self.x = me // self.columns, me % self.columns
        self.upper = self.z // (self.depth // 2)
        self.way = 1 - 2 * self.upper
        self.inner = self.upper * (self.depth - 1) + self.way * self.z
        self.capacity = capacity
        self.rows, self.model = self.normed.shape
        self.width = self.model // CHUNKS
        self.share = 2 * capacity
        self.started = []

    def role(self, inner):
        return self.inner == inner

    def plane(self, r):
        place = (self.inner, 1 - self.inner, self.depth - 1, self.depth - 2)[r]
        return self.upper * (self.depth - 1) + self.way * place

    def remote(self, src, dst, send, recv, target):
        return pltpu.make_async_remote_copy(
            src_ref=src,
            dst_ref=dst,
            send_sem=send,
            recv_sem=recv,
            device_id={"sp": target},
            device_id_type=MESH,
        )

    def at(self, step):
        return (self.z + step) * self.columns + self.x

    def beside(self, k):
        return self.z * self.columns + (self.x + k) % self.columns

    def cols(self, c):
        return slice(c * self.width, (c + 1) * self.width)

    def send(self, make, inner=None):
        if inner is None:
            make().start()
        else:

            @pl.when(self.role(inner))
            def _():
                make().start()

        self.started.append((make, inner))

    def prepare(self, phase):
        planes = self.depth

        def table_copy(d):
            target = (self.z + d) % planes
            return self.remote(
                self.tables.at[self.z],
                self.tables.at[self.z],
                self.table_sem.at[0, d],
                self.table_sem.at[1, d],
                target * self.columns + self.x,
            )

        if phase == 0:
            rows = self.rows
            self.tables[self.z] = jnp.concatenate(
                [self.routes[...].astype(F32), self.gates[...], jnp.zeros((4, rows), F32)], axis=0
            )
            for d in range(1, planes):
                self.send(functools.partial(table_copy, d))
            return
        for d in range(1, planes):
            table_copy(d).wait_recv()
        for r in range(planes):
            choice, high, low = selection(
                self.tables[self.plane(r)],
                self.z * self.columns,
                self.x,
                self.columns,
                self.capacity,
            )
            self.pick[r] = choice
            self.high[r] = high
            self.low[r] = low

    def column_copy(self, kind, c):
        source, place, step = {
            "forth": (None, None, 1),
            "back": (None, 1, -1),
            1: (1, 2, 1),
            2: (2, 2, -1),
            3: (3, 3, -1),
        }[kind]
        cols = self.cols(c)
        src = self.normed.at[:, cols] if source is None else self.column.at[source - 1, :, cols]
        if place is None:
            place = 1 + 2 * self.inner
        index = ("forth", "back", 1, 2, 3).index(kind)
        return self.remote(
            src,
            self.column.at[place - 1, :, cols],
            self.column_send.at[index, c],
            self.column_recv.at[place - 1, c],
            self.at(step * self.way),
        )

    def column_arrive(self, r, c):
        cols = self.cols(c)
        self.remote(
            self.column.at[r - 1, :, cols],
            self.column.at[r - 1, :, cols],
            self.column_send.at[0, c],
            self.column_recv.at[r - 1, c],
            self.at(0),
        ).wait_recv()

    def ask_copy(self, r, c, k):
        cols = self.cols(c)
        return self.remote(
            self.asked.at[r, pl.ds((k - 1) * self.share, self.share), cols],
            self.served.at[r, pl.ds((self.columns - k) * self.share, self.share), cols],
            self.ask_send.at[r, c, k],
            self.ask_recv.at[r, c, self.columns - k],
            self.beside(k),
        )

    def give_copy(self, r, c, k):
        cols = self.cols(c)
        return self.remote(
            self.given.at[r, pl.ds((k - 1) * self.share, self.share), cols],
            self.answer.at[r, pl.ds((self.columns - k) * self.share, self.share), cols],
            self.give_send.at[r, c, k],
            self.give_recv.at[r, c, self.columns - k],
            self.beside(k),
        )

    def ask(self, r, c, inner=None):
        def body():
            cols = self.cols(c)
            if r > 0:
                self.column_arrive(r, c)
            if r > 0 and inner != 0:

                @pl.when(self.role(1))
                def _():
                    self.column_copy(r, c).start()

            lines = self.normed[:, cols] if r == 0 else self.column[r - 1, :, cols]
            chosen = jnp.dot(self.pick[r], lines, preferred_element_type=F32).astype(BF16)
            self.served[r, 0 : self.share, cols] = chosen[0 : self.share]
            for k in range(1, self.columns):
                part = slice((k - 1) * self.share, k * self.share)
                self.asked[r, part, cols] = chosen[k * self.share : (k + 1) * self.share]
                self.ask_copy(r, c, k).start()

        if inner is None:
            body()
        else:
            pl.when(self.role(inner))(body)

    def serve_up(self, r, h):
        for c in range(h * CHUNKS // 2, (h + 1) * CHUNKS // 2):
            for k in range(1, self.columns):
                self.ask_copy(r, c, self.columns - k).wait_recv()
        if r == 0 and h == 0:
            self.loads[0].wait()
            self.loads[1].wait()
        deep = slice(h * self.model // 2, (h + 1) * self.model // 2)
        acc = self.acc

        def up_tile(t, carry):
            cols = pl.ds(pl.multiple_of(t * TILE, TILE), TILE)
            lines = self.served[r, :, deep]
            gate = jnp.dot(lines, self.gate[deep, cols], preferred_element_type=F32)
            up = jnp.dot(lines, self.up[deep, cols], preferred_element_type=F32)
            if h == 0:
                acc[0, :, cols] = gate
                acc[1, :, cols] = up
            else:
                gate = gate + acc[0, :, cols]
                up = up + acc[1, :, cols]
                self.hidden[:, cols] = (gate / (1.0 + jnp.exp(-gate)) * up).astype(BF16)
            return carry

        lax.fori_loop(0, self.gate.shape[1] // TILE, up_tile, 0)

    def serve_down(self, r, c):
        if r == 0 and c == 0:
            self.loads[2].wait()

        def down_tile(t, carry):
            cols = pl.ds(pl.multiple_of(c * self.width + t * TILE, TILE), TILE)
            lines = jnp.dot(
                self.hidden[...], self.down[:, cols], preferred_element_type=F32
            ).astype(BF16)
            self.answer[r, 0 : self.share, cols] = lines[0 : self.share]
            self.given[r, :, cols] = lines[self.share :]
            return carry

        lax.fori_loop(0, self.width // TILE, down_tile, 0)
        for k in range(1, self.columns):
            self.give_copy(r, c, k).start()

    def combine(self, r, c):
        for k in range(1, self.columns):
            self.give_copy(r, c, self.columns - k).wait_recv()
        lines = self.answer[r, :, self.cols(c)]
        return jnp.dot(self.high[r], lines, preferred_element_type=F32) + jnp.dot(
            self.low[r], lines, preferred_element_type=F32
        )

    def part_copy(self, slot, place, step, c):
        cols = self.cols(c)
        return self.remote(
            self.partial.at[slot, :, cols],
            self.incoming.at[place, :, cols],
            self.part_send.at[slot, c],
            self.part_recv.at[place, c],
            self.at(step * self.way),
        )

    def part_arrive(self, place, c):
        cols = self.cols(c)
        self.remote(
            self.partial.at[0, :, cols],
            self.incoming.at[place, :, cols],
            self.part_send.at[0, c],
            self.part_recv.at[place, c],
            self.at(0),
        ).wait_recv()
        return self.incoming[place, :, cols].astype(F32)

    def merge(self, inner, r, c, slot, place, step, feed=None):
        @pl.when(self.role(inner))
        def _():
            total = self.combine(r, c)
            if feed is not None:
                total = total + self.part_arrive(feed, c)
            self.partial[slot, :, self.cols(c)] = total.astype(BF16)
            self.part_copy(slot, place, step, c).start()

    def own(self, c):
        cols = self.cols(c)
        self.hold[:, cols] = self.mixed[:, cols] + self.combine(0, c)

    def finish(self, inner, places):
        @pl.when(self.role(inner))
        def _():
            for c in range(CHUNKS):
                cols = self.cols(c)
                total = self.hold[:, cols]
                for place in places:
                    total = total + self.part_arrive(place, c)
                self.result[:, cols] = total.astype(BF16)
                self.out_copy(c).start()

    def out_copy(self, c):
        cols = self.cols(c)
        return pltpu.make_async_copy(
            self.result.at[:, cols], self.out.at[:, cols], self.out_sem.at[c]
        )

    def run(self):
        chunks = range(CHUNKS)
        half = CHUNKS // 2

        def forth(cs):
            for c in cs:
                self.column_copy("forth", c).start()

        for c in chunks:

            @pl.when(self.role(1))
            def _():
                self.column_copy("back", c).start()

            if c < half:
                self.column_copy("forth", c).start()
            else:

                @pl.when(self.role(0))
                def _():
                    self.column_copy("forth", c).start()

        for c in chunks:
            self.ask(0, c)
        self.ask(1, 0)
        self.serve_up(0, 0)
        self.ask(1, 1)
        self.serve_up(0, 1)
        self.ask(1, 2)
        self.ask(2, 0, 1)
        self.serve_up(1, 0)
        self.ask(1, 3)

        @pl.when(self.role(1))
        def _():
            forth(range(half, CHUNKS))

        self.ask(2, 1, 1)
        for c in chunks:
            self.serve_down(0, c)
        self.ask(2, 0, 0)
        self.ask(2, 2, 1)
        self.serve_up(1, 1)
        self.serve_down(1, 0)
        self.serve_down(1, 1)
        self.ask(2, 1, 0)
        self.ask(2, 3, 1)
        self.serve_down(1, 2)
        self.serve_down(1, 3)
        self.ask(3, 0, 1)
        self.ask(3, 1, 1)
        self.ask(2, 2, 0)
        self.merge(0, 1, 0, 0, 0, 1)
        self.merge(0, 1, 1, 0, 0, 1)
        self.serve_up(2, 0)
        self.ask(2, 3, 0)
        self.ask(3, 2, 1)
        self.merge(0, 1, 2, 0, 0, 1)
        self.merge(0, 1, 3, 0, 0, 1)
        self.ask(3, 0, 0)
        self.ask(3, 3, 1)
        self.serve_up(2, 1)
        self.serve_down(2, 0)
        self.serve_down(2, 1)
        self.ask(3, 1, 0)
        self.serve_down(2, 2)
        self.serve_down(2, 3)
        self.ask(3, 2, 0)
        self.merge(0, 2, 0, 1, 1, 1)
        self.merge(0, 2, 1, 1, 1, 1)
        self.serve_up(3, 0)
        self.ask(3, 3, 0)
        self.merge(0, 2, 2, 1, 1, 1)
        self.merge(0, 2, 3, 1, 1, 1)
        self.own(0)
        self.own(1)
        self.serve_up(3, 1)
        for c in chunks:
            self.serve_down(3, c)
        for c in chunks:
            self.merge(0, 3, c, 2, 2, 1)
        self.own(2)
        self.own(3)

        def far(c):
            self.merge(1, 2, c, 1, 3, 1, 1)

        def near(c):
            self.merge(1, 1, c, 3, 5, -1, 3)

        for c in chunks:
            far(c)
            if c > 0:
                near(c - 1)
        near(CHUNKS - 1)
        for c in chunks:
            self.merge(1, 3, c, 2, 4, 1, 2)
        self.finish(0, (5,))
        self.finish(1, (0, 4))
        self.drain()

    def drain(self):
        for make, _ in self.started:
            make().wait_send()
        for c in range(CHUNKS):
            self.column_copy("forth", c).wait_send()

            @pl.when(self.role(1))
            def _():
                self.column_copy("back", c).wait_send()
                for r in (1, 2, 3):
                    self.column_copy(r, c).wait_send()
                for slot, place, step in ((1, 3, 1), (2, 4, 1), (3, 5, -1)):
                    self.part_copy(slot, place, step, c).wait_send()

            @pl.when(self.role(0))
            def _():
                for slot in range(3):
                    self.part_copy(slot, slot, 1, c).wait_send()

            for r in range(self.depth):
                for k in range(1, self.columns):
                    self.ask_copy(r, c, k).wait_send()
                    self.give_copy(r, c, k).wait_send()
            self.out_copy(c).wait()


def layer_kernel(n, dp, capacity, *refs):
    inputs, refs = refs[:10], refs[10:]
    weights, out_ref, refs = refs[:3], refs[3], refs[4:]
    middle, refs = refs[:2], refs[2:]
    attention, refs = refs[:37], refs[37:]
    load_sem, stores = refs[0], refs[1:4]
    loads = [
        pltpu.make_async_copy(src.at[0], dst, load_sem.at[i])
        for i, (src, dst) in enumerate(zip(weights, stores))
    ]

    def start_loads():
        for load in loads:
            load.start()

    experts = Experts(n, capacity, *inputs[8:], middle, loads, out_ref, *refs[1:])
    attention_part(n, dp, start_loads, *inputs[:8], *middle, experts.prepare, *attention)
    experts.run()


def on_device(
    n,
    dp,
    queries,
    key_rows,
    values,
    query_gain,
    key_gain,
    out_weight,
    residual,
    norm_gain,
    expert_gate,
    expert_up,
    expert_down,
    routes,
    route_weight,
):
    _, rows, heads, width = queries.shape
    kv_heads = key_rows.shape[2]
    model = heads * width
    length = rows * n
    experts = expert_gate.shape[0] * n
    capacity = max(2, 4 * (rows // 2) // experts)
    across = max(x for x in range(1, n + 1) if n % x == 0 and x * x <= n)
    depth = n // across
    local_kv, local = kv_heads // across, heads // across
    units = across * local_kv
    slots = 2 * across * capacity
    aside = 2 * (across - 1) * capacity
    w_rows, w_cols = out_weight.shape
    dma = pltpu.SemaphoreType.DMA
    ny = dp // 2
    ff = expert_gate.shape[2]
    attention_scratch = [
        pltpu.VMEM((rows, heads, width), BF16),
        pltpu.VMEM((rows, kv_heads, width), BF16),
        pltpu.VMEM((rows, kv_heads, width), BF16),
        pltpu.VMEM((rows, heads, width), F32),
        pltpu.VMEM((across, 2 * local_kv, rows, width), BF16),
        pltpu.VMEM((across - 1, local, rows, width), BF16),
        pltpu.VMEM((local, across * rows, width), BF16),
        pltpu.VMEM((2 * local_kv, length, width), BF16),
        pltpu.VMEM((w_rows * n, w_cols), BF16),
        pltpu.VMEM((across - 1, rows, local * width), BF16),
        pltpu.VMEM((dp, rows, model), BF16),
        pltpu.VMEM((dp, rows, w_cols), BF16),
        pltpu.VMEM((dp, rows, w_cols), BF16),
        pltpu.VMEM((rows, model), BF16),
        pltpu.VMEM((2, 1, width), F32),
        pltpu.VMEM((1, model), F32),
        dma((8,)),
        dma((across, local_kv)),
        dma((across, local_kv)),
        dma((units, depth, 2)),
        dma((units, depth)),
        dma((across,)),
        dma((across,)),
        dma((4, depth, across)),
        dma((4, depth, across)),
        dma((4, depth, 2)),
        dma((4, depth)),
        dma((across, local_kv)),
        dma((across, local_kv)),
        dma((ny, units)),
        dma((ny, units)),
        dma((units,)),
        dma((units,)),
        dma((ny, units)),
        dma((ny, units)),
        dma((dp, 2)),
        dma((dp, 2)),
    ]
    result = pl.pallas_call(
        functools.partial(layer_kernel, n, dp, capacity),
        out_shape=jax.ShapeDtypeStruct((rows, model), BF16),
        in_specs=[ANY] * 8 + [VMEM] * 2 + [ANY] * 3,
        out_specs=ANY,
        scratch_shapes=[
            pltpu.VMEM((rows, model), F32),
            pltpu.VMEM((rows, model), BF16),
            *attention_scratch,
            dma((3,)),
            pltpu.VMEM((model, ff), BF16),
            pltpu.VMEM((model, ff), BF16),
            pltpu.VMEM((ff, model), BF16),
            pltpu.VMEM((depth, 8, rows), F32),
            pltpu.VMEM((depth, slots, rows), BF16),
            pltpu.VMEM((depth, rows, slots), BF16),
            pltpu.VMEM((depth, rows, slots), BF16),
            pltpu.VMEM((depth - 1, rows, model), BF16),
            pltpu.VMEM((depth, aside, model), BF16),
            pltpu.VMEM((depth, slots, model), BF16),
            pltpu.VMEM((depth, slots, model), BF16),
            pltpu.VMEM((depth, aside, model), BF16),
            pltpu.VMEM((2, slots, ff), F32),
            pltpu.VMEM((slots, ff), BF16),
            pltpu.VMEM((4, rows, model), BF16),
            pltpu.VMEM((6, rows, model), BF16),
            pltpu.VMEM((rows, model), F32),
            pltpu.VMEM((rows, model), BF16),
            dma((2, depth)),
            dma((5, CHUNKS)),
            dma((depth - 1, CHUNKS)),
            dma((depth, CHUNKS, across)),
            dma((depth, CHUNKS, across)),
            dma((depth, CHUNKS, across)),
            dma((depth, CHUNKS, across)),
            dma((4, CHUNKS)),
            dma((6, CHUNKS)),
            dma((CHUNKS,)),
        ],
        compiler_params=pltpu.CompilerParams(
            collective_id=0, has_side_effects=True, vmem_limit_bytes=56 * 1024 * 1024
        ),
        name="layer",
    )(
        queries[0],
        key_rows[0],
        values[0],
        query_gain[None],
        key_gain[None],
        out_weight,
        residual[0],
        norm_gain[None],
        routes[0].T,
        route_weight[0].T,
        expert_gate,
        expert_up,
        expert_down,
    )
    return result[None]


def solution(mesh):
    in_specs = (
        P("dp", "sp", None, None),
        P("dp", "sp", None, None),
        P("dp", "sp", None, None),
        P(),
        P(),
        P("sp", "dp"),
        P("dp", "sp", None),
        P(),
        P("sp", None, None),
        P("sp", None, None),
        P("sp", None, None),
        P("dp", "sp", None),
        P("dp", "sp", None),
    )
    out_specs = P("dp", "sp", None)
    return jax.shard_map(
        functools.partial(on_device, mesh.shape["sp"], mesh.shape["dp"]),
        mesh=mesh,
        in_specs=in_specs,
        out_specs=out_specs,
        check_vma=False,
    )
```

```python
import functools
import math

import jax
import jax.numpy as jnp
from jax import lax
from jax.experimental import pallas as pl
from jax.experimental.pallas import tpu as pltpu
from jax.sharding import PartitionSpec as P

GRID_W = 64
EPS = 1e-06
CHUNKS = 4
TILE = 256
THETA = 10000.0
MESH = pl.DeviceIdType.MESH
VMEM = pl.BlockSpec(memory_space=pltpu.VMEM)
ANY = pl.BlockSpec(memory_space=pl.ANY)
F32 = jnp.float32
BF16 = jnp.bfloat16


def rotation_tables(start, rows, width):
    quarter = width // 4
    lane = lax.broadcasted_iota(jnp.int32, (rows, width), 1)
    position = start + lax.broadcasted_iota(jnp.int32, (rows, width), 0)
    place = jnp.where(lane < 2 * quarter, position // GRID_W, position % GRID_W)
    part = lane % (2 * quarter)
    power = (part % quarter).astype(F32) * (-math.log(THETA) / quarter)
    angles = place.astype(F32) * jnp.exp(power)
    sign = jnp.where(part < quarter, -1.0, 1.0).astype(F32)
    return jnp.cos(angles), jnp.sin(angles) * sign


def turn(rows, gain, cosine, sine):
    width = rows.shape[-1]
    quarter = width // 4
    a = rows.astype(F32)
    a = a * lax.rsqrt(jnp.mean(a * a, axis=-1, keepdims=True) + EPS) * gain
    lane = lax.broadcasted_iota(jnp.int32, a.shape, 1) % (2 * quarter)
    partner = jnp.where(
        lane < quarter, pltpu.roll(a, width - quarter, 1), pltpu.roll(a, quarter, 1)
    )
    return (a * cosine + partner * sine).astype(BF16)


class Line:
    def __init__(self, depth, width, block, send, recv):
        self.depth, self.width, self.block = depth, width, block
        self.send, self.recv = send, recv
        me = lax.axis_index("sp")
        self.z, self.x = me // width, me % width

    def copy(self, unit, plane, way, target):
        return pltpu.make_async_remote_copy(
            src_ref=self.block(unit, plane * self.width + self.x),
            dst_ref=self.block(unit, plane * self.width + self.x),
            send_sem=self.send.at[way],
            recv_sem=self.recv.at[unit, plane],
            device_id={"sp": target * self.width + self.x},
            device_id_type=MESH,
        )

    def start(self, condition, unit, plane, way, target):
        @pl.when(condition)
        def _():
            self.copy(unit, plane, way, target).start()

    def up(self, condition, unit, plane):
        self.start(condition & (self.z < self.depth - 1), unit, plane, 0, self.z + 1)

    def down(self, condition, unit, plane):
        self.start(condition & (self.z > 0), unit, plane, 1, self.z - 1)

    def arrive(self, condition, unit, plane):
        @pl.when(condition)
        def _():
            self.copy(unit, plane, 0, plane).wait_recv()

    def step(self, t, unit, condition=True, then=None):
        below = (self.z - t >= 0) & condition
        above = (self.z + t < self.depth) & condition
        self.arrive(below, unit, self.z - t)
        self.up(below, unit, self.z - t)
        if then is not None:
            then(below, unit, self.z - t)
        self.arrive(above, unit, self.z + t)
        self.down(above, unit, self.z + t)
        if then is not None:
            then(above, unit, self.z + t)

    def drain(self, planes):
        for way in range(2):
            for count in range(1, self.depth):
                z = count - 1 if way == 0 else self.depth - count

                @pl.when(self.z == z)
                def _():
                    pltpu.make_async_remote_copy(
                        src_ref=planes(count),
                        dst_ref=planes(count),
                        send_sem=self.send.at[way],
                        recv_sem=self.recv.at[0, 0],
                        device_id={"sp": self.z * self.width + self.x},
                        device_id_type=MESH,
                    ).wait_send()


def selection(table, first_expert, column, columns, capacity):
    rows = table.shape[1]
    few = rows // 2
    slots = columns * 2 * capacity
    slot = lax.broadcasted_iota(jnp.int32, (slots, rows), 0)
    row = lax.broadcasted_iota(jnp.int32, (slots, rows), 1)
    side = (column + slot // (2 * capacity)) % columns
    expert = (first_expert + side).astype(F32)
    same = (slot // capacity) % 2 == row // few
    first = (table[0:1, :] == expert) & same
    second = (table[1:2, :] == expert) & same
    named = jnp.where(first | second, 1.0, 0.0).astype(BF16)
    before = lax.broadcasted_iota(jnp.int32, (rows, rows), 0)
    after = lax.broadcasted_iota(jnp.int32, (rows, rows), 1)
    earlier = jnp.where(before < after, 1.0, 0.0).astype(BF16)
    rank = jnp.dot(named, earlier, preferred_element_type=F32)
    here = rank == (slot % capacity).astype(F32)
    choice = jnp.where((first | second) & here, 1.0, 0.0)
    weight = jnp.where(first & here, table[2:3, :], 0.0)
    weight = weight + jnp.where(second & here, table[3:4, :], 0.0)
    weight = weight.T
    high = weight.astype(BF16)
    low = (weight - high.astype(F32)).astype(BF16)
    return choice.astype(BF16), high, low


def attention_part(
    n,
    dp,
    start_loads,
    q_ref,
    k_ref,
    v_ref,
    qg_ref,
    kg_ref,
    w_ref,
    res_ref,
    ng_ref,
    mixed_ref,
    normed_ref,
    prepare,
    q_in,
    k_in,
    v_in,
    wide,
    stage,
    q_stage,
    q_all,
    kv,
    w_full,
    swap,
    att,
    proj,
    back,
    res_in,
    gains,
    norm_in,
    in_sem,
    kvx_send,
    kvx_recv,
    kvz_send,
    kvz_recv,
    qx_send,
    qx_recv,
    wx_send,
    wx_recv,
    wz_send,
    wz_recv,
    ax_send,
    ax_recv,
    y_send,
    y_recv,
    pair_sem,
    fwd_sem,
    back_sem,
):
    me = lax.axis_index("sp")
    mine = lax.axis_index("dp")
    rows, heads, width = q_ref.shape
    kv_heads = k_ref.shape[1]
    group = heads // kv_heads
    model = heads * width
    across = stage.shape[0]
    depth = n // across
    local_kv = kv_heads // across
    local = heads // across
    z, x = me // across, me % across
    always = me >= 0
    ny = dp // 2
    core = mine % 2
    row_y = mine // 2
    partner = row_y * 2 + 1 - core
    w_rows, w_cols = w_ref.shape

    def span(start, size):
        return pl.ds(pl.multiple_of(start * size, size), size)

    fetches = [
        pltpu.make_async_copy(src, dst, in_sem.at[i])
        for i, (src, dst) in enumerate(
            (
                (k_ref, k_in),
                (v_ref, v_in),
                (kg_ref, gains.at[0]),
                (q_ref, q_in),
                (qg_ref, gains.at[1]),
                (w_ref, w_full.at[span(me, w_rows)]),
                (res_ref, res_in),
                (ng_ref, norm_in),
            )
        )
    ]
    for fetch in fetches:
        fetch.start()
    barrier = pltpu.get_barrier_semaphore()
    for d in range(1, n):
        pl.semaphore_signal(
            barrier, inc=1, device_id={"sp": lax.rem(me + d, n)}, device_id_type=MESH
        )
    for d in range(1, dp):
        pl.semaphore_signal(
            barrier, inc=1, device_id={"dp": lax.rem(mine + d, dp)}, device_id_type=MESH
        )

    cosine, sine = rotation_tables(me * rows, rows, width)
    my_rows = span(me, rows)
    for fetch in fetches[:3]:
        fetch.wait()
    for part, source in ((0, k_in), (1, v_in)):
        wide[:, 0:kv_heads, :] = source[...].astype(F32)
        for g in range(kv_heads):
            lines = wide[:, g, :]
            slot = 2 * (g % local_kv) + part
            if part == 0:
                lines = turn(lines, gains[0], cosine, sine)
            stage[g // local_kv, slot] = lines.astype(BF16)
    for c in range(2 * local_kv):
        kv[c, my_rows, :] = stage[x, c]
    pl.semaphore_wait(barrier, n - 1 + dp - 1)

    def remote(src, dst, send, recv, **device):
        return pltpu.make_async_remote_copy(
            src_ref=src,
            dst_ref=dst,
            send_sem=send,
            recv_sem=recv,
            device_id=device,
            device_id_type=MESH,
        )

    def beside(k):
        return z * across + lax.rem(x + k, across)

    def kv_block(g, sp):
        return kv.at[pl.ds(2 * g, 2), span(sp, rows), :]

    kv_units = [(k, g) for g in range(local_kv) for k in range(across)]
    own_units = [u for u, (k, _) in enumerate(kv_units) if k == 0]

    def kv_unit(u, sp):
        k, g = kv_units[u]
        return kv_block(g, sp - sp % across + lax.rem(sp % across + k, across))

    halves = 2
    w_units = [(j, k) for j in range(halves) for k in range(2)]
    part_rows, part_cols = w_rows // 2, w_cols // halves

    def w_unit(u, sp):
        j, k = w_units[u]
        start = pl.multiple_of(sp * w_rows + k * part_rows, part_rows)
        return w_full.at[pl.ds(start, part_rows), pl.ds(j * part_cols, part_cols)]

    kv_line = Line(depth, across, kv_unit, kvz_send, kvz_recv)
    w_line = Line(depth, across, w_unit, wz_send, wz_recv)
    kvx, qx, ax = {}, {}, {}
    for g in range(local_kv):
        for k in range(1, across):
            kvx[k, g] = remote(
                stage.at[lax.rem(x + k, across), pl.ds(2 * g, 2)],
                kv_block(g, me),
                kvx_send.at[0],
                kvx_recv.at[across - k - 1, g],
                sp=beside(k),
            )
            kvx[k, g].start()
        kv_line.up(always, own_units[g], z)
        kv_line.down(always, own_units[g], z)

    start_loads()
    fetches[3].wait()
    fetches[4].wait()
    for h in range(0, heads, 8):
        wide[:, h : h + 8, :] = q_in[:, h : h + 8, :].astype(F32)
    for k in list(range(1, across)) + [0]:
        first = lax.rem(x + k, across) * local

        def turn_head(i, carry):
            lines = turn(wide[:, pl.ds(first + i, 1), :].reshape(rows, width), gains[1], cosine, sine)
            if k == 0:
                q_all[i, 0:rows] = lines
            else:
                q_stage[k - 1, i] = lines
            return carry

        lax.fori_loop(0, local, turn_head, 0)
        if k > 0:
            qx[k] = remote(
                q_stage.at[k - 1],
                q_all.at[:, pl.ds((across - k) * rows, rows), :],
                qx_send.at[0],
                qx_recv.at[0],
                sp=beside(k),
            )
            qx[k].start()
        if k == across - 1:
            for u, (kk, g) in enumerate(kv_units):
                if kk == 0:
                    continue
                remote(
                    stage.at[0, pl.ds(2 * g, 2)],
                    kv_block(g, beside(kk)),
                    kvx_send.at[0],
                    kvx_recv.at[kk - 1, g],
                    sp=me,
                ).wait_recv()
                kv_line.up(always, u, z)
                kv_line.down(always, u, z)
    fetches[5].wait()

    def w_across(condition, u, plane):
        for k in range(1, across):

            @pl.when(condition)
            def _():
                remote(
                    w_unit(u, plane * across + x),
                    w_unit(u, plane * across + x),
                    wx_send.at[0],
                    wx_recv.at[w_units[u][0]],
                    sp=beside(k),
                ).start()

    def w_begin(t):
        for u in range(len(w_units)):
            w_line.up(z == t, u, z)
            w_line.down(depth - 1 - z == t, u, z)

    w_begin(0)
    prepare(0)
    for u in range(len(w_units)):
        w_across(always, u, z)
    for t in range(1, depth - 1):
        for u in range(len(kv_units)):
            kv_line.step(t, u)
        w_begin(t)
    middle = (z > 0) & (z < depth - 1)
    prepare(1)
    remote(
        q_stage,
        q_all.at[:, pl.ds(rows, (across - 1) * rows), :],
        qx_send.at[0],
        qx_recv.at[0],
        sp=me,
    ).wait_recv()

    scale = width ** (-0.5)
    wide_group = group * width

    def att_cols(k, g):
        side = lax.rem(x + k, across)
        start = (side * local_kv + g) * wide_group
        return pl.ds(pl.multiple_of(start, wide_group), wide_group)

    def spread_att(u):
        k, g = kv_units[u]
        block = att.at[mine, :, att_cols(k, g)]
        for j in range(1, ny):
            target = lax.rem(row_y + j, ny) * 2 + core
            remote(block, block, y_send.at[0], y_recv.at[j - 1, u], dp=target).start()
        remote(block, block, pair_sem.at[0], pair_sem.at[1], dp=partner).start()

    def forward(u):
        for j in range(1, ny):
            source = lax.rem(row_y + ny - j, ny) * 2 + core
            remote(
                att.at[mine, :, att_cols(*kv_units[u])],
                att.at[mine, :, att_cols(*kv_units[u])],
                y_send.at[0],
                y_recv.at[j - 1, u],
                dp=mine,
            ).wait_recv()
            block = att.at[source, :, att_cols(*kv_units[u])]
            remote(block, block, fwd_sem.at[0], fwd_sem.at[1], dp=partner).start()

    for g in range(local_kv):
        for u, (_, gg) in enumerate(kv_units):
            if gg == g:
                kv_line.step(depth - 1, u)
        if g == local_kv - 1:
            for u in range(len(w_units)):
                w_line.step(1, u, middle, w_across)

        def one_head(i, carry):
            h = g * group + i
            scores = (
                lax.dot_general(
                    q_all[h], kv[2 * g], (((1,), (1,)), ((), ())), preferred_element_type=F32
                )
                * scale
            )
            exponent = jnp.exp(scores - jnp.max(scores, axis=-1, keepdims=True))
            weights = (exponent / jnp.sum(exponent, axis=-1, keepdims=True)).astype(BF16)
            out = jnp.dot(weights, kv[2 * g + 1], preferred_element_type=F32).astype(BF16)
            cols = pl.ds(pl.multiple_of((x * local + h) * width, width), width)
            att[mine, :, cols] = out[0:rows]
            cols = pl.ds(pl.multiple_of(h * width, width), width)
            for k in range(1, across):
                swap[k - 1, :, cols] = out[k * rows : (k + 1) * rows]
            return carry

        lax.fori_loop(0, group, one_head, 0)
        for k in range(1, across):
            ax[k, g] = remote(
                swap.at[k - 1, :, pl.ds(g * wide_group, wide_group)],
                att.at[mine, :, att_cols(0, g)],
                ax_send.at[0],
                ax_recv.at[across - k - 1, g],
                sp=beside(k),
            )
            ax[k, g].start()
        spread_att(own_units[g])
    for t in range(2, depth - 1):
        for u in range(len(w_units)):
            w_line.step(t, u, middle, w_across)
    for u in range(len(w_units)):
        w_line.step(1, u, jnp.logical_not(middle), w_across)
    for u, (k, g) in enumerate(kv_units):
        if k == 0:
            continue
        remote(
            swap.at[0, :, pl.ds(g * wide_group, wide_group)],
            att.at[mine, :, att_cols(k, g)],
            ax_send.at[0],
            ax_recv.at[k - 1, g],
            sp=me,
        ).wait_recv()
        spread_att(u)
    for t in range(2, depth - 1):
        for u in range(len(w_units)):
            w_line.step(t, u, jnp.logical_not(middle), w_across)
    order = own_units + [u for u in range(len(kv_units)) if u not in own_units]
    for i in range(max(len(order), len(w_units))):
        if i < len(w_units):
            w_line.step(depth - 1, i, True, w_across)
        if i < len(order):
            forward(order[i])
    if ny > 1:
        remote(
            att.at[pl.ds(0, ny - 1)],
            att.at[pl.ds(0, ny - 1)],
            fwd_sem.at[0],
            fwd_sem.at[1],
            dp=mine,
        ).wait_recv()
    remote(att.at[mine], att.at[mine], pair_sem.at[0], pair_sem.at[1], dp=mine).wait_recv()

    for j in range(halves):
        cols = slice(j * part_cols, (j + 1) * part_cols)
        block = w_full.at[pl.ds(0, depth * (across - 1) * w_rows), cols]
        remote(block, block, wx_send.at[0], wx_recv.at[j], sp=me).wait_recv()
        result = jnp.dot(
            att[...].reshape(dp * rows, model), w_full[:, cols], preferred_element_type=F32
        ).astype(BF16)
        for s in range(dp):
            proj[s, :, cols] = result[s * rows : (s + 1) * rows]
        back[mine, :, cols] = proj[mine, :, cols]
        order = sorted(range(1, dp), key=lambda d: d % 2)
        for d in order:
            target = lax.rem(mine + d, dp)
            remote(
                proj.at[target, :, cols],
                back.at[mine, :, cols],
                back_sem.at[0],
                back_sem.at[1],
                dp=target,
            ).start()

    fetches[6].wait()
    fetches[7].wait()
    block = back.at[pl.ds(0, dp - 1)]
    remote(block, block, back_sem.at[0], back_sem.at[1], dp=mine).wait_recv()
    square = jnp.zeros((rows, 1), F32)
    for s in range(dp):
        cols = slice(s * w_cols, (s + 1) * w_cols)
        part = res_in[:, cols].astype(F32) + back[s].astype(F32)
        mixed_ref[:, cols] = part
        square = square + jnp.sum(part * part, axis=-1, keepdims=True)
    factor = lax.rsqrt(square / model + EPS)
    for s in range(dp):
        cols = slice(s * w_cols, (s + 1) * w_cols)
        normed_ref[:, cols] = (mixed_ref[:, cols] * factor * norm_in[:, cols]).astype(BF16)

    def drain():
        kv_line.drain(lambda count: kv.at[:, pl.ds(0, count * across * rows), :])
        w_line.drain(lambda count: w_full.at[pl.ds(0, count * w_rows)])
        block = w_full.at[pl.ds(0, depth * (across - 1) * w_rows)]
        whole = [
            (block, wx_send.at[0]),
            (stage.at[pl.ds(0, across - 1)], kvx_send.at[0]),
            (q_stage, qx_send.at[0]),
            (swap, ax_send.at[0]),
            (att.at[mine], pair_sem.at[0]),
            (proj.at[pl.ds(0, dp - 1)], back_sem.at[0]),
        ]
        if ny > 1:
            whole.append((att.at[pl.ds(0, ny - 1)], y_send.at[0]))
            whole.append((att.at[pl.ds(0, ny - 1)], fwd_sem.at[0]))
        for block, sem in whole:
            remote(block, block, sem, back_sem.at[1], sp=me).wait_send()

    return drain


class Experts:
    def __init__(self, n, capacity, routes, gates, middle, loads, out, *refs):
        (
            self.gate,
            self.up,
            self.down,
            self.tables,
            self.pick,
            self.high,
            self.low,
            self.column,
            self.asked,
            self.served,
            self.answer,
            self.given,
            self.hidden,
            self.partial,
            self.incoming,
            self.hold,
            self.result,
            self.table_sem,
            self.column_send,
            self.column_recv,
            self.ask_send,
            self.ask_recv,
            self.give_send,
            self.give_recv,
            self.part_send,
            self.part_recv,
            self.out_sem,
        ) = refs
        self.mixed, self.normed = middle
        self.routes, self.gates = routes, gates
        self.loads, self.out = loads, out
        me = lax.axis_index("sp")
        self.columns = max(x for x in range(1, n + 1) if n % x == 0 and x * x <= n)
        self.depth = n // self.columns
        self.z, self.x = me // self.columns, me % self.columns
        self.upper = self.z // (self.depth // 2)
        self.way = 1 - 2 * self.upper
        self.inner = self.upper * (self.depth - 1) + self.way * self.z
        self.capacity = capacity
        self.rows, self.model = self.normed.shape
        self.width = self.model // CHUNKS
        self.share = 2 * capacity

    def role(self, inner):
        return self.inner == inner

    def plane(self, r):
        place = (self.inner, 1 - self.inner, self.depth - 1, self.depth - 2)[r]
        return self.upper * (self.depth - 1) + self.way * place

    def remote(self, src, dst, send, recv, target):
        return pltpu.make_async_remote_copy(
            src_ref=src,
            dst_ref=dst,
            send_sem=send,
            recv_sem=recv,
            device_id={"sp": target},
            device_id_type=MESH,
        )

    def at(self, step):
        return (self.z + step) * self.columns + self.x

    def beside(self, k):
        return self.z * self.columns + (self.x + k) % self.columns

    def cols(self, c):
        return slice(c * self.width, (c + 1) * self.width)

    def tables_all(self):
        block = self.tables.at[pl.ds(0, self.depth - 1)]
        return self.remote(block, block, self.table_sem.at[0], self.table_sem.at[1], self.at(0))

    def prepare(self, phase):
        planes = self.depth

        def table_copy(d):
            target = (self.z + d) % planes
            return self.remote(
                self.tables.at[self.z],
                self.tables.at[self.z],
                self.table_sem.at[0],
                self.table_sem.at[1],
                target * self.columns + self.x,
            )

        if phase == 0:
            rows = self.rows
            self.tables[self.z] = jnp.concatenate(
                [self.routes[...].astype(F32), self.gates[...], jnp.zeros((4, rows), F32)], axis=0
            )
            for d in range(1, planes):
                table_copy(d).start()
            return
        self.tables_all().wait_recv()
        for r in range(planes):
            choice, high, low = selection(
                self.tables[self.plane(r)],
                self.z * self.columns,
                self.x,
                self.columns,
                self.capacity,
            )
            self.pick[r] = choice
            self.high[r] = high
            self.low[r] = low

    def column_copy(self, kind, c):
        source, place, step = {
            "forth": (None, None, 1),
            "back": (None, 1, -1),
            1: (1, 2, 1),
            2: (2, 2, -1),
            3: (3, 3, -1),
        }[kind]
        cols = self.cols(c)
        src = self.normed.at[:, cols] if source is None else self.column.at[source - 1, :, cols]
        if place is None:
            place = 1 + 2 * self.inner
        index = {"forth": 0, "back": 1}.get(kind, 2)
        return self.remote(
            src,
            self.column.at[place - 1, :, cols],
            self.column_send.at[index],
            self.column_recv.at[place - 1, c],
            self.at(step * self.way),
        )

    def column_arrive(self, r, c):
        cols = self.cols(c)
        self.remote(
            self.column.at[r - 1, :, cols],
            self.column.at[r - 1, :, cols],
            self.column_send.at[0],
            self.column_recv.at[r - 1, c],
            self.at(0),
        ).wait_recv()

    def ask_copy(self, r, c, k):
        cols = self.cols(c)
        return self.remote(
            self.asked.at[r, pl.ds((k - 1) * self.share, self.share), cols],
            self.served.at[r, pl.ds((self.columns - k) * self.share, self.share), cols],
            self.ask_send.at[0],
            self.ask_recv.at[r],
            self.beside(k),
        )

    def give_copy(self, r, c, k):
        cols = self.cols(c)
        return self.remote(
            self.given.at[r, pl.ds((k - 1) * self.share, self.share), cols],
            self.answer.at[r, pl.ds((self.columns - k) * self.share, self.share), cols],
            self.give_send.at[0],
            self.give_recv.at[r, c],
            self.beside(k),
        )

    def ask(self, inner, r, c):
        cols = self.cols(c)
        if r > 0:
            self.column_arrive(r, c)
            if inner == 1:
                self.column_copy(r, c).start()
        lines = self.normed[:, cols] if r == 0 else self.column[r - 1, :, cols]
        chosen = jnp.dot(self.pick[r], lines, preferred_element_type=F32).astype(BF16)
        self.served[r, 0 : self.share, cols] = chosen[0 : self.share]
        for k in range(1, self.columns):
            part = slice((k - 1) * self.share, k * self.share)
            self.asked[r, part, cols] = chosen[k * self.share : (k + 1) * self.share]
            self.ask_copy(r, c, k).start()

    def serve_up(self, r):
        block = self.asked.at[r]
        self.remote(
            block, block, self.ask_send.at[0], self.ask_recv.at[r], self.at(0)
        ).wait_recv()
        if r == 0:
            self.loads[0].wait()
            self.loads[1].wait()

        def up_tile(t, carry):
            cols = pl.ds(pl.multiple_of(t * TILE, TILE), TILE)
            lines = self.served[r]
            gate = jnp.dot(lines, self.gate[:, cols], preferred_element_type=F32)
            up = jnp.dot(lines, self.up[:, cols], preferred_element_type=F32)
            self.hidden[:, cols] = (gate / (1.0 + jnp.exp(-gate)) * up).astype(BF16)
            return carry

        lax.fori_loop(0, self.gate.shape[1] // TILE, up_tile, 0)

    def serve_down(self, r, c):
        if r == 0 and c == 0:
            self.loads[2].wait()

        def down_tile(t, carry):
            cols = pl.ds(pl.multiple_of(c * self.width + t * TILE, TILE), TILE)
            lines = jnp.dot(
                self.hidden[...], self.down[:, cols], preferred_element_type=F32
            ).astype(BF16)
            self.answer[r, 0 : self.share, cols] = lines[0 : self.share]
            self.given[r, :, cols] = lines[self.share :]
            return carry

        lax.fori_loop(0, self.width // TILE, down_tile, 0)
        for k in range(1, self.columns):
            self.give_copy(r, c, k).start()

    def combine(self, r, c):
        block = self.given.at[r, :, self.cols(c)]
        self.remote(
            block, block, self.give_send.at[0], self.give_recv.at[r, c], self.at(0)
        ).wait_recv()
        lines = self.answer[r, :, self.cols(c)]
        return jnp.dot(self.high[r], lines, preferred_element_type=F32) + jnp.dot(
            self.low[r], lines, preferred_element_type=F32
        )

    def part_copy(self, slot, place, step, c):
        cols = self.cols(c)
        return self.remote(
            self.partial.at[slot, :, cols],
            self.incoming.at[place, :, cols],
            self.part_send.at[0],
            self.part_recv.at[place, c],
            self.at(step * self.way),
        )

    def part_arrive(self, place, c):
        cols = self.cols(c)
        self.remote(
            self.partial.at[0, :, cols],
            self.incoming.at[place, :, cols],
            self.part_send.at[0],
            self.part_recv.at[place, c],
            self.at(0),
        ).wait_recv()
        return self.incoming[place, :, cols].astype(F32)

    def merge(self, r, c, slot, place, step, feed=None):
        total = self.combine(r, c)
        if feed is not None:
            total = total + self.part_arrive(feed, c)
        self.partial[slot, :, self.cols(c)] = total.astype(BF16)
        self.part_copy(slot, place, step, c).start()

    def own(self, c):
        cols = self.cols(c)
        self.hold[:, cols] = self.mixed[:, cols] + self.combine(0, c)

    def finish(self, c, places):
        cols = self.cols(c)
        total = self.hold[:, cols]
        for place in places:
            total = total + self.part_arrive(place, c)
        self.result[:, cols] = total.astype(BF16)
        self.out_copy(c).start()

    def out_copy(self, c):
        cols = self.cols(c)
        return pltpu.make_async_copy(
            self.result.at[:, cols], self.out.at[:, cols], self.out_sem.at[0]
        )

    def edge(self):
        chunks = range(CHUNKS)
        ask = functools.partial(self.ask, 0)

        def toward(r, c):
            self.merge(r, c, r - 1, r - 1, 1)

        for c in chunks:
            self.column_copy("forth", c).start()
        for c in chunks:
            ask(0, c)
        for c in chunks:
            ask(1, c)
        self.serve_up(0)
        for c in chunks:
            self.serve_down(0, c)
        self.serve_up(1)
        for c in chunks:
            self.serve_down(1, c)
        ask(2, 0)
        ask(2, 1)
        toward(1, 0)
        ask(2, 2)
        for c in range(1, CHUNKS):
            toward(1, c)
        ask(2, 3)
        self.serve_up(2)
        for c in chunks:
            self.serve_down(2, c)
        ask(3, 0)
        ask(3, 1)
        toward(2, 0)
        ask(3, 2)
        for c in range(1, CHUNKS):
            toward(2, c)
        ask(3, 3)
        for c in chunks:
            self.own(c)
        self.serve_up(3)
        for c in chunks:
            self.serve_down(3, c)
        for c in chunks:
            toward(3, c)
        for c in chunks:
            self.finish(c, (5,))

    def inside(self):
        chunks = range(CHUNKS)
        half = CHUNKS // 2
        ask = functools.partial(self.ask, 1)
        for c in chunks:
            self.column_copy("back", c).start()
            if c < half:
                self.column_copy("forth", c).start()
        for c in chunks:
            ask(0, c)
        ask(1, 0)
        self.serve_up(0)
        ask(1, 1)
        self.serve_down(0, 0)
        self.serve_down(0, 1)
        ask(2, 0)
        ask(1, 2)
        self.serve_down(0, 2)
        self.serve_down(0, 3)
        ask(2, 1)
        ask(1, 3)
        for c in range(half, CHUNKS):
            self.column_copy("forth", c).start()
        ask(2, 2)
        ask(2, 3)
        ask(3, 0)
        ask(3, 1)
        self.serve_up(1)
        self.serve_down(1, 0)
        self.serve_down(1, 1)
        ask(3, 2)
        self.serve_down(1, 2)
        self.serve_down(1, 3)
        ask(3, 3)
        for r in (2, 3):
            self.serve_up(r)
            for c in chunks:
                self.serve_down(r, c)
        for c in chunks:
            self.own(c)

        def far(c):
            self.merge(2, c, 1, 3, 1, 1)

        def near(c):
            self.merge(1, c, 3, 5, -1, 3)

        for c in chunks:
            far(c)
            if c > 0:
                near(c - 1)
        near(CHUNKS - 1)
        for c in chunks:
            self.merge(3, c, 2, 4, 1, 2)
        for c in chunks:
            self.finish(c, (0, 4))

    def run(self):
        pl.when(self.role(0))(self.edge)
        pl.when(self.role(1))(self.inside)
        ends = [
            (self.normed, self.column_send.at[0]),
            (self.asked, self.ask_send.at[0]),
            (self.given, self.give_send.at[0]),
            (self.partial.at[pl.ds(0, 3)], self.part_send.at[0]),
        ]
        for block, sem in ends:
            self.remote(block, block, sem, self.part_recv.at[0, 0], self.at(0)).wait_send()

        @pl.when(self.role(1))
        def _():
            for block, way in ((self.normed, 1), (self.column, 2)):
                self.remote(
                    block, block, self.column_send.at[way], self.part_recv.at[0, 0], self.at(0)
                ).wait_send()

        self.tables_all().wait_send()
        pltpu.make_async_copy(self.result, self.out, self.out_sem.at[0]).wait()


def layer_kernel(n, dp, capacity, *refs):
    inputs, refs = refs[:10], refs[10:]
    weights, out_ref, refs = refs[:3], refs[3], refs[4:]
    middle, refs = refs[:2], refs[2:]
    attention, refs = refs[:34], refs[34:]
    load_sem, stores = refs[0], refs[1:4]
    loads = [
        pltpu.make_async_copy(src.at[0], dst, load_sem.at[i])
        for i, (src, dst) in enumerate(zip(weights, stores))
    ]

    def start_loads():
        for load in loads:
            load.start()

    experts = Experts(n, capacity, *inputs[8:], middle, loads, out_ref, *refs[1:])
    drain = attention_part(n, dp, start_loads, *inputs[:8], *middle, experts.prepare, *attention)
    experts.run()
    drain()


def on_device(
    n,
    dp,
    queries,
    key_rows,
    values,
    query_gain,
    key_gain,
    out_weight,
    residual,
    norm_gain,
    expert_gate,
    expert_up,
    expert_down,
    routes,
    route_weight,
):
    _, rows, heads, width = queries.shape
    kv_heads = key_rows.shape[2]
    model = heads * width
    length = rows * n
    experts = expert_gate.shape[0] * n
    capacity = max(2, 4 * (rows // 2) // experts)
    across = max(x for x in range(1, n + 1) if n % x == 0 and x * x <= n)
    depth = n // across
    local_kv, local = kv_heads // across, heads // across
    units = across * local_kv
    slots = 2 * across * capacity
    aside = 2 * (across - 1) * capacity
    w_rows, w_cols = out_weight.shape
    dma = pltpu.SemaphoreType.DMA
    ny = dp // 2
    ff = expert_gate.shape[2]
    attention_scratch = [
        pltpu.VMEM((rows, heads, width), BF16),
        pltpu.VMEM((rows, kv_heads, width), BF16),
        pltpu.VMEM((rows, kv_heads, width), BF16),
        pltpu.VMEM((rows, heads, width), F32),
        pltpu.VMEM((across, 2 * local_kv, rows, width), BF16),
        pltpu.VMEM((across - 1, local, rows, width), BF16),
        pltpu.VMEM((local, across * rows, width), BF16),
        pltpu.VMEM((2 * local_kv, length, width), BF16),
        pltpu.VMEM((w_rows * n, w_cols), BF16),
        pltpu.VMEM((across - 1, rows, local * width), BF16),
        pltpu.VMEM((dp, rows, model), BF16),
        pltpu.VMEM((dp, rows, w_cols), BF16),
        pltpu.VMEM((dp, rows, w_cols), BF16),
        pltpu.VMEM((rows, model), BF16),
        pltpu.VMEM((2, 1, width), F32),
        pltpu.VMEM((1, model), F32),
        dma((8,)),
        dma((1,)),
        dma((across - 1, local_kv)),
        dma((2,)),
        dma((units, depth)),
        dma((1,)),
        dma((1,)),
        dma((1,)),
        dma((2,)),
        dma((2,)),
        dma((4, depth)),
        dma((1,)),
        dma((across - 1, local_kv)),
        dma((1,)),
        dma((max(1, ny - 1), units)),
        dma((2,)),
        dma((2,)),
        dma((2,)),
    ]
    result = pl.pallas_call(
        functools.partial(layer_kernel, n, dp, capacity),
        out_shape=jax.ShapeDtypeStruct((rows, model), BF16),
        in_specs=[ANY] * 8 + [VMEM] * 2 + [ANY] * 3,
        out_specs=ANY,
        scratch_shapes=[
            pltpu.VMEM((rows, model), F32),
            pltpu.VMEM((rows, model), BF16),
            *attention_scratch,
            dma((3,)),
            pltpu.VMEM((model, ff), BF16),
            pltpu.VMEM((model, ff), BF16),
            pltpu.VMEM((ff, model), BF16),
            pltpu.VMEM((depth, 8, rows), F32),
            pltpu.VMEM((depth, slots, rows), BF16),
            pltpu.VMEM((depth, rows, slots), BF16),
            pltpu.VMEM((depth, rows, slots), BF16),
            pltpu.VMEM((depth - 1, rows, model), BF16),
            pltpu.VMEM((depth, aside, model), BF16),
            pltpu.VMEM((depth, slots, model), BF16),
            pltpu.VMEM((depth, slots, model), BF16),
            pltpu.VMEM((depth, aside, model), BF16),
            pltpu.VMEM((slots, ff), BF16),
            pltpu.VMEM((4, rows, model), BF16),
            pltpu.VMEM((6, rows, model), BF16),
            pltpu.VMEM((rows, model), F32),
            pltpu.VMEM((rows, model), BF16),
            dma((2,)),
            dma((3,)),
            dma((depth - 1, CHUNKS)),
            dma((1,)),
            dma((depth,)),
            dma((1,)),
            dma((depth, CHUNKS)),
            dma((1,)),
            dma((6, CHUNKS)),
            dma((1,)),
        ],
        compiler_params=pltpu.CompilerParams(
            collective_id=0, has_side_effects=True, vmem_limit_bytes=56 * 1024 * 1024
        ),
        name="layer",
    )(
        queries[0],
        key_rows[0],
        values[0],
        query_gain[None],
        key_gain[None],
        out_weight,
        residual[0],
        norm_gain[None],
        routes[0].T,
        route_weight[0].T,
        expert_gate,
        expert_up,
        expert_down,
    )
    return result[None]


def solution(mesh):
    in_specs = (
        P("dp", "sp", None, None),
        P("dp", "sp", None, None),
        P("dp", "sp", None, None),
        P(),
        P(),
        P("sp", "dp"),
        P("dp", "sp", None),
        P(),
        P("sp", None, None),
        P("sp", None, None),
        P("sp", None, None),
        P("dp", "sp", None),
        P("dp", "sp", None),
    )
    out_specs = P("dp", "sp", None)
    return jax.shard_map(
        functools.partial(on_device, mesh.shape["sp"], mesh.shape["dp"]),
        mesh=mesh,
        in_specs=in_specs,
        out_specs=out_specs,
        check_vma=False,
    )
```

```python
import functools
import math

import jax
import jax.numpy as jnp
from jax import lax
from jax.experimental import pallas as pl
from jax.experimental.pallas import tpu as pltpu
from jax.sharding import PartitionSpec as P

GRID_W = 64
EPS = 1e-06
CHUNKS = 4
TILE = 256
THETA = 10000.0
MESH = pl.DeviceIdType.MESH
VMEM = pl.BlockSpec(memory_space=pltpu.VMEM)
ANY = pl.BlockSpec(memory_space=pl.ANY)
F32 = jnp.float32
BF16 = jnp.bfloat16


def rotation_tables(start, rows, width):
    quarter = width // 4
    lane = lax.broadcasted_iota(jnp.int32, (rows, width), 1)
    position = start + lax.broadcasted_iota(jnp.int32, (rows, width), 0)
    place = jnp.where(lane < 2 * quarter, position // GRID_W, position % GRID_W)
    part = lane % (2 * quarter)
    power = (part % quarter).astype(F32) * (-math.log(THETA) / quarter)
    angles = place.astype(F32) * jnp.exp(power)
    sign = jnp.where(part < quarter, -1.0, 1.0).astype(F32)
    return jnp.cos(angles), jnp.sin(angles) * sign


def turn(rows, gain, cosine, sine):
    width = rows.shape[-1]
    quarter = width // 4
    a = rows.astype(F32)
    a = a * lax.rsqrt(jnp.mean(a * a, axis=-1, keepdims=True) + EPS) * gain
    lane = lax.broadcasted_iota(jnp.int32, a.shape, 1) % (2 * quarter)
    partner = jnp.where(
        lane < quarter, pltpu.roll(a, width - quarter, 1), pltpu.roll(a, quarter, 1)
    )
    return (a * cosine + partner * sine).astype(BF16)


class Line:
    def __init__(self, depth, width, block, send, recv):
        self.depth, self.width, self.block = depth, width, block
        self.send, self.recv = send, recv
        me = lax.axis_index("sp")
        self.z, self.x = me // width, me % width

    def copy(self, unit, plane, way, target):
        return pltpu.make_async_remote_copy(
            src_ref=self.block(unit, plane * self.width + self.x),
            dst_ref=self.block(unit, plane * self.width + self.x),
            send_sem=self.send.at[way],
            recv_sem=self.recv.at[unit, plane],
            device_id={"sp": target * self.width + self.x},
            device_id_type=MESH,
        )

    def start(self, condition, unit, plane, way, target):
        @pl.when(condition)
        def _():
            self.copy(unit, plane, way, target).start()

    def up(self, condition, unit, plane):
        self.start(condition & (self.z < self.depth - 1), unit, plane, 0, self.z + 1)

    def down(self, condition, unit, plane):
        self.start(condition & (self.z > 0), unit, plane, 1, self.z - 1)

    def arrive(self, condition, unit, plane):
        @pl.when(condition)
        def _():
            self.copy(unit, plane, 0, plane).wait_recv()

    def step(self, t, unit, condition=True, then=None):
        below = (self.z - t >= 0) & condition
        above = (self.z + t < self.depth) & condition
        self.arrive(below, unit, self.z - t)
        self.up(below, unit, self.z - t)
        if then is not None:
            then(below, unit, self.z - t)
        self.arrive(above, unit, self.z + t)
        self.down(above, unit, self.z + t)
        if then is not None:
            then(above, unit, self.z + t)

    def drain(self, planes):
        for way in range(2):
            for count in range(1, self.depth):
                z = count - 1 if way == 0 else self.depth - count

                @pl.when(self.z == z)
                def _():
                    pltpu.make_async_remote_copy(
                        src_ref=planes(count),
                        dst_ref=planes(count),
                        send_sem=self.send.at[way],
                        recv_sem=self.recv.at[0, 0],
                        device_id={"sp": self.z * self.width + self.x},
                        device_id_type=MESH,
                    ).wait_send()


def selection(table, first_expert, column, columns, capacity):
    rows = table.shape[1]
    few = rows // 2
    slots = columns * 2 * capacity
    slot = lax.broadcasted_iota(jnp.int32, (slots, rows), 0)
    row = lax.broadcasted_iota(jnp.int32, (slots, rows), 1)
    side = (column + slot // (2 * capacity)) % columns
    expert = (first_expert + side).astype(F32)
    same = (slot // capacity) % 2 == row // few
    first = (table[0:1, :] == expert) & same
    second = (table[1:2, :] == expert) & same
    named = jnp.where(first | second, 1.0, 0.0).astype(BF16)
    before = lax.broadcasted_iota(jnp.int32, (rows, rows), 0)
    after = lax.broadcasted_iota(jnp.int32, (rows, rows), 1)
    earlier = jnp.where(before < after, 1.0, 0.0).astype(BF16)
    rank = jnp.dot(named, earlier, preferred_element_type=F32)
    here = rank == (slot % capacity).astype(F32)
    choice = jnp.where((first | second) & here, 1.0, 0.0)
    weight = jnp.where(first & here, table[2:3, :], 0.0)
    weight = weight + jnp.where(second & here, table[3:4, :], 0.0)
    weight = weight.T
    high = weight.astype(BF16)
    low = (weight - high.astype(F32)).astype(BF16)
    return choice.astype(BF16), high, low


def attention_part(
    n,
    dp,
    start_loads,
    q_ref,
    k_ref,
    v_ref,
    qg_ref,
    kg_ref,
    w_ref,
    res_ref,
    ng_ref,
    mixed_ref,
    normed_ref,
    prepare,
    q_in,
    k_in,
    v_in,
    wide,
    stage,
    q_stage,
    q_all,
    kv,
    w_full,
    swap,
    att,
    proj,
    back,
    res_in,
    gains,
    norm_in,
    in_sem,
    kvx_send,
    kvx_recv,
    kvz_send,
    kvz_recv,
    qx_send,
    qx_recv,
    wx_send,
    wx_recv,
    wo_sem,
    wz_send,
    wz_recv,
    ax_send,
    ax_recv,
    y_send,
    y_recv,
    pair_sem,
    fwd_sem,
    back_sem,
):
    me = lax.axis_index("sp")
    mine = lax.axis_index("dp")
    rows, heads, width = q_ref.shape
    kv_heads = k_ref.shape[1]
    group = heads // kv_heads
    model = heads * width
    across = stage.shape[0]
    depth = n // across
    local_kv = kv_heads // across
    local = heads // across
    z, x = me // across, me % across
    always = me >= 0
    ny = dp // 2
    core = mine % 2
    row_y = mine // 2
    partner = row_y * 2 + 1 - core
    w_rows, w_cols = w_ref.shape

    def span(start, size):
        return pl.ds(pl.multiple_of(start * size, size), size)

    fetches = [
        pltpu.make_async_copy(src, dst, in_sem.at[i])
        for i, (src, dst) in enumerate(
            (
                (k_ref, k_in),
                (v_ref, v_in),
                (kg_ref, gains.at[0]),
                (q_ref, q_in),
                (qg_ref, gains.at[1]),
                (w_ref, w_full.at[span(me, w_rows)]),
                (res_ref, res_in),
                (ng_ref, norm_in),
            )
        )
    ]
    for fetch in fetches:
        fetch.start()
    barrier = pltpu.get_barrier_semaphore()
    for d in range(1, n):
        pl.semaphore_signal(
            barrier, inc=1, device_id={"sp": lax.rem(me + d, n)}, device_id_type=MESH
        )
    for d in range(1, dp):
        pl.semaphore_signal(
            barrier, inc=1, device_id={"dp": lax.rem(mine + d, dp)}, device_id_type=MESH
        )

    cosine, sine = rotation_tables(me * rows, rows, width)
    my_rows = span(me, rows)
    for fetch in fetches[:3]:
        fetch.wait()
    for part, source in ((0, k_in), (1, v_in)):
        wide[:, 0:kv_heads, :] = source[...].astype(F32)
        for g in range(kv_heads):
            lines = wide[:, g, :]
            slot = 2 * (g % local_kv) + part
            if part == 0:
                lines = turn(lines, gains[0], cosine, sine)
            stage[g // local_kv, slot] = lines.astype(BF16)
    for c in range(2 * local_kv):
        kv[c, my_rows, :] = stage[x, c]
    pl.semaphore_wait(barrier, n - 1 + dp - 1)

    def remote(src, dst, send, recv, **device):
        return pltpu.make_async_remote_copy(
            src_ref=src,
            dst_ref=dst,
            send_sem=send,
            recv_sem=recv,
            device_id=device,
            device_id_type=MESH,
        )

    def beside(k):
        return z * across + lax.rem(x + k, across)

    def kv_block(g, sp):
        return kv.at[pl.ds(2 * g, 2), span(sp, rows), :]

    kv_units = [(k, g) for g in range(local_kv) for k in range(across)]
    own_units = [u for u, (k, _) in enumerate(kv_units) if k == 0]

    def kv_unit(u, sp):
        k, g = kv_units[u]
        return kv_block(g, sp - sp % across + lax.rem(sp % across + k, across))

    halves = 2
    w_units = [(j, k) for j in range(halves) for k in range(2)]
    part_rows, part_cols = w_rows // 2, w_cols // halves

    def w_unit(u, sp):
        j, k = w_units[u]
        start = pl.multiple_of(sp * w_rows + k * part_rows, part_rows)
        return w_full.at[pl.ds(start, part_rows), pl.ds(j * part_cols, part_cols)]

    kv_line = Line(depth, across, kv_unit, kvz_send, kvz_recv)
    w_line = Line(depth, across, w_unit, wz_send, wz_recv)
    kvx, qx, ax = {}, {}, {}
    for g in range(local_kv):
        for k in range(1, across):
            kvx[k, g] = remote(
                stage.at[lax.rem(x + k, across), pl.ds(2 * g, 2)],
                kv_block(g, me),
                kvx_send.at[0],
                kvx_recv.at[across - k - 1, g],
                sp=beside(k),
            )
            kvx[k, g].start()
        kv_line.up(always, own_units[g], z)
        kv_line.down(always, own_units[g], z)

    start_loads()
    fetches[3].wait()
    fetches[4].wait()
    for h in range(0, heads, 8):
        wide[:, h : h + 8, :] = q_in[:, h : h + 8, :].astype(F32)
    for k in list(range(1, across)) + [0]:
        first = lax.rem(x + k, across) * local

        def turn_head(i, carry):
            lines = turn(wide[:, pl.ds(first + i, 1), :].reshape(rows, width), gains[1], cosine, sine)
            if k == 0:
                q_all[i, 0:rows] = lines
            else:
                q_stage[k - 1, i] = lines
            return carry

        lax.fori_loop(0, local, turn_head, 0)
        if k > 0:
            qx[k] = remote(
                q_stage.at[k - 1],
                q_all.at[:, pl.ds((across - k) * rows, rows), :],
                qx_send.at[0],
                qx_recv.at[0],
                sp=beside(k),
            )
            qx[k].start()
        if k == across - 1:
            for u, (kk, g) in enumerate(kv_units):
                if kk == 0:
                    continue
                remote(
                    stage.at[0, pl.ds(2 * g, 2)],
                    kv_block(g, beside(kk)),
                    kvx_send.at[0],
                    kvx_recv.at[kk - 1, g],
                    sp=me,
                ).wait_recv()
                kv_line.up(always, u, z)
                kv_line.down(always, u, z)
    fetches[5].wait()

    def w_across(condition, u, plane):
        for k in range(1, across):

            @pl.when(condition)
            def _():
                remote(
                    w_unit(u, plane * across + x),
                    w_unit(u, plane * across + x),
                    wx_send.at[w_units[u][0]],
                    wx_recv.at[w_units[u][0]] if plane is not z else wo_sem.at[0],
                    sp=beside(k),
                ).start()

    upper = z // (depth // 2)
    way = 1 - 2 * upper
    middle = (z > 0) & (z < depth - 1)
    edge = jnp.logical_not(middle)

    def w_half(sp, j):
        return w_full.at[span(sp, w_rows), pl.ds(j * part_cols, part_cols)]

    def w_along():
        block = w_full.at[pl.ds(0, (across - 1) * w_rows)]
        remote(block, block, wo_sem.at[1], wo_sem.at[0], sp=me).wait_recv()
        for j in range(halves):
            for k in range(1, across):
                block = w_half(beside(k), j)
                target = me + way * across
                remote(block, block, wo_sem.at[1], wx_recv.at[j], sp=target).start()

        @pl.when(middle)
        def _():
            for k in range(1, across):
                block = w_half(beside(k), 0)
                target = me - way * across
                remote(block, block, wo_sem.at[2], wx_recv.at[0], sp=target).start()

    def w_aside(units):
        def then(condition, u, plane):
            if w_units[u][0] in units:
                w_across(condition, u, plane)

        return then

    def w_begin(t):
        for u in range(len(w_units)):
            w_line.up(z == t, u, z)
            w_line.down(depth - 1 - z == t, u, z)

    w_begin(0)
    prepare(0)
    for u in range(len(w_units)):
        w_across(always, u, z)
    for t in range(1, depth - 1):
        for u in range(len(kv_units)):
            kv_line.step(t, u)
        w_begin(t)
    prepare(1)
    remote(
        q_stage,
        q_all.at[:, pl.ds(rows, (across - 1) * rows), :],
        qx_send.at[0],
        qx_recv.at[0],
        sp=me,
    ).wait_recv()

    scale = width ** (-0.5)
    wide_group = group * width

    def att_cols(k, g):
        side = lax.rem(x + k, across)
        start = (side * local_kv + g) * wide_group
        return pl.ds(pl.multiple_of(start, wide_group), wide_group)

    def spread_att(u):
        k, g = kv_units[u]
        block = att.at[mine, :, att_cols(k, g)]
        for j in range(1, ny):
            target = lax.rem(row_y + j, ny) * 2 + core
            remote(block, block, y_send.at[0], y_recv.at[j - 1, u], dp=target).start()
        remote(block, block, pair_sem.at[0], pair_sem.at[1], dp=partner).start()

    def forward(u):
        for j in range(1, ny):
            source = lax.rem(row_y + ny - j, ny) * 2 + core
            remote(
                att.at[mine, :, att_cols(*kv_units[u])],
                att.at[mine, :, att_cols(*kv_units[u])],
                y_send.at[0],
                y_recv.at[j - 1, u],
                dp=mine,
            ).wait_recv()
            block = att.at[source, :, att_cols(*kv_units[u])]
            remote(block, block, fwd_sem.at[0], fwd_sem.at[1], dp=partner).start()

    for g in range(local_kv):
        for u, (_, gg) in enumerate(kv_units):
            if gg == g:
                kv_line.step(depth - 1, u)
        if g == local_kv - 1:
            for u in range(len(w_units)):
                w_line.step(1, u, middle)
            w_along()

        def one_head(i, carry):
            h = g * group + i
            scores = (
                lax.dot_general(
                    q_all[h], kv[2 * g], (((1,), (1,)), ((), ())), preferred_element_type=F32
                )
                * scale
            )
            exponent = jnp.exp(scores - jnp.max(scores, axis=-1, keepdims=True))
            weights = (exponent / jnp.sum(exponent, axis=-1, keepdims=True)).astype(BF16)
            out = jnp.dot(weights, kv[2 * g + 1], preferred_element_type=F32).astype(BF16)
            cols = pl.ds(pl.multiple_of((x * local + h) * width, width), width)
            att[mine, :, cols] = out[0:rows]
            cols = pl.ds(pl.multiple_of(h * width, width), width)
            for k in range(1, across):
                swap[k - 1, :, cols] = out[k * rows : (k + 1) * rows]
            return carry

        lax.fori_loop(0, group, one_head, 0)
        for k in range(1, across):
            ax[k, g] = remote(
                swap.at[k - 1, :, pl.ds(g * wide_group, wide_group)],
                att.at[mine, :, att_cols(0, g)],
                ax_send.at[0],
                ax_recv.at[across - k - 1, g],
                sp=beside(k),
            )
            ax[k, g].start()
        spread_att(own_units[g])
    for t in range(2, depth - 1):
        for u in range(len(w_units)):
            w_line.step(t, u, middle, w_across)
    for u in range(len(w_units)):
        w_line.step(1, u, edge, w_aside((1,)))
    for u, (k, g) in enumerate(kv_units):
        if k == 0:
            continue
        remote(
            swap.at[0, :, pl.ds(g * wide_group, wide_group)],
            att.at[mine, :, att_cols(k, g)],
            ax_send.at[0],
            ax_recv.at[k - 1, g],
            sp=me,
        ).wait_recv()
        spread_att(u)
    for t in range(2, depth - 1):
        for u in range(len(w_units)):
            w_line.step(t, u, edge, w_across)
    order = own_units + [u for u in range(len(kv_units)) if u not in own_units]
    for i in range(max(len(order), len(w_units))):
        if i < len(w_units):
            w_line.step(depth - 1, i, True, w_across)
        if i < len(order):
            forward(order[i])
    if ny > 1:
        remote(
            att.at[pl.ds(0, ny - 1)],
            att.at[pl.ds(0, ny - 1)],
            fwd_sem.at[0],
            fwd_sem.at[1],
            dp=mine,
        ).wait_recv()
    remote(att.at[mine], att.at[mine], pair_sem.at[0], pair_sem.at[1], dp=mine).wait_recv()

    for j in range(halves):
        cols = slice(j * part_cols, (j + 1) * part_cols)
        block = w_full.at[pl.ds(0, (depth - 1) * (across - 1) * w_rows), cols]
        remote(block, block, wx_send.at[0], wx_recv.at[j], sp=me).wait_recv()
        result = jnp.dot(
            att[...].reshape(dp * rows, model), w_full[:, cols], preferred_element_type=F32
        ).astype(BF16)
        for s in range(dp):
            proj[s, :, cols] = result[s * rows : (s + 1) * rows]
        back[mine, :, cols] = proj[mine, :, cols]
        order = sorted(range(1, dp), key=lambda d: d % 2)
        for d in order:
            target = lax.rem(mine + d, dp)
            remote(
                proj.at[target, :, cols],
                back.at[mine, :, cols],
                back_sem.at[0],
                back_sem.at[1],
                dp=target,
            ).start()

    fetches[6].wait()
    fetches[7].wait()
    block = back.at[pl.ds(0, dp - 1)]
    remote(block, block, back_sem.at[0], back_sem.at[1], dp=mine).wait_recv()
    square = jnp.zeros((rows, 1), F32)
    for s in range(dp):
        cols = slice(s * w_cols, (s + 1) * w_cols)
        part = res_in[:, cols].astype(F32) + back[s].astype(F32)
        mixed_ref[:, cols] = part
        square = square + jnp.sum(part * part, axis=-1, keepdims=True)
    factor = lax.rsqrt(square / model + EPS)
    for s in range(dp):
        cols = slice(s * w_cols, (s + 1) * w_cols)
        normed_ref[:, cols] = (mixed_ref[:, cols] * factor * norm_in[:, cols]).astype(BF16)

    def drain():
        kv_line.drain(lambda count: kv.at[:, pl.ds(0, count * across * rows), :])
        w_line.drain(lambda count: w_full.at[pl.ds(0, count * w_rows)])
        for role, counts in ((edge, (depth - 1, depth)), (middle, (2, 2))):

            @pl.when(role)
            def _():
                for j, count in enumerate(counts):
                    block = w_full.at[
                        pl.ds(0, count * (across - 1) * w_rows), pl.ds(0, part_cols)
                    ]
                    remote(block, block, wx_send.at[j], back_sem.at[1], sp=me).wait_send()

        @pl.when(middle)
        def _():
            block = w_full.at[pl.ds(0, (across - 1) * w_rows), pl.ds(0, part_cols)]
            remote(block, block, wo_sem.at[2], back_sem.at[1], sp=me).wait_send()

        whole = [
            (w_full.at[pl.ds(0, (across - 1) * w_rows)], wo_sem.at[1]),
            (stage.at[pl.ds(0, across - 1)], kvx_send.at[0]),
            (q_stage, qx_send.at[0]),
            (swap, ax_send.at[0]),
            (att.at[mine], pair_sem.at[0]),
            (proj.at[pl.ds(0, dp - 1)], back_sem.at[0]),
        ]
        if ny > 1:
            whole.append((att.at[pl.ds(0, ny - 1)], y_send.at[0]))
            whole.append((att.at[pl.ds(0, ny - 1)], fwd_sem.at[0]))
        for block, sem in whole:
            remote(block, block, sem, back_sem.at[1], sp=me).wait_send()

    return drain


class Experts:
    def __init__(self, n, capacity, routes, gates, middle, loads, out, *refs):
        (
            self.gate,
            self.up,
            self.down,
            self.tables,
            self.pick,
            self.high,
            self.low,
            self.column,
            self.asked,
            self.served,
            self.answer,
            self.given,
            self.hidden,
            self.partial,
            self.incoming,
            self.hold,
            self.result,
            self.table_sem,
            self.column_send,
            self.column_recv,
            self.ask_send,
            self.ask_recv,
            self.give_send,
            self.give_recv,
            self.part_send,
            self.part_recv,
            self.out_sem,
        ) = refs
        self.mixed, self.normed = middle
        self.routes, self.gates = routes, gates
        self.loads, self.out = loads, out
        me = lax.axis_index("sp")
        self.columns = max(x for x in range(1, n + 1) if n % x == 0 and x * x <= n)
        self.depth = n // self.columns
        self.z, self.x = me // self.columns, me % self.columns
        self.upper = self.z // (self.depth // 2)
        self.way = 1 - 2 * self.upper
        self.inner = self.upper * (self.depth - 1) + self.way * self.z
        self.capacity = capacity
        self.rows, self.model = self.normed.shape
        self.width = self.model // CHUNKS
        self.share = 2 * capacity

    def role(self, inner):
        return self.inner == inner

    def plane(self, r):
        place = (self.inner, 1 - self.inner, self.depth - 1, self.depth - 2)[r]
        return self.upper * (self.depth - 1) + self.way * place

    def remote(self, src, dst, send, recv, target):
        return pltpu.make_async_remote_copy(
            src_ref=src,
            dst_ref=dst,
            send_sem=send,
            recv_sem=recv,
            device_id={"sp": target},
            device_id_type=MESH,
        )

    def at(self, step):
        return (self.z + step) * self.columns + self.x

    def beside(self, k):
        return self.z * self.columns + (self.x + k) % self.columns

    def cols(self, c):
        return slice(c * self.width, (c + 1) * self.width)

    def tables_all(self):
        block = self.tables.at[pl.ds(0, self.depth - 1)]
        return self.remote(block, block, self.table_sem.at[0], self.table_sem.at[1], self.at(0))

    def prepare(self, phase):
        planes = self.depth

        def table_copy(d):
            target = (self.z + d) % planes
            return self.remote(
                self.tables.at[self.z],
                self.tables.at[self.z],
                self.table_sem.at[0],
                self.table_sem.at[1],
                target * self.columns + self.x,
            )

        if phase == 0:
            rows = self.rows
            self.tables[self.z] = jnp.concatenate(
                [self.routes[...].astype(F32), self.gates[...], jnp.zeros((4, rows), F32)], axis=0
            )
            for d in range(1, planes):
                table_copy(d).start()
            return
        self.tables_all().wait_recv()
        for r in range(planes):
            choice, high, low = selection(
                self.tables[self.plane(r)],
                self.z * self.columns,
                self.x,
                self.columns,
                self.capacity,
            )
            self.pick[r] = choice
            self.high[r] = high
            self.low[r] = low

    def column_copy(self, kind, c):
        source, place, step = {
            "forth": (None, None, 1),
            "back": (None, 1, -1),
            1: (1, 2, 1),
            2: (2, 2, -1),
            3: (3, 3, -1),
        }[kind]
        cols = self.cols(c)
        src = self.normed.at[:, cols] if source is None else self.column.at[source - 1, :, cols]
        if place is None:
            place = 1 + 2 * self.inner
        index = {"forth": 0, "back": 1}.get(kind, 2)
        return self.remote(
            src,
            self.column.at[place - 1, :, cols],
            self.column_send.at[index],
            self.column_recv.at[place - 1, c],
            self.at(step * self.way),
        )

    def column_arrive(self, r, c):
        cols = self.cols(c)
        self.remote(
            self.column.at[r - 1, :, cols],
            self.column.at[r - 1, :, cols],
            self.column_send.at[0],
            self.column_recv.at[r - 1, c],
            self.at(0),
        ).wait_recv()

    def ask_copy(self, r, c, k):
        cols = self.cols(c)
        return self.remote(
            self.asked.at[r, pl.ds((k - 1) * self.share, self.share), cols],
            self.served.at[r, pl.ds((self.columns - k) * self.share, self.share), cols],
            self.ask_send.at[0],
            self.ask_recv.at[r],
            self.beside(k),
        )

    def give_copy(self, r, c, k):
        cols = self.cols(c)
        return self.remote(
            self.given.at[r, pl.ds((k - 1) * self.share, self.share), cols],
            self.answer.at[r, pl.ds((self.columns - k) * self.share, self.share), cols],
            self.give_send.at[0],
            self.give_recv.at[r, c],
            self.beside(k),
        )

    def ask(self, inner, r, c):
        cols = self.cols(c)
        if r > 0:
            self.column_arrive(r, c)
            if inner == 1:
                self.column_copy(r, c).start()
        lines = self.normed[:, cols] if r == 0 else self.column[r - 1, :, cols]
        chosen = jnp.dot(self.pick[r], lines, preferred_element_type=F32).astype(BF16)
        self.served[r, 0 : self.share, cols] = chosen[0 : self.share]
        for k in range(1, self.columns):
            part = slice((k - 1) * self.share, k * self.share)
            self.asked[r, part, cols] = chosen[k * self.share : (k + 1) * self.share]
            self.ask_copy(r, c, k).start()

    def serve_up(self, r, first=False):
        block = self.asked.at[r]
        self.remote(
            block, block, self.ask_send.at[0], self.ask_recv.at[r], self.at(0)
        ).wait_recv()
        if first:
            self.loads[0].wait()
            self.loads[1].wait()

        def up_tile(t, carry):
            cols = pl.ds(pl.multiple_of(t * TILE, TILE), TILE)
            lines = self.served[r]
            gate = jnp.dot(lines, self.gate[:, cols], preferred_element_type=F32)
            up = jnp.dot(lines, self.up[:, cols], preferred_element_type=F32)
            self.hidden[min(r, 1), :, cols] = (gate / (1.0 + jnp.exp(-gate)) * up).astype(BF16)
            return carry

        lax.fori_loop(0, self.gate.shape[1] // TILE, up_tile, 0)

    def serve_down(self, r, c, first=False):
        if first:
            self.loads[2].wait()

        def down_tile(t, carry):
            cols = pl.ds(pl.multiple_of(c * self.width + t * TILE, TILE), TILE)
            lines = jnp.dot(
                self.hidden[min(r, 1)], self.down[:, cols], preferred_element_type=F32
            ).astype(BF16)
            self.answer[r, 0 : self.share, cols] = lines[0 : self.share]
            self.given[r, :, cols] = lines[self.share :]
            return carry

        lax.fori_loop(0, self.width // TILE, down_tile, 0)
        for k in range(1, self.columns):
            self.give_copy(r, c, k).start()

    def combine(self, r, c):
        block = self.given.at[r, :, self.cols(c)]
        self.remote(
            block, block, self.give_send.at[0], self.give_recv.at[r, c], self.at(0)
        ).wait_recv()
        lines = self.answer[r, :, self.cols(c)]
        return jnp.dot(self.high[r], lines, preferred_element_type=F32) + jnp.dot(
            self.low[r], lines, preferred_element_type=F32
        )

    def part_copy(self, slot, place, step, c):
        cols = self.cols(c)
        return self.remote(
            self.partial.at[slot, :, cols],
            self.incoming.at[place, :, cols],
            self.part_send.at[0],
            self.part_recv.at[place, c],
            self.at(step * self.way),
        )

    def part_arrive(self, place, c):
        cols = self.cols(c)
        self.remote(
            self.partial.at[0, :, cols],
            self.incoming.at[place, :, cols],
            self.part_send.at[0],
            self.part_recv.at[place, c],
            self.at(0),
        ).wait_recv()
        return self.incoming[place, :, cols].astype(F32)

    def merge(self, r, c, slot, place, step, feed=None):
        total = self.combine(r, c)
        if feed is not None:
            total = total + self.part_arrive(feed, c)
        self.partial[slot, :, self.cols(c)] = total.astype(BF16)
        self.part_copy(slot, place, step, c).start()

    def own(self, c):
        cols = self.cols(c)
        self.hold[:, cols] = self.mixed[:, cols] + self.combine(0, c)

    def finish(self, c, places):
        cols = self.cols(c)
        total = self.hold[:, cols]
        for place in places:
            total = total + self.part_arrive(place, c)
        self.result[:, cols] = total.astype(BF16)
        self.out_copy(c).start()

    def out_copy(self, c):
        cols = self.cols(c)
        return pltpu.make_async_copy(
            self.result.at[:, cols], self.out.at[:, cols], self.out_sem.at[0]
        )

    def edge(self):
        chunks = range(CHUNKS)
        ask = functools.partial(self.ask, 0)

        def toward(r, c):
            self.merge(r, c, r - 1, r - 1, 1)

        def down(r, *cs):
            for c in cs:
                self.serve_down(r, c, r == 1 and c == 0)

        for c in chunks:
            self.column_copy("forth", c).start()
        for c in chunks:
            ask(1, c)
        for c in chunks:
            ask(0, c)
        self.serve_up(1, True)
        down(1, *chunks)
        ask(2, 0)
        toward(1, 0)
        ask(2, 1)
        toward(1, 1)
        toward(1, 2)
        ask(2, 2)
        toward(1, 3)
        ask(2, 3)
        ask(3, 0)
        ask(3, 1)
        self.serve_up(0)
        ask(3, 2)
        ask(3, 3)
        self.serve_up(2)
        down(2, *chunks)
        toward(2, 0)
        toward(2, 1)
        self.serve_up(3)
        toward(2, 2)
        toward(2, 3)
        down(3, *chunks)
        down(0, *chunks)
        for c in chunks:
            toward(3, c)
        for c in chunks:
            self.own(c)
        for c in chunks:
            self.finish(c, (5,))

    def inside(self):
        chunks = range(CHUNKS)
        ask = functools.partial(self.ask, 1)

        def down(r, *cs):
            for c in cs:
                self.serve_down(r, c, r == 0 and c == 0)

        for c in chunks:
            self.column_copy("back", c).start()
            self.column_copy("forth", c).start()
        for c in chunks:
            ask(0, c)
        ask(3, 0)
        self.serve_up(0, True)
        ask(1, 0)
        down(0, 0, 1)
        ask(1, 1)
        ask(2, 0)
        down(0, 2, 3)
        ask(1, 2)
        ask(2, 1)
        ask(1, 3)
        ask(2, 2)
        ask(2, 3)
        ask(3, 1)
        ask(3, 2)
        ask(3, 3)
        for r in (1, 2, 3):
            self.serve_up(r)
            down(r, *chunks)
        for c in chunks:
            self.own(c)

        def far(c):
            self.merge(2, c, 1, 3, 1, 1)

        def near(c):
            self.merge(1, c, 3, 5, -1, 3)

        for c in chunks:
            far(c)
            if c > 0:
                near(c - 1)
        near(CHUNKS - 1)
        for c in chunks:
            self.merge(3, c, 2, 4, 1, 2)
        for c in chunks:
            self.finish(c, (0, 4))

    def run(self):
        pl.when(self.role(0))(self.edge)
        pl.when(self.role(1))(self.inside)
        ends = [
            (self.normed, self.column_send.at[0]),
            (self.asked, self.ask_send.at[0]),
            (self.given, self.give_send.at[0]),
            (self.partial.at[pl.ds(0, 3)], self.part_send.at[0]),
        ]
        for block, sem in ends:
            self.remote(block, block, sem, self.part_recv.at[0, 0], self.at(0)).wait_send()

        @pl.when(self.role(1))
        def _():
            for block, way in ((self.normed, 1), (self.column, 2)):
                self.remote(
                    block, block, self.column_send.at[way], self.part_recv.at[0, 0], self.at(0)
                ).wait_send()

        self.tables_all().wait_send()
        pltpu.make_async_copy(self.result, self.out, self.out_sem.at[0]).wait()


def layer_kernel(n, dp, capacity, *refs):
    inputs, refs = refs[:10], refs[10:]
    weights, out_ref, refs = refs[:3], refs[3], refs[4:]
    middle, refs = refs[:2], refs[2:]
    attention, refs = refs[:35], refs[35:]
    load_sem, stores = refs[0], refs[1:4]
    loads = [
        pltpu.make_async_copy(src.at[0], dst, load_sem.at[i])
        for i, (src, dst) in enumerate(zip(weights, stores))
    ]

    def start_loads():
        for load in loads:
            load.start()

    experts = Experts(n, capacity, *inputs[8:], middle, loads, out_ref, *refs[1:])
    drain = attention_part(n, dp, start_loads, *inputs[:8], *middle, experts.prepare, *attention)
    experts.run()
    drain()


def on_device(
    n,
    dp,
    queries,
    key_rows,
    values,
    query_gain,
    key_gain,
    out_weight,
    residual,
    norm_gain,
    expert_gate,
    expert_up,
    expert_down,
    routes,
    route_weight,
):
    _, rows, heads, width = queries.shape
    kv_heads = key_rows.shape[2]
    model = heads * width
    length = rows * n
    experts = expert_gate.shape[0] * n
    capacity = max(2, 4 * (rows // 2) // experts)
    across = max(x for x in range(1, n + 1) if n % x == 0 and x * x <= n)
    depth = n // across
    local_kv, local = kv_heads // across, heads // across
    units = across * local_kv
    slots = 2 * across * capacity
    aside = 2 * (across - 1) * capacity
    w_rows, w_cols = out_weight.shape
    dma = pltpu.SemaphoreType.DMA
    ny = dp // 2
    ff = expert_gate.shape[2]
    attention_scratch = [
        pltpu.VMEM((rows, heads, width), BF16),
        pltpu.VMEM((rows, kv_heads, width), BF16),
        pltpu.VMEM((rows, kv_heads, width), BF16),
        pltpu.VMEM((rows, heads, width), F32),
        pltpu.VMEM((across, 2 * local_kv, rows, width), BF16),
        pltpu.VMEM((across - 1, local, rows, width), BF16),
        pltpu.VMEM((local, across * rows, width), BF16),
        pltpu.VMEM((2 * local_kv, length, width), BF16),
        pltpu.VMEM((w_rows * n, w_cols), BF16),
        pltpu.VMEM((across - 1, rows, local * width), BF16),
        pltpu.VMEM((dp, rows, model), BF16),
        pltpu.VMEM((dp, rows, w_cols), BF16),
        pltpu.VMEM((dp, rows, w_cols), BF16),
        pltpu.VMEM((rows, model), BF16),
        pltpu.VMEM((2, 1, width), F32),
        pltpu.VMEM((1, model), F32),
        dma((8,)),
        dma((1,)),
        dma((across - 1, local_kv)),
        dma((2,)),
        dma((units, depth)),
        dma((1,)),
        dma((1,)),
        dma((2,)),
        dma((2,)),
        dma((3,)),
        dma((2,)),
        dma((4, depth)),
        dma((1,)),
        dma((across - 1, local_kv)),
        dma((1,)),
        dma((max(1, ny - 1), units)),
        dma((2,)),
        dma((2,)),
        dma((2,)),
    ]
    result = pl.pallas_call(
        functools.partial(layer_kernel, n, dp, capacity),
        out_shape=jax.ShapeDtypeStruct((rows, model), BF16),
        in_specs=[ANY] * 8 + [VMEM] * 2 + [ANY] * 3,
        out_specs=ANY,
        scratch_shapes=[
            pltpu.VMEM((rows, model), F32),
            pltpu.VMEM((rows, model), BF16),
            *attention_scratch,
            dma((3,)),
            pltpu.VMEM((model, ff), BF16),
            pltpu.VMEM((model, ff), BF16),
            pltpu.VMEM((ff, model), BF16),
            pltpu.VMEM((depth, 8, rows), F32),
            pltpu.VMEM((depth, slots, rows), BF16),
            pltpu.VMEM((depth, rows, slots), BF16),
            pltpu.VMEM((depth, rows, slots), BF16),
            pltpu.VMEM((depth - 1, rows, model), BF16),
            pltpu.VMEM((depth, aside, model), BF16),
            pltpu.VMEM((depth, slots, model), BF16),
            pltpu.VMEM((depth, slots, model), BF16),
            pltpu.VMEM((depth, aside, model), BF16),
            pltpu.VMEM((2, slots, ff), BF16),
            pltpu.VMEM((4, rows, model), BF16),
            pltpu.VMEM((6, rows, model), BF16),
            pltpu.VMEM((rows, model), F32),
            pltpu.VMEM((rows, model), BF16),
            dma((2,)),
            dma((3,)),
            dma((depth - 1, CHUNKS)),
            dma((1,)),
            dma((depth,)),
            dma((1,)),
            dma((depth, CHUNKS)),
            dma((1,)),
            dma((6, CHUNKS)),
            dma((1,)),
        ],
        compiler_params=pltpu.CompilerParams(
            collective_id=0, has_side_effects=True, vmem_limit_bytes=56 * 1024 * 1024
        ),
        name="layer",
    )(
        queries[0],
        key_rows[0],
        values[0],
        query_gain[None],
        key_gain[None],
        out_weight,
        residual[0],
        norm_gain[None],
        routes[0].T,
        route_weight[0].T,
        expert_gate,
        expert_up,
        expert_down,
    )
    return result[None]


def solution(mesh):
    in_specs = (
        P("dp", "sp", None, None),
        P("dp", "sp", None, None),
        P("dp", "sp", None, None),
        P(),
        P(),
        P("sp", "dp"),
        P("dp", "sp", None),
        P(),
        P("sp", None, None),
        P("sp", None, None),
        P("sp", None, None),
        P("dp", "sp", None),
        P("dp", "sp", None),
    )
    out_specs = P("dp", "sp", None)
    return jax.shard_map(
        functools.partial(on_device, mesh.shape["sp"], mesh.shape["dp"]),
        mesh=mesh,
        in_specs=in_specs,
        out_specs=out_specs,
        check_vma=False,
    )
```

```python
import functools
import math

import jax
import jax.numpy as jnp
from jax import lax
from jax.experimental import pallas as pl
from jax.experimental.pallas import tpu as pltpu
from jax.sharding import PartitionSpec as P

GRID_W = 64
EPS = 1e-06
CHUNKS = 4
TILE = 256
THETA = 10000.0
MESH = pl.DeviceIdType.MESH
VMEM = pl.BlockSpec(memory_space=pltpu.VMEM)
ANY = pl.BlockSpec(memory_space=pl.ANY)
F32 = jnp.float32
BF16 = jnp.bfloat16


def rotation_tables(start, rows, width):
    quarter = width // 4
    lane = lax.broadcasted_iota(jnp.int32, (rows, width), 1)
    position = start + lax.broadcasted_iota(jnp.int32, (rows, width), 0)
    place = jnp.where(lane < 2 * quarter, position // GRID_W, position % GRID_W)
    part = lane % (2 * quarter)
    power = (part % quarter).astype(F32) * (-math.log(THETA) / quarter)
    angles = place.astype(F32) * jnp.exp(power)
    sign = jnp.where(part < quarter, -1.0, 1.0).astype(F32)
    return jnp.cos(angles), jnp.sin(angles) * sign


def turn(rows, gain, cosine, sine):
    width = rows.shape[-1]
    quarter = width // 4
    a = rows.astype(F32)
    a = a * lax.rsqrt(jnp.mean(a * a, axis=-1, keepdims=True) + EPS) * gain
    lane = lax.broadcasted_iota(jnp.int32, a.shape, 1) % (2 * quarter)
    partner = jnp.where(
        lane < quarter, pltpu.roll(a, width - quarter, 1), pltpu.roll(a, quarter, 1)
    )
    return (a * cosine + partner * sine).astype(BF16)


class Line:
    def __init__(self, depth, width, block, send, recv):
        self.depth, self.width, self.block = depth, width, block
        self.send, self.recv = send, recv
        me = lax.axis_index("sp")
        self.z, self.x = me // width, me % width

    def copy(self, unit, plane, way, target):
        return pltpu.make_async_remote_copy(
            src_ref=self.block(unit, plane * self.width + self.x),
            dst_ref=self.block(unit, plane * self.width + self.x),
            send_sem=self.send.at[way],
            recv_sem=self.recv.at[unit, plane],
            device_id={"sp": target * self.width + self.x},
            device_id_type=MESH,
        )

    def start(self, condition, unit, plane, way, target):
        @pl.when(condition)
        def _():
            self.copy(unit, plane, way, target).start()

    def up(self, condition, unit, plane):
        self.start(condition & (self.z < self.depth - 1), unit, plane, 0, self.z + 1)

    def down(self, condition, unit, plane):
        self.start(condition & (self.z > 0), unit, plane, 1, self.z - 1)

    def arrive(self, condition, unit, plane):
        @pl.when(condition)
        def _():
            self.copy(unit, plane, 0, plane).wait_recv()

    def step(self, t, unit, condition=True, then=None):
        below = (self.z - t >= 0) & condition
        above = (self.z + t < self.depth) & condition
        self.arrive(below, unit, self.z - t)
        self.up(below, unit, self.z - t)
        if then is not None:
            then(below, unit, self.z - t)
        self.arrive(above, unit, self.z + t)
        self.down(above, unit, self.z + t)
        if then is not None:
            then(above, unit, self.z + t)

    def drain(self, planes):
        for way in range(2):
            for count in range(1, self.depth):
                z = count - 1 if way == 0 else self.depth - count

                @pl.when(self.z == z)
                def _():
                    pltpu.make_async_remote_copy(
                        src_ref=planes(count),
                        dst_ref=planes(count),
                        send_sem=self.send.at[way],
                        recv_sem=self.recv.at[0, 0],
                        device_id={"sp": self.z * self.width + self.x},
                        device_id_type=MESH,
                    ).wait_send()


def selection(table, first_expert, column, columns, capacity):
    rows = table.shape[1]
    few = rows // 2
    slots = columns * 2 * capacity
    slot = lax.broadcasted_iota(jnp.int32, (slots, rows), 0)
    row = lax.broadcasted_iota(jnp.int32, (slots, rows), 1)
    side = (column + slot // (2 * capacity)) % columns
    expert = (first_expert + side).astype(F32)
    same = (slot // capacity) % 2 == row // few
    first = (table[0:1, :] == expert) & same
    second = (table[1:2, :] == expert) & same
    named = jnp.where(first | second, 1.0, 0.0).astype(BF16)
    before = lax.broadcasted_iota(jnp.int32, (rows, rows), 0)
    after = lax.broadcasted_iota(jnp.int32, (rows, rows), 1)
    earlier = jnp.where(before < after, 1.0, 0.0).astype(BF16)
    rank = jnp.dot(named, earlier, preferred_element_type=F32)
    here = rank == (slot % capacity).astype(F32)
    choice = jnp.where((first | second) & here, 1.0, 0.0)
    weight = jnp.where(first & here, table[2:3, :], 0.0)
    weight = weight + jnp.where(second & here, table[3:4, :], 0.0)
    weight = weight.T
    high = weight.astype(BF16)
    low = (weight - high.astype(F32)).astype(BF16)
    return choice.astype(BF16), high, low


def attention_part(
    n,
    dp,
    start_loads,
    q_ref,
    k_ref,
    v_ref,
    qg_ref,
    kg_ref,
    w_ref,
    res_ref,
    ng_ref,
    mixed_ref,
    normed_ref,
    experts,
    q_in,
    k_in,
    v_in,
    wide,
    stage,
    q_stage,
    q_all,
    kv,
    w_full,
    swap,
    att,
    proj,
    back,
    res_in,
    gains,
    norm_in,
    in_sem,
    kvx_send,
    kvx_recv,
    kvz_send,
    kvz_recv,
    qx_send,
    qx_recv,
    wx_send,
    wx_recv,
    wo_sem,
    wz_send,
    wz_recv,
    ax_send,
    ax_recv,
    y_send,
    y_recv,
    pair_sem,
    fwd_sem,
    back_send,
    back_recv,
):
    me = lax.axis_index("sp")
    mine = lax.axis_index("dp")
    rows, heads, width = q_ref.shape
    kv_heads = k_ref.shape[1]
    group = heads // kv_heads
    model = heads * width
    across = stage.shape[0]
    depth = n // across
    local_kv = kv_heads // across
    local = heads // across
    z, x = me // across, me % across
    always = me >= 0
    ny = dp // 2
    core = mine % 2
    row_y = mine // 2
    partner = row_y * 2 + 1 - core
    w_rows, w_cols = w_ref.shape

    def span(start, size):
        return pl.ds(pl.multiple_of(start * size, size), size)

    fetches = [
        pltpu.make_async_copy(src, dst, in_sem.at[i])
        for i, (src, dst) in enumerate(
            (
                (k_ref, k_in),
                (v_ref, v_in),
                (kg_ref, gains.at[0]),
                (q_ref, q_in),
                (qg_ref, gains.at[1]),
                (w_ref, w_full.at[span(me, w_rows)]),
                (res_ref, res_in),
                (ng_ref, norm_in),
            )
        )
    ]
    for fetch in fetches:
        fetch.start()
    barrier = pltpu.get_barrier_semaphore()
    for d in range(1, n):
        pl.semaphore_signal(
            barrier, inc=1, device_id={"sp": lax.rem(me + d, n)}, device_id_type=MESH
        )
    for d in range(1, dp):
        pl.semaphore_signal(
            barrier, inc=1, device_id={"dp": lax.rem(mine + d, dp)}, device_id_type=MESH
        )

    cosine, sine = rotation_tables(me * rows, rows, width)
    my_rows = span(me, rows)
    for fetch in fetches[:3]:
        fetch.wait()
    for part, source in ((0, k_in), (1, v_in)):
        wide[:, 0:kv_heads, :] = source[...].astype(F32)
        for g in range(kv_heads):
            lines = wide[:, g, :]
            slot = 2 * (g % local_kv) + part
            if part == 0:
                lines = turn(lines, gains[0], cosine, sine)
            stage[g // local_kv, slot] = lines.astype(BF16)
    for c in range(2 * local_kv):
        kv[c, my_rows, :] = stage[x, c]
    pl.semaphore_wait(barrier, n - 1 + dp - 1)

    def remote(src, dst, send, recv, **device):
        return pltpu.make_async_remote_copy(
            src_ref=src,
            dst_ref=dst,
            send_sem=send,
            recv_sem=recv,
            device_id=device,
            device_id_type=MESH,
        )

    def beside(k):
        return z * across + lax.rem(x + k, across)

    def kv_block(g, sp):
        return kv.at[pl.ds(2 * g, 2), span(sp, rows), :]

    kv_units = [(k, g) for g in range(local_kv) for k in range(across)]
    own_units = [u for u, (k, _) in enumerate(kv_units) if k == 0]

    def kv_unit(u, sp):
        k, g = kv_units[u]
        return kv_block(g, sp - sp % across + lax.rem(sp % across + k, across))

    halves = 2
    w_units = [(j, k) for j in range(halves) for k in range(2)]
    part_rows, part_cols = w_rows // 2, w_cols // halves

    def w_unit(u, sp):
        j, k = w_units[u]
        start = pl.multiple_of(sp * w_rows + k * part_rows, part_rows)
        return w_full.at[pl.ds(start, part_rows), pl.ds(j * part_cols, part_cols)]

    kv_line = Line(depth, across, kv_unit, kvz_send, kvz_recv)
    w_line = Line(depth, across, w_unit, wz_send, wz_recv)
    kvx, qx, ax = {}, {}, {}
    for g in range(local_kv):
        for k in range(1, across):
            kvx[k, g] = remote(
                stage.at[lax.rem(x + k, across), pl.ds(2 * g, 2)],
                kv_block(g, me),
                kvx_send.at[0],
                kvx_recv.at[across - k - 1, g],
                sp=beside(k),
            )
            kvx[k, g].start()
        kv_line.up(always, own_units[g], z)
        kv_line.down(always, own_units[g], z)

    start_loads()
    fetches[3].wait()
    fetches[4].wait()
    for h in range(0, heads, 8):
        wide[:, h : h + 8, :] = q_in[:, h : h + 8, :].astype(F32)
    for k in list(range(1, across)) + [0]:
        first = lax.rem(x + k, across) * local

        def turn_head(i, carry):
            lines = turn(wide[:, pl.ds(first + i, 1), :].reshape(rows, width), gains[1], cosine, sine)
            if k == 0:
                q_all[i, 0:rows] = lines
            else:
                q_stage[k - 1, i] = lines
            return carry

        lax.fori_loop(0, local, turn_head, 0)
        if k > 0:
            qx[k] = remote(
                q_stage.at[k - 1],
                q_all.at[:, pl.ds((across - k) * rows, rows), :],
                qx_send.at[0],
                qx_recv.at[0],
                sp=beside(k),
            )
            qx[k].start()
        if k == across - 1:
            for u, (kk, g) in enumerate(kv_units):
                if kk == 0:
                    continue
                remote(
                    stage.at[0, pl.ds(2 * g, 2)],
                    kv_block(g, beside(kk)),
                    kvx_send.at[0],
                    kvx_recv.at[kk - 1, g],
                    sp=me,
                ).wait_recv()
                kv_line.up(always, u, z)
                kv_line.down(always, u, z)
    fetches[5].wait()

    def w_across(condition, u, plane):
        for k in range(1, across):

            @pl.when(condition)
            def _():
                remote(
                    w_unit(u, plane * across + x),
                    w_unit(u, plane * across + x),
                    wx_send.at[w_units[u][0]],
                    wx_recv.at[w_units[u][0]] if plane is not z else wo_sem.at[0],
                    sp=beside(k),
                ).start()

    upper = z // (depth // 2)
    way = 1 - 2 * upper

    def block_of(i, step):
        row = lax.rem(row_y + ny + step * (i // 2), ny)
        return row * 2 + (core if i % 2 == 0 else 1 - core)

    middle = (z > 0) & (z < depth - 1)
    edge = jnp.logical_not(middle)

    def w_half(sp, j):
        return w_full.at[span(sp, w_rows), pl.ds(j * part_cols, part_cols)]

    def w_along():
        block = w_full.at[pl.ds(0, (across - 1) * w_rows)]
        remote(block, block, wo_sem.at[1], wo_sem.at[0], sp=me).wait_recv()
        for j in range(halves):
            for k in range(1, across):
                block = w_half(beside(k), j)
                target = me + way * across
                remote(block, block, wo_sem.at[1], wx_recv.at[j], sp=target).start()

        @pl.when(middle)
        def _():
            for k in range(1, across):
                block = w_half(beside(k), 0)
                target = me - way * across
                remote(block, block, wo_sem.at[2], wx_recv.at[0], sp=target).start()

    def w_aside(units):
        def then(condition, u, plane):
            if w_units[u][0] in units:
                w_across(condition, u, plane)

        return then

    def w_begin(t):
        for u in range(len(w_units)):
            w_line.up(z == t, u, z)
            w_line.down(depth - 1 - z == t, u, z)

    w_begin(0)
    experts.prepare(0)
    for u in range(len(w_units)):
        w_across(always, u, z)
    for t in range(1, depth - 1):
        for u in range(len(kv_units)):
            kv_line.step(t, u)
        w_begin(t)
    experts.prepare(1)
    remote(
        q_stage,
        q_all.at[:, pl.ds(rows, (across - 1) * rows), :],
        qx_send.at[0],
        qx_recv.at[0],
        sp=me,
    ).wait_recv()

    scale = width ** (-0.5)
    wide_group = group * width

    def att_cols(k, g):
        side = lax.rem(x + k, across)
        start = (side * local_kv + g) * wide_group
        return pl.ds(pl.multiple_of(start, wide_group), wide_group)

    def spread_att(u):
        k, g = kv_units[u]
        block = att.at[mine, :, att_cols(k, g)]
        for j in range(1, ny):
            target = lax.rem(row_y + j, ny) * 2 + core
            remote(block, block, y_send.at[0], y_recv.at[j - 1, u], dp=target).start()
        remote(block, block, pair_sem.at[0], pair_sem.at[1], dp=partner).start()

    def forward(u):
        for j in range(1, ny):
            source = lax.rem(row_y + ny - j, ny) * 2 + core
            remote(
                att.at[mine, :, att_cols(*kv_units[u])],
                att.at[mine, :, att_cols(*kv_units[u])],
                y_send.at[0],
                y_recv.at[j - 1, u],
                dp=mine,
            ).wait_recv()
            block = att.at[source, :, att_cols(*kv_units[u])]
            remote(block, block, fwd_sem.at[0], fwd_sem.at[1], dp=partner).start()

    for g in range(local_kv):
        for u, (_, gg) in enumerate(kv_units):
            if gg == g:
                kv_line.step(depth - 1, u)
        if g == local_kv - 1:
            for u in range(len(w_units)):
                w_line.step(1, u, middle)
            w_along()

        def one_head(i, carry):
            h = g * group + i
            scores = (
                lax.dot_general(
                    q_all[h], kv[2 * g], (((1,), (1,)), ((), ())), preferred_element_type=F32
                )
                * scale
            )
            exponent = jnp.exp(scores - jnp.max(scores, axis=-1, keepdims=True))
            weights = (exponent / jnp.sum(exponent, axis=-1, keepdims=True)).astype(BF16)
            out = jnp.dot(weights, kv[2 * g + 1], preferred_element_type=F32).astype(BF16)
            cols = pl.ds(pl.multiple_of((x * local + h) * width, width), width)
            att[mine, :, cols] = out[0:rows]
            cols = pl.ds(pl.multiple_of(h * width, width), width)
            for k in range(1, across):
                swap[k - 1, :, cols] = out[k * rows : (k + 1) * rows]
            return carry

        lax.fori_loop(0, group, one_head, 0)
        for k in range(1, across):
            ax[k, g] = remote(
                swap.at[k - 1, :, pl.ds(g * wide_group, wide_group)],
                att.at[mine, :, att_cols(0, g)],
                ax_send.at[0],
                ax_recv.at[across - k - 1, g],
                sp=beside(k),
            )
            ax[k, g].start()
        spread_att(own_units[g])
    for t in range(2, depth - 1):
        for u in range(len(w_units)):
            w_line.step(t, u, middle, w_across)
    for u in range(len(w_units)):
        w_line.step(1, u, edge, w_aside((1,)))
    for u, (k, g) in enumerate(kv_units):
        if k == 0:
            continue
        remote(
            swap.at[0, :, pl.ds(g * wide_group, wide_group)],
            att.at[mine, :, att_cols(k, g)],
            ax_send.at[0],
            ax_recv.at[k - 1, g],
            sp=me,
        ).wait_recv()
        spread_att(u)
    for t in range(2, depth - 1):
        for u in range(len(w_units)):
            w_line.step(t, u, edge, w_across)
    order = own_units + [u for u in range(len(kv_units)) if u not in own_units]
    for i in range(max(len(order), len(w_units))):
        if i < len(w_units):
            w_line.step(depth - 1, i, True, w_across)
        if i < len(order):
            forward(order[i])
    if ny > 1:
        remote(
            att.at[pl.ds(0, ny - 1)],
            att.at[pl.ds(0, ny - 1)],
            fwd_sem.at[0],
            fwd_sem.at[1],
            dp=mine,
        ).wait_recv()
    remote(att.at[mine], att.at[mine], pair_sem.at[0], pair_sem.at[1], dp=mine).wait_recv()

    for j in range(halves):
        cols = slice(j * part_cols, (j + 1) * part_cols)
        block = w_full.at[pl.ds(0, (depth - 1) * (across - 1) * w_rows), cols]
        remote(block, block, wx_send.at[0], wx_recv.at[j], sp=me).wait_recv()
        result = jnp.dot(
            att[...].reshape(dp * rows, model), w_full[:, cols], preferred_element_type=F32
        ).astype(BF16)
        for s in range(dp):
            proj[s, :, cols] = result[s * rows : (s + 1) * rows]
        back[mine, :, cols] = proj[mine, :, cols]
        for i in list(range(2, dp)) + [1]:
            target = block_of(i, 1)
            remote(
                proj.at[target, :, cols],
                back.at[mine, :, cols],
                back_send.at[0],
                back_recv.at[i],
                dp=target,
            ).start()

    fetches[6].wait()
    fetches[7].wait()
    square = jnp.zeros((rows, 1), F32)
    each = dp // CHUNKS
    for i in range(dp):
        source = block_of(i, -1)
        if i > 0:
            remote(back.at[mine], back.at[source], back_send.at[0], back_recv.at[i], dp=mine).wait_recv()
        cols = span(source, w_cols)
        part = res_in[:, cols].astype(F32) + back[source].astype(F32)
        mixed_ref[:, cols] = part
        square = square + jnp.sum(part * part, axis=-1, keepdims=True)
        normed_ref[:, i * w_cols : (i + 1) * w_cols] = part.astype(BF16)
        if i == dp - 1:
            factor = lax.rsqrt(square / model + EPS)
            high = factor.astype(BF16).astype(F32)
            mid = (factor - high).astype(BF16).astype(F32)
            lane = lax.broadcasted_iota(jnp.int32, (rows, width), 1)
            pieces = jnp.where(lane == 0, high, jnp.where(lane == 1, mid, 0.0))
            pieces = jnp.where(lane == 2, factor - high - mid, pieces)
            normed_ref[:, model : model + width] = pieces.astype(BF16)
        if i % each == each - 1:
            experts.launch(i // each)
        if i == dp // 2 - 1:
            experts.early()

    def drain():
        kv_line.drain(lambda count: kv.at[:, pl.ds(0, count * across * rows), :])
        w_line.drain(lambda count: w_full.at[pl.ds(0, count * w_rows)])
        for role, counts in ((edge, (depth - 1, depth)), (middle, (2, 2))):

            @pl.when(role)
            def _():
                for j, count in enumerate(counts):
                    block = w_full.at[
                        pl.ds(0, count * (across - 1) * w_rows), pl.ds(0, part_cols)
                    ]
                    remote(block, block, wx_send.at[j], back_recv.at[0], sp=me).wait_send()

        @pl.when(middle)
        def _():
            block = w_full.at[pl.ds(0, (across - 1) * w_rows), pl.ds(0, part_cols)]
            remote(block, block, wo_sem.at[2], back_recv.at[0], sp=me).wait_send()

        whole = [
            (w_full.at[pl.ds(0, (across - 1) * w_rows)], wo_sem.at[1]),
            (stage.at[pl.ds(0, across - 1)], kvx_send.at[0]),
            (q_stage, qx_send.at[0]),
            (swap, ax_send.at[0]),
            (att.at[mine], pair_sem.at[0]),
            (proj.at[pl.ds(0, dp - 1)], back_send.at[0]),
        ]
        if ny > 1:
            whole.append((att.at[pl.ds(0, ny - 1)], y_send.at[0]))
            whole.append((att.at[pl.ds(0, ny - 1)], fwd_sem.at[0]))
        for block, sem in whole:
            remote(block, block, sem, back_recv.at[0], sp=me).wait_send()

    return drain


class Experts:
    def __init__(self, n, dp, capacity, norm, routes, gates, middle, loads, out, *refs):
        (
            self.gate,
            self.up,
            self.down,
            self.tables,
            self.pick,
            self.high,
            self.low,
            self.column,
            self.asked,
            self.served,
            self.answer,
            self.given,
            self.ready,
            self.hidden,
            self.partial,
            self.incoming,
            self.hold,
            self.table_sem,
            self.column_send,
            self.column_recv,
            self.ask_send,
            self.ask_recv,
            self.give_send,
            self.give_recv,
            self.part_send,
            self.part_recv,
        ) = refs
        self.mixed, self.normed = middle
        self.routes, self.gates = routes, gates
        self.loads, self.out = loads, out
        me = lax.axis_index("sp")
        self.columns = max(x for x in range(1, n + 1) if n % x == 0 and x * x <= n)
        self.depth = n // self.columns
        self.z, self.x = me // self.columns, me % self.columns
        self.upper = self.z // (self.depth // 2)
        self.way = 1 - 2 * self.upper
        self.inner = self.upper * (self.depth - 1) + self.way * self.z
        self.capacity = capacity
        self.norm, self.dp = norm, dp
        self.rows, self.model = self.mixed.shape
        self.width = self.model // CHUNKS
        self.share = 2 * capacity

    def role(self, inner):
        return self.inner == inner

    def plane(self, r):
        place = (self.inner, 1 - self.inner, self.depth - 1, self.depth - 2)[r]
        return self.upper * (self.depth - 1) + self.way * place

    def remote(self, src, dst, send, recv, target):
        return pltpu.make_async_remote_copy(
            src_ref=src,
            dst_ref=dst,
            send_sem=send,
            recv_sem=recv,
            device_id={"sp": target},
            device_id_type=MESH,
        )

    def at(self, step):
        return (self.z + step) * self.columns + self.x

    def beside(self, k):
        return self.z * self.columns + (self.x + k) % self.columns

    def lanes(self, c):
        end = (c + 1) * self.width if c < CHUNKS - 1 else self.normed.shape[1]
        return slice(c * self.width, end)

    def early(self):
        @pl.when(self.role(0))
        def _():
            for c in range(CHUNKS // 2):
                self.ask(0, 1, c)

    def launch(self, c):
        self.column_copy("forth", c).start()

        @pl.when(self.role(1))
        def _():
            self.column_copy("back", c).start()

    def cols(self, c):
        return slice(c * self.width, (c + 1) * self.width)

    def tables_all(self):
        block = self.tables.at[pl.ds(0, self.depth - 1)]
        return self.remote(block, block, self.table_sem.at[0], self.table_sem.at[1], self.at(0))

    def prepare(self, phase):
        planes = self.depth

        def table_copy(d):
            target = (self.z + d) % planes
            return self.remote(
                self.tables.at[self.z],
                self.tables.at[self.z],
                self.table_sem.at[0],
                self.table_sem.at[1],
                target * self.columns + self.x,
            )

        if phase == 0:
            rows = self.rows
            self.tables[self.z] = jnp.concatenate(
                [self.routes[...].astype(F32), self.gates[...], jnp.zeros((4, rows), F32)], axis=0
            )
            for d in range(1, planes):
                table_copy(d).start()
            return
        self.tables_all().wait_recv()
        for r in range(planes):
            choice, high, low = selection(
                self.tables[self.plane(r)],
                self.z * self.columns,
                self.x,
                self.columns,
                self.capacity,
            )
            self.pick[r] = choice
            self.high[r] = high
            self.low[r] = low

    def column_copy(self, kind, c):
        source, place, step = {
            "forth": (None, None, 1),
            "back": (None, 1, -1),
            1: (1, 2, 1),
            2: (2, 2, -1),
            3: (3, 3, -1),
        }[kind]
        cols = self.lanes(c)
        src = self.normed.at[:, cols] if source is None else self.column.at[source - 1, :, cols]
        if place is None:
            place = 1 + 2 * self.inner
        index = {"forth": 0, "back": 1}.get(kind, 2)
        return self.remote(
            src,
            self.column.at[place - 1, :, cols],
            self.column_send.at[index],
            self.column_recv.at[place - 1, c],
            self.at(step * self.way),
        )

    def column_arrive(self, r, c):
        cols = self.lanes(c)
        self.remote(
            self.column.at[r - 1, :, cols],
            self.column.at[r - 1, :, cols],
            self.column_send.at[0],
            self.column_recv.at[r - 1, c],
            self.at(0),
        ).wait_recv()

    def ask_copy(self, r, c, k):
        cols = self.lanes(c)
        return self.remote(
            self.asked.at[r, pl.ds((k - 1) * self.share, self.share), cols],
            self.served.at[r, pl.ds((self.columns - k) * self.share, self.share), cols],
            self.ask_send.at[0],
            self.ask_recv.at[r],
            self.beside(k),
        )

    def give_copy(self, r, c, k):
        cols = self.cols(c)
        return self.remote(
            self.given.at[r, pl.ds((k - 1) * self.share, self.share), cols],
            self.answer.at[r, pl.ds((self.columns - k) * self.share, self.share), cols],
            self.give_send.at[0],
            self.give_recv.at[r, c],
            self.beside(k),
        )

    def ask(self, inner, r, c):
        cols = self.lanes(c)
        if r > 0:
            self.column_arrive(r, c)
            if inner == 1:
                self.column_copy(r, c).start()
        lines = self.normed[:, cols] if r == 0 else self.column[r - 1, :, cols]
        chosen = jnp.dot(self.pick[r], lines, preferred_element_type=F32).astype(BF16)
        self.served[r, 0 : self.share, cols] = chosen[0 : self.share]
        for k in range(1, self.columns):
            part = slice((k - 1) * self.share, k * self.share)
            self.asked[r, part, cols] = chosen[k * self.share : (k + 1) * self.share]
            self.ask_copy(r, c, k).start()

    def serve_up(self, r, first=False):
        block = self.asked.at[r]
        self.remote(
            block, block, self.ask_send.at[0], self.ask_recv.at[r], self.at(0)
        ).wait_recv()
        if first:
            self.loads[0].wait()
            self.loads[1].wait()

        pieces = self.served[r, :, self.model :].astype(F32)
        factor = jnp.sum(pieces, axis=-1, keepdims=True)
        mine = lax.axis_index("dp")
        size = self.model // self.dp
        for i in range(self.dp):
            row = (mine // 2 + self.dp // 2 - i // 2) % (self.dp // 2)
            block = row * 2 + (mine % 2 if i % 2 == 0 else 1 - mine % 2)
            cols = pl.ds(pl.multiple_of(block * size, size), size)
            lines = self.served[r, :, i * size : (i + 1) * size].astype(F32)
            self.ready[:, cols] = (lines * factor * self.norm[:, cols]).astype(BF16)

        def up_tile(t, carry):
            cols = pl.ds(pl.multiple_of(t * TILE, TILE), TILE)
            lines = self.ready[...]
            gate = jnp.dot(lines, self.gate[:, cols], preferred_element_type=F32)
            up = jnp.dot(lines, self.up[:, cols], preferred_element_type=F32)
            self.hidden[min(r, 1), :, cols] = (gate / (1.0 + jnp.exp(-gate)) * up).astype(BF16)
            return carry

        lax.fori_loop(0, self.gate.shape[1] // TILE, up_tile, 0)

    def serve_down(self, r, c, first=False):
        if first:
            self.loads[2].wait()

        def down_tile(t, carry):
            cols = pl.ds(pl.multiple_of(c * self.width + t * TILE, TILE), TILE)
            lines = jnp.dot(
                self.hidden[min(r, 1)], self.down[:, cols], preferred_element_type=F32
            ).astype(BF16)
            self.answer[r, 0 : self.share, cols] = lines[0 : self.share]
            self.given[r, :, cols] = lines[self.share :]
            return carry

        lax.fori_loop(0, self.width // TILE, down_tile, 0)
        for k in range(1, self.columns):
            self.give_copy(r, c, k).start()

    def combine(self, r, c):
        block = self.given.at[r, :, self.cols(c)]
        self.remote(
            block, block, self.give_send.at[0], self.give_recv.at[r, c], self.at(0)
        ).wait_recv()
        lines = self.answer[r, :, self.cols(c)]
        return jnp.dot(self.high[r], lines, preferred_element_type=F32) + jnp.dot(
            self.low[r], lines, preferred_element_type=F32
        )

    def part_copy(self, slot, place, step, c):
        cols = self.cols(c)
        return self.remote(
            self.partial.at[slot, :, cols],
            self.incoming.at[place, :, cols],
            self.part_send.at[0],
            self.part_recv.at[place, c],
            self.at(step * self.way),
        )

    def part_arrive(self, place, c):
        cols = self.cols(c)
        self.remote(
            self.partial.at[0, :, cols],
            self.incoming.at[place, :, cols],
            self.part_send.at[0],
            self.part_recv.at[place, c],
            self.at(0),
        ).wait_recv()
        return self.incoming[place, :, cols].astype(F32)

    def merge(self, r, c, slot, place, step, feed=None):
        total = self.combine(r, c)
        if feed is not None:
            total = total + self.part_arrive(feed, c)
        self.partial[slot, :, self.cols(c)] = total.astype(BF16)
        self.part_copy(slot, place, step, c).start()

    def own(self, c):
        cols = self.cols(c)
        self.hold[:, cols] = self.mixed[:, cols] + self.combine(0, c)

    def finish(self, c, places):
        cols = self.cols(c)
        total = self.hold[:, cols]
        for place in places:
            total = total + self.part_arrive(place, c)
        self.out[:, cols] = total.astype(BF16)

    def edge(self):
        chunks = range(CHUNKS)
        ask = functools.partial(self.ask, 0)

        def toward(r, c):
            self.merge(r, c, r - 1, r - 1, 1)

        def down(r, *cs):
            for c in cs:
                self.serve_down(r, c, r == 1 and c == 0)

        for c in range(CHUNKS // 2, CHUNKS):
            ask(1, c)
        for c in chunks:
            ask(0, c)
        self.serve_up(1, True)
        down(1, *chunks)
        ask(2, 0)
        toward(1, 0)
        ask(2, 1)
        toward(1, 1)
        toward(1, 2)
        ask(2, 2)
        toward(1, 3)
        ask(2, 3)
        ask(3, 0)
        self.serve_up(0)
        ask(3, 1)
        self.serve_up(2)
        down(2, *chunks)
        ask(3, 2)
        ask(3, 3)
        for c in chunks:
            toward(2, c)
        self.serve_up(3)
        down(3, *chunks)
        down(0, *chunks)
        for c in chunks:
            toward(3, c)
        for c in chunks:
            self.own(c)
        for c in chunks:
            self.finish(c, (5,))

    def inside(self):
        chunks = range(CHUNKS)
        ask = functools.partial(self.ask, 1)

        def down(r, *cs):
            for c in cs:
                self.serve_down(r, c, r == 0 and c == 0)

        for c in chunks:
            ask(0, c)
        ask(3, 0)
        ask(1, 0)
        ask(1, 1)
        ask(2, 0)
        ask(1, 2)
        ask(2, 1)
        ask(1, 3)
        ask(2, 2)
        ask(2, 3)
        ask(3, 1)
        ask(3, 2)
        ask(3, 3)
        for r in (0, 1, 2, 3):
            self.serve_up(r, r == 0)
            down(r, *chunks)
        for c in chunks:
            self.own(c)

        def far(c):
            self.merge(2, c, 1, 3, 1, 1)

        def near(c):
            self.merge(1, c, 3, 5, -1, 3)

        for c in chunks:
            far(c)
            if c > 0:
                near(c - 1)
        near(CHUNKS - 1)
        for c in chunks:
            self.merge(3, c, 2, 4, 1, 2)
        for c in chunks:
            self.finish(c, (0, 4))

    def run(self):
        pl.when(self.role(0))(self.edge)
        pl.when(self.role(1))(self.inside)
        ends = [
            (self.normed, self.column_send.at[0]),
            (self.asked, self.ask_send.at[0]),
            (self.given, self.give_send.at[0]),
            (self.partial.at[pl.ds(0, 3)], self.part_send.at[0]),
        ]
        for block, sem in ends:
            self.remote(block, block, sem, self.part_recv.at[0, 0], self.at(0)).wait_send()

        @pl.when(self.role(1))
        def _():
            for block, way in ((self.normed, 1), (self.column, 2)):
                self.remote(
                    block, block, self.column_send.at[way], self.part_recv.at[0, 0], self.at(0)
                ).wait_send()

        self.tables_all().wait_send()


def layer_kernel(n, dp, capacity, *refs):
    inputs, refs = refs[:10], refs[10:]
    weights, out_ref, refs = refs[:3], refs[3], refs[4:]
    middle, refs = refs[:2], refs[2:]
    attention, refs = refs[:36], refs[36:]
    load_sem, stores = refs[0], refs[1:4]
    loads = [
        pltpu.make_async_copy(src.at[0], dst, load_sem.at[i])
        for i, (src, dst) in enumerate(zip(weights, stores))
    ]

    def start_loads():
        for load in loads:
            load.start()

    norm = attention[15]
    experts = Experts(n, dp, capacity, norm, *inputs[8:], middle, loads, out_ref, *refs[1:])
    drain = attention_part(n, dp, start_loads, *inputs[:8], *middle, experts, *attention)
    experts.run()
    drain()


def on_device(
    n,
    dp,
    queries,
    key_rows,
    values,
    query_gain,
    key_gain,
    out_weight,
    residual,
    norm_gain,
    expert_gate,
    expert_up,
    expert_down,
    routes,
    route_weight,
):
    _, rows, heads, width = queries.shape
    kv_heads = key_rows.shape[2]
    model = heads * width
    length = rows * n
    experts = expert_gate.shape[0] * n
    capacity = max(2, 4 * (rows // 2) // experts)
    across = max(x for x in range(1, n + 1) if n % x == 0 and x * x <= n)
    depth = n // across
    local_kv, local = kv_heads // across, heads // across
    units = across * local_kv
    slots = 2 * across * capacity
    aside = 2 * (across - 1) * capacity
    w_rows, w_cols = out_weight.shape
    dma = pltpu.SemaphoreType.DMA
    ny = dp // 2
    ff = expert_gate.shape[2]
    attention_scratch = [
        pltpu.VMEM((rows, heads, width), BF16),
        pltpu.VMEM((rows, kv_heads, width), BF16),
        pltpu.VMEM((rows, kv_heads, width), BF16),
        pltpu.VMEM((rows, heads, width), F32),
        pltpu.VMEM((across, 2 * local_kv, rows, width), BF16),
        pltpu.VMEM((across - 1, local, rows, width), BF16),
        pltpu.VMEM((local, across * rows, width), BF16),
        pltpu.VMEM((2 * local_kv, length, width), BF16),
        pltpu.VMEM((w_rows * n, w_cols), BF16),
        pltpu.VMEM((across - 1, rows, local * width), BF16),
        pltpu.VMEM((dp, rows, model), BF16),
        pltpu.VMEM((dp, rows, w_cols), BF16),
        pltpu.VMEM((dp, rows, w_cols), BF16),
        pltpu.VMEM((rows, model), BF16),
        pltpu.VMEM((2, 1, width), F32),
        pltpu.VMEM((1, model), F32),
        dma((8,)),
        dma((1,)),
        dma((across - 1, local_kv)),
        dma((2,)),
        dma((units, depth)),
        dma((1,)),
        dma((1,)),
        dma((2,)),
        dma((2,)),
        dma((3,)),
        dma((2,)),
        dma((4, depth)),
        dma((1,)),
        dma((across - 1, local_kv)),
        dma((1,)),
        dma((max(1, ny - 1), units)),
        dma((2,)),
        dma((2,)),
        dma((1,)),
        dma((dp,)),
    ]
    result = pl.pallas_call(
        functools.partial(layer_kernel, n, dp, capacity),
        out_shape=pltpu.VMEM((rows, model), BF16),
        in_specs=[ANY] * 8 + [VMEM] * 2 + [ANY] * 3,
        out_specs=VMEM,
        scratch_shapes=[
            pltpu.VMEM((rows, model), F32),
            pltpu.VMEM((rows, model + width), BF16),
            *attention_scratch,
            dma((3,)),
            pltpu.VMEM((model, ff), BF16),
            pltpu.VMEM((model, ff), BF16),
            pltpu.VMEM((ff, model), BF16),
            pltpu.VMEM((depth, 8, rows), F32),
            pltpu.VMEM((depth, slots, rows), BF16),
            pltpu.VMEM((depth, rows, slots), BF16),
            pltpu.VMEM((depth, rows, slots), BF16),
            pltpu.VMEM((depth - 1, rows, model + width), BF16),
            pltpu.VMEM((depth, aside, model + width), BF16),
            pltpu.VMEM((depth, slots, model + width), BF16),
            pltpu.VMEM((depth, slots, model), BF16),
            pltpu.VMEM((depth, aside, model), BF16),
            pltpu.VMEM((slots, model), BF16),
            pltpu.VMEM((2, slots, ff), BF16),
            pltpu.VMEM((4, rows, model), BF16),
            pltpu.VMEM((6, rows, model), BF16),
            pltpu.VMEM((rows, model), F32),
            dma((2,)),
            dma((3,)),
            dma((depth - 1, CHUNKS)),
            dma((1,)),
            dma((depth,)),
            dma((1,)),
            dma((depth, CHUNKS)),
            dma((1,)),
            dma((6, CHUNKS)),
        ],
        compiler_params=pltpu.CompilerParams(
            collective_id=0, has_side_effects=True, vmem_limit_bytes=56 * 1024 * 1024
        ),
        name="layer",
    )(
        queries[0],
        key_rows[0],
        values[0],
        query_gain[None],
        key_gain[None],
        out_weight,
        residual[0],
        norm_gain[None],
        routes[0].T,
        route_weight[0].T,
        expert_gate,
        expert_up,
        expert_down,
    )
    return result[None]


def solution(mesh):
    in_specs = (
        P("dp", "sp", None, None),
        P("dp", "sp", None, None),
        P("dp", "sp", None, None),
        P(),
        P(),
        P("sp", "dp"),
        P("dp", "sp", None),
        P(),
        P("sp", None, None),
        P("sp", None, None),
        P("sp", None, None),
        P("dp", "sp", None),
        P("dp", "sp", None),
    )
    out_specs = P("dp", "sp", None)
    return jax.shard_map(
        functools.partial(on_device, mesh.shape["sp"], mesh.shape["dp"]),
        mesh=mesh,
        in_specs=in_specs,
        out_specs=out_specs,
        check_vma=False,
    )
```

```python
import functools
import math

import jax
import jax.numpy as jnp
from jax import lax
from jax.experimental import pallas as pl
from jax.experimental.pallas import tpu as pltpu
from jax.sharding import PartitionSpec as P

GRID_W = 64
EPS = 1e-06
CHUNKS = 4
TILE = 256
THETA = 10000.0
MESH = pl.DeviceIdType.MESH
VMEM = pl.BlockSpec(memory_space=pltpu.VMEM)
ANY = pl.BlockSpec(memory_space=pl.ANY)
F32 = jnp.float32
BF16 = jnp.bfloat16


def rotation_tables(start, rows, width):
    quarter = width // 4
    lane = lax.broadcasted_iota(jnp.int32, (rows, width), 1)
    position = start + lax.broadcasted_iota(jnp.int32, (rows, width), 0)
    place = jnp.where(lane < 2 * quarter, position // GRID_W, position % GRID_W)
    part = lane % (2 * quarter)
    power = (part % quarter).astype(F32) * (-math.log(THETA) / quarter)
    angles = place.astype(F32) * jnp.exp(power)
    sign = jnp.where(part < quarter, -1.0, 1.0).astype(F32)
    return jnp.cos(angles), jnp.sin(angles) * sign


def turn(rows, gain, cosine, sine):
    width = rows.shape[-1]
    quarter = width // 4
    a = rows.astype(F32)
    a = a * lax.rsqrt(jnp.mean(a * a, axis=-1, keepdims=True) + EPS) * gain
    lane = lax.broadcasted_iota(jnp.int32, a.shape, 1) % (2 * quarter)
    partner = jnp.where(
        lane < quarter, pltpu.roll(a, width - quarter, 1), pltpu.roll(a, quarter, 1)
    )
    return (a * cosine + partner * sine).astype(BF16)


class Line:
    def __init__(self, depth, width, block, send, recv):
        self.depth, self.width, self.block = depth, width, block
        self.send, self.recv = send, recv
        me = lax.axis_index("sp")
        self.z, self.x = me // width, me % width

    def copy(self, unit, plane, way, target):
        return pltpu.make_async_remote_copy(
            src_ref=self.block(unit, plane * self.width + self.x),
            dst_ref=self.block(unit, plane * self.width + self.x),
            send_sem=self.send.at[way],
            recv_sem=self.recv.at[unit, plane],
            device_id={"sp": target * self.width + self.x},
            device_id_type=MESH,
        )

    def start(self, condition, unit, plane, way, target):
        @pl.when(condition)
        def _():
            self.copy(unit, plane, way, target).start()

    def up(self, condition, unit, plane):
        self.start(condition & (self.z < self.depth - 1), unit, plane, 0, self.z + 1)

    def down(self, condition, unit, plane):
        self.start(condition & (self.z > 0), unit, plane, 1, self.z - 1)

    def arrive(self, condition, unit, plane):
        @pl.when(condition)
        def _():
            self.copy(unit, plane, 0, plane).wait_recv()

    def step(self, t, unit, condition=True, then=None):
        below = (self.z - t >= 0) & condition
        above = (self.z + t < self.depth) & condition
        self.arrive(below, unit, self.z - t)
        self.up(below, unit, self.z - t)
        if then is not None:
            then(below, unit, self.z - t)
        self.arrive(above, unit, self.z + t)
        self.down(above, unit, self.z + t)
        if then is not None:
            then(above, unit, self.z + t)

    def drain(self, planes):
        for way in range(2):
            for count in range(1, self.depth):
                z = count - 1 if way == 0 else self.depth - count

                @pl.when(self.z == z)
                def _():
                    pltpu.make_async_remote_copy(
                        src_ref=planes(count),
                        dst_ref=planes(count),
                        send_sem=self.send.at[way],
                        recv_sem=self.recv.at[0, 0],
                        device_id={"sp": self.z * self.width + self.x},
                        device_id_type=MESH,
                    ).wait_send()


def selection(table, first_expert, column, columns, capacity):
    rows = table.shape[1]
    few = rows // 2
    slots = columns * 2 * capacity
    slot = lax.broadcasted_iota(jnp.int32, (slots, rows), 0)
    row = lax.broadcasted_iota(jnp.int32, (slots, rows), 1)
    side = (column + slot // (2 * capacity)) % columns
    expert = (first_expert + side).astype(F32)
    same = (slot // capacity) % 2 == row // few
    first = (table[0:1, :] == expert) & same
    second = (table[1:2, :] == expert) & same
    named = jnp.where(first | second, 1.0, 0.0).astype(BF16)
    before = lax.broadcasted_iota(jnp.int32, (rows, rows), 0)
    after = lax.broadcasted_iota(jnp.int32, (rows, rows), 1)
    earlier = jnp.where(before < after, 1.0, 0.0).astype(BF16)
    rank = jnp.dot(named, earlier, preferred_element_type=F32)
    here = rank == (slot % capacity).astype(F32)
    choice = jnp.where((first | second) & here, 1.0, 0.0)
    weight = jnp.where(first & here, table[2:3, :], 0.0)
    weight = weight + jnp.where(second & here, table[3:4, :], 0.0)
    weight = weight.T
    high = weight.astype(BF16)
    low = (weight - high.astype(F32)).astype(BF16)
    return choice.astype(BF16), high, low


def attention_part(
    n,
    dp,
    start_loads,
    q_ref,
    k_ref,
    v_ref,
    qg_ref,
    kg_ref,
    w_ref,
    res_ref,
    ng_ref,
    mixed_ref,
    normed_ref,
    experts,
    q_in,
    k_in,
    v_in,
    wide,
    stage,
    q_stage,
    q_all,
    kv,
    w_full,
    swap,
    att,
    total,
    proj,
    back,
    res_in,
    gains,
    norm_in,
    in_sem,
    kvx_send,
    kvx_recv,
    kvz_send,
    kvz_recv,
    qx_send,
    qx_recv,
    wx_send,
    wx_recv,
    wo_sem,
    wz_send,
    wz_recv,
    ax_send,
    ax_recv,
    y_send,
    y_recv,
    pair_sem,
    fwd_sem,
    back_send,
    back_recv,
):
    me = lax.axis_index("sp")
    mine = lax.axis_index("dp")
    rows, heads, width = q_ref.shape
    kv_heads = k_ref.shape[1]
    group = heads // kv_heads
    model = heads * width
    across = stage.shape[0]
    depth = n // across
    local_kv = kv_heads // across
    local = heads // across
    z, x = me // across, me % across
    always = me >= 0
    ny = dp // 2
    core = mine % 2
    row_y = mine // 2
    partner = row_y * 2 + 1 - core
    w_rows, w_cols = w_ref.shape

    def span(start, size):
        return pl.ds(pl.multiple_of(start * size, size), size)

    fetches = [
        pltpu.make_async_copy(src, dst, in_sem.at[i])
        for i, (src, dst) in enumerate(
            (
                (k_ref, k_in),
                (v_ref, v_in),
                (kg_ref, gains.at[0]),
                (q_ref, q_in),
                (qg_ref, gains.at[1]),
                (w_ref, w_full.at[span(me, w_rows)]),
                (res_ref, res_in),
                (ng_ref, norm_in),
            )
        )
    ]
    for fetch in fetches:
        fetch.start()
    barrier = pltpu.get_barrier_semaphore()
    for d in range(1, n):
        pl.semaphore_signal(
            barrier, inc=1, device_id={"sp": lax.rem(me + d, n)}, device_id_type=MESH
        )
    for d in range(1, dp):
        pl.semaphore_signal(
            barrier, inc=1, device_id={"dp": lax.rem(mine + d, dp)}, device_id_type=MESH
        )

    cosine, sine = rotation_tables(me * rows, rows, width)
    my_rows = span(me, rows)
    for fetch in fetches[:3]:
        fetch.wait()
    for part, source in ((0, k_in), (1, v_in)):
        wide[:, 0:kv_heads, :] = source[...].astype(F32)
        for g in range(kv_heads):
            lines = wide[:, g, :]
            slot = 2 * (g % local_kv) + part
            if part == 0:
                lines = turn(lines, gains[0], cosine, sine)
            stage[g // local_kv, slot] = lines.astype(BF16)
    for c in range(2 * local_kv):
        kv[c, my_rows, :] = stage[x, c]
    pl.semaphore_wait(barrier, n - 1 + dp - 1)

    def remote(src, dst, send, recv, **device):
        return pltpu.make_async_remote_copy(
            src_ref=src,
            dst_ref=dst,
            send_sem=send,
            recv_sem=recv,
            device_id=device,
            device_id_type=MESH,
        )

    def beside(k):
        return z * across + lax.rem(x + k, across)

    def kv_block(g, sp):
        return kv.at[pl.ds(2 * g, 2), span(sp, rows), :]

    kv_units = [(k, g) for g in range(local_kv) for k in range(across)]
    own_units = [u for u, (k, _) in enumerate(kv_units) if k == 0]

    def kv_unit(u, sp):
        k, g = kv_units[u]
        return kv_block(g, sp - sp % across + lax.rem(sp % across + k, across))

    halves = 2
    w_units = [(j, k) for j in range(halves) for k in range(2)]
    part_rows, part_cols = w_rows // 2, w_cols // halves

    def w_unit(u, sp):
        j, k = w_units[u]
        start = pl.multiple_of(sp * w_rows + k * part_rows, part_rows)
        return w_full.at[pl.ds(start, part_rows), pl.ds(j * part_cols, part_cols)]

    kv_line = Line(depth, across, kv_unit, kvz_send, kvz_recv)
    w_line = Line(depth, across, w_unit, wz_send, wz_recv)
    kvx, qx, ax = {}, {}, {}
    for g in range(local_kv):
        for k in range(1, across):
            kvx[k, g] = remote(
                stage.at[lax.rem(x + k, across), pl.ds(2 * g, 2)],
                kv_block(g, me),
                kvx_send.at[0],
                kvx_recv.at[across - k - 1, g],
                sp=beside(k),
            )
            kvx[k, g].start()
        kv_line.up(always, own_units[g], z)
        kv_line.down(always, own_units[g], z)

    start_loads()
    fetches[3].wait()
    fetches[4].wait()
    for h in range(0, heads, 8):
        wide[:, h : h + 8, :] = q_in[:, h : h + 8, :].astype(F32)
    for k in list(range(1, across)) + [0]:
        first = lax.rem(x + k, across) * local

        def turn_head(i, carry):
            lines = turn(wide[:, pl.ds(first + i, 1), :].reshape(rows, width), gains[1], cosine, sine)
            if k == 0:
                q_all[i, 0:rows] = lines
            else:
                q_stage[k - 1, i] = lines
            return carry

        lax.fori_loop(0, local, turn_head, 0)
        if k > 0:
            qx[k] = remote(
                q_stage.at[k - 1],
                q_all.at[:, pl.ds((across - k) * rows, rows), :],
                qx_send.at[0],
                qx_recv.at[0],
                sp=beside(k),
            )
            qx[k].start()
        if k == across - 1:
            for u, (kk, g) in enumerate(kv_units):
                if kk == 0:
                    continue
                remote(
                    stage.at[0, pl.ds(2 * g, 2)],
                    kv_block(g, beside(kk)),
                    kvx_send.at[0],
                    kvx_recv.at[kk - 1, g],
                    sp=me,
                ).wait_recv()
                kv_line.up(always, u, z)
                kv_line.down(always, u, z)
    fetches[5].wait()

    far = depth - 1 - z

    def is_far(plane):
        return jnp.where(plane == far, 1, 0)

    def w_across(condition, u, plane):
        for k in range(1, across):

            @pl.when(condition)
            def _():
                remote(
                    w_unit(u, plane * across + x),
                    w_unit(u, plane * across + x),
                    wx_send.at[w_units[u][0]],
                    wx_recv.at[w_units[u][0], is_far(plane)] if plane is not z else wo_sem.at[0],
                    sp=beside(k),
                ).start()

    upper = z // (depth // 2)
    way = 1 - 2 * upper

    def block_of(i, step):
        row = lax.rem(row_y + ny + step * (i // 2), ny)
        return row * 2 + (core if i % 2 == 0 else 1 - core)

    middle = (z > 0) & (z < depth - 1)
    edge = jnp.logical_not(middle)

    def w_half(sp, j):
        return w_full.at[span(sp, w_rows), pl.ds(j * part_cols, part_cols)]

    def w_along():
        block = w_full.at[pl.ds(0, (across - 1) * w_rows)]
        remote(block, block, wo_sem.at[1], wo_sem.at[0], sp=me).wait_recv()
        for j in range(halves):
            for k in range(1, across):
                block = w_half(beside(k), j)
                target = me + way * across
                inner = jnp.where(middle, 1, 0)
                remote(block, block, wo_sem.at[1], wx_recv.at[j, inner], sp=target).start()

    def w_back():
        @pl.when(middle)
        def _():
            for k in range(1, across):
                block = w_half(beside(k), 0)
                target = me - way * across
                remote(block, block, wo_sem.at[2], wx_recv.at[0, 0], sp=target).start()

    def w_aside(units):
        def then(condition, u, plane):
            if w_units[u][0] in units:
                w_across(condition, u, plane)

        return then

    def w_begin(t):
        for u in range(len(w_units)):
            w_line.up(z == t, u, z)
            w_line.down(depth - 1 - z == t, u, z)

    w_begin(0)
    experts.prepare(0)
    for u in range(len(w_units)):
        w_across(always, u, z)
    for t in range(1, depth - 1):
        for u in range(len(kv_units)):
            kv_line.step(t, u)
        w_begin(t)
    experts.prepare(1)
    remote(
        q_stage,
        q_all.at[:, pl.ds(rows, (across - 1) * rows), :],
        qx_send.at[0],
        qx_recv.at[0],
        sp=me,
    ).wait_recv()

    scale = width ** (-0.5)
    wide_group = group * width

    def att_cols(k, g):
        side = lax.rem(x + k, across)
        start = (side * local_kv + g) * wide_group
        return pl.ds(pl.multiple_of(start, wide_group), wide_group)

    def spread_att(u):
        k, g = kv_units[u]
        block = att.at[mine, :, att_cols(k, g)]
        for j in range(1, ny):
            target = lax.rem(row_y + j, ny) * 2 + core
            remote(block, block, y_send.at[0], y_recv.at[j - 1, u], dp=target).start()
        remote(block, block, pair_sem.at[0], pair_sem.at[1], dp=partner).start()

    def forward(u):
        for j in range(1, ny):
            source = lax.rem(row_y + ny - j, ny) * 2 + core
            remote(
                att.at[mine, :, att_cols(*kv_units[u])],
                att.at[mine, :, att_cols(*kv_units[u])],
                y_send.at[0],
                y_recv.at[j - 1, u],
                dp=mine,
            ).wait_recv()
            block = att.at[source, :, att_cols(*kv_units[u])]
            remote(block, block, fwd_sem.at[0], fwd_sem.at[1], dp=partner).start()

    for g in range(local_kv):
        for u, (_, gg) in enumerate(kv_units):
            if gg == g:
                kv_line.step(depth - 1, u)
        if g == local_kv - 1:
            for u in range(len(w_units)):
                w_line.step(1, u, middle)
            w_along()

        def one_head(i, carry):
            h = g * group + i
            scores = (
                lax.dot_general(
                    q_all[h], kv[2 * g], (((1,), (1,)), ((), ())), preferred_element_type=F32
                )
                * scale
            )
            exponent = jnp.exp(scores - jnp.max(scores, axis=-1, keepdims=True))
            weights = (exponent / jnp.sum(exponent, axis=-1, keepdims=True)).astype(BF16)
            out = jnp.dot(weights, kv[2 * g + 1], preferred_element_type=F32).astype(BF16)
            cols = pl.ds(pl.multiple_of((x * local + h) * width, width), width)
            att[mine, :, cols] = out[0:rows]
            cols = pl.ds(pl.multiple_of(h * width, width), width)
            for k in range(1, across):
                swap[k - 1, :, cols] = out[k * rows : (k + 1) * rows]
            return carry

        lax.fori_loop(0, group, one_head, 0)
        for k in range(1, across):
            ax[k, g] = remote(
                swap.at[k - 1, :, pl.ds(g * wide_group, wide_group)],
                att.at[mine, :, att_cols(0, g)],
                ax_send.at[0],
                ax_recv.at[across - k - 1, g],
                sp=beside(k),
            )
            ax[k, g].start()
        spread_att(own_units[g])
    for t in range(2, depth - 1):
        for u in range(len(w_units)):
            w_line.step(t, u, middle, w_across)
    w_back()
    for u in range(len(w_units)):
        w_line.step(1, u, edge, w_aside((1,)))
    for u, (k, g) in enumerate(kv_units):
        if k == 0:
            continue
        remote(
            swap.at[0, :, pl.ds(g * wide_group, wide_group)],
            att.at[mine, :, att_cols(k, g)],
            ax_send.at[0],
            ax_recv.at[k - 1, g],
            sp=me,
        ).wait_recv()
        spread_att(u)
    for t in range(2, depth - 1):
        for u in range(len(w_units)):
            w_line.step(t, u, edge, w_across)
    order = own_units + [u for u in range(len(kv_units)) if u not in own_units]
    for i in range(max(len(order), len(w_units))):
        if i < len(w_units):
            w_line.step(depth - 1, i, True, w_across)
        if i < len(order):
            forward(order[i])
    if ny > 1:
        remote(
            att.at[pl.ds(0, ny - 1)],
            att.at[pl.ds(0, ny - 1)],
            fwd_sem.at[0],
            fwd_sem.at[1],
            dp=mine,
        ).wait_recv()
    remote(att.at[mine], att.at[mine], pair_sem.at[0], pair_sem.at[1], dp=mine).wait_recv()

    deep = across * w_rows

    def project(place, cols):
        lines = pl.ds(pl.multiple_of(place * deep, deep), deep)
        return jnp.dot(
            att[:, :, lines].reshape(dp * rows, deep),
            w_full[lines, cols],
            preferred_element_type=F32,
        )

    def w_wait(j, planes, which):
        block = w_full.at[
            pl.ds(0, planes * (across - 1) * w_rows), pl.ds(j * part_cols, part_cols)
        ]
        remote(block, block, wx_send.at[0], wx_recv.at[j, which], sp=me).wait_recv()

    for j in range(halves):
        cols = slice(j * part_cols, (j + 1) * part_cols)
        w_wait(j, depth - 2, 0)
        total[:, cols] = project(lax.rem(far + 1, depth), cols)
        for step in range(2, depth):
            total[:, cols] += project(lax.rem(far + step, depth), cols)
    for j in range(halves):
        cols = slice(j * part_cols, (j + 1) * part_cols)
        w_wait(j, 1, 1)
        result = (total[:, cols] + project(far, cols)).astype(BF16)
        for s in range(dp):
            proj[s, :, cols] = result[s * rows : (s + 1) * rows]
        back[mine, :, cols] = proj[mine, :, cols]
        for i in list(range(2, dp)) + [1]:
            target = block_of(i, 1)
            remote(
                proj.at[target, :, cols],
                back.at[mine, :, cols],
                back_send.at[0],
                back_recv.at[i],
                dp=target,
            ).start()

    fetches[6].wait()
    fetches[7].wait()
    square = jnp.zeros((rows, 1), F32)
    each = dp // CHUNKS
    for i in range(dp):
        source = block_of(i, -1)
        if i > 0:
            remote(back.at[mine], back.at[source], back_send.at[0], back_recv.at[i], dp=mine).wait_recv()
        cols = span(source, w_cols)
        part = res_in[:, cols].astype(F32) + back[source].astype(F32)
        mixed_ref[:, cols] = part
        square = square + jnp.sum(part * part, axis=-1, keepdims=True)
        normed_ref[:, i * w_cols : (i + 1) * w_cols] = part.astype(BF16)
        if i == dp - 1:
            factor = lax.rsqrt(square / model + EPS)
            high = factor.astype(BF16).astype(F32)
            mid = (factor - high).astype(BF16).astype(F32)
            lane = lax.broadcasted_iota(jnp.int32, (rows, width), 1)
            pieces = jnp.where(lane == 0, high, jnp.where(lane == 1, mid, 0.0))
            pieces = jnp.where(lane == 2, factor - high - mid, pieces)
            normed_ref[:, model : model + width] = pieces.astype(BF16)
        if i % each == each - 1:
            experts.launch(i // each)
        if i == dp // 2 - 1:
            experts.early()

    def drain():
        kv_line.drain(lambda count: kv.at[:, pl.ds(0, count * across * rows), :])
        w_line.drain(lambda count: w_full.at[pl.ds(0, count * w_rows)])
        for role, counts in ((edge, (depth - 1, depth)), (middle, (2, 2))):

            @pl.when(role)
            def _():
                for j, count in enumerate(counts):
                    block = w_full.at[
                        pl.ds(0, count * (across - 1) * w_rows), pl.ds(0, part_cols)
                    ]
                    remote(block, block, wx_send.at[j], back_recv.at[0], sp=me).wait_send()

        @pl.when(middle)
        def _():
            block = w_full.at[pl.ds(0, (across - 1) * w_rows), pl.ds(0, part_cols)]
            remote(block, block, wo_sem.at[2], back_recv.at[0], sp=me).wait_send()

        whole = [
            (w_full.at[pl.ds(0, (across - 1) * w_rows)], wo_sem.at[1]),
            (stage.at[pl.ds(0, across - 1)], kvx_send.at[0]),
            (q_stage, qx_send.at[0]),
            (swap, ax_send.at[0]),
            (att.at[mine], pair_sem.at[0]),
            (proj.at[pl.ds(0, dp - 1)], back_send.at[0]),
        ]
        if ny > 1:
            whole.append((att.at[pl.ds(0, ny - 1)], y_send.at[0]))
            whole.append((att.at[pl.ds(0, ny - 1)], fwd_sem.at[0]))
        for block, sem in whole:
            remote(block, block, sem, back_recv.at[0], sp=me).wait_send()

    return drain


class Experts:
    def __init__(self, n, dp, capacity, norm, routes, gates, middle, loads, out, *refs):
        (
            self.gate,
            self.up,
            self.down,
            self.tables,
            self.pick,
            self.high,
            self.low,
            self.column,
            self.asked,
            self.served,
            self.answer,
            self.given,
            self.ready,
            self.hidden,
            self.partial,
            self.incoming,
            self.hold,
            self.table_sem,
            self.column_send,
            self.column_recv,
            self.ask_send,
            self.ask_recv,
            self.give_send,
            self.give_recv,
            self.part_send,
            self.part_recv,
        ) = refs
        self.mixed, self.normed = middle
        self.routes, self.gates = routes, gates
        self.loads, self.out = loads, out
        me = lax.axis_index("sp")
        self.columns = max(x for x in range(1, n + 1) if n % x == 0 and x * x <= n)
        self.depth = n // self.columns
        self.z, self.x = me // self.columns, me % self.columns
        self.upper = self.z // (self.depth // 2)
        self.way = 1 - 2 * self.upper
        self.inner = self.upper * (self.depth - 1) + self.way * self.z
        self.capacity = capacity
        self.norm, self.dp = norm, dp
        self.rows, self.model = self.mixed.shape
        self.width = self.model // CHUNKS
        self.share = 2 * capacity

    def role(self, inner):
        return self.inner == inner

    def plane(self, r):
        place = (self.inner, 1 - self.inner, self.depth - 1, self.depth - 2)[r]
        return self.upper * (self.depth - 1) + self.way * place

    def remote(self, src, dst, send, recv, target):
        return pltpu.make_async_remote_copy(
            src_ref=src,
            dst_ref=dst,
            send_sem=send,
            recv_sem=recv,
            device_id={"sp": target},
            device_id_type=MESH,
        )

    def at(self, step):
        return (self.z + step) * self.columns + self.x

    def beside(self, k):
        return self.z * self.columns + (self.x + k) % self.columns

    def lanes(self, c):
        end = (c + 1) * self.width if c < CHUNKS - 1 else self.normed.shape[1]
        return slice(c * self.width, end)

    def early(self):
        @pl.when(self.role(0))
        def _():
            for c in range(CHUNKS // 2):
                self.ask(0, 1, c)

    def launch(self, c):
        self.column_copy("forth", c).start()

        @pl.when(self.role(1))
        def _():
            self.column_copy("back", c).start()

    def cols(self, c):
        return slice(c * self.width, (c + 1) * self.width)

    def tables_all(self):
        block = self.tables.at[pl.ds(0, self.depth - 1)]
        return self.remote(block, block, self.table_sem.at[0], self.table_sem.at[1], self.at(0))

    def prepare(self, phase):
        planes = self.depth

        def table_copy(d):
            target = (self.z + d) % planes
            return self.remote(
                self.tables.at[self.z],
                self.tables.at[self.z],
                self.table_sem.at[0],
                self.table_sem.at[1],
                target * self.columns + self.x,
            )

        if phase == 0:
            rows = self.rows
            self.tables[self.z] = jnp.concatenate(
                [self.routes[...].astype(F32), self.gates[...], jnp.zeros((4, rows), F32)], axis=0
            )
            for d in range(1, planes):
                table_copy(d).start()
            return
        self.tables_all().wait_recv()
        for r in range(planes):
            choice, high, low = selection(
                self.tables[self.plane(r)],
                self.z * self.columns,
                self.x,
                self.columns,
                self.capacity,
            )
            self.pick[r] = choice
            self.high[r] = high
            self.low[r] = low

    def column_copy(self, kind, c):
        source, place, step = {
            "forth": (None, None, 1),
            "back": (None, 1, -1),
            1: (1, 2, 1),
            2: (2, 2, -1),
            3: (3, 3, -1),
        }[kind]
        cols = self.lanes(c)
        src = self.normed.at[:, cols] if source is None else self.column.at[source - 1, :, cols]
        if place is None:
            place = 1 + 2 * self.inner
        index = {"forth": 0, "back": 1}.get(kind, 2)
        return self.remote(
            src,
            self.column.at[place - 1, :, cols],
            self.column_send.at[index],
            self.column_recv.at[place - 1, c],
            self.at(step * self.way),
        )

    def column_arrive(self, r, c):
        cols = self.lanes(c)
        self.remote(
            self.column.at[r - 1, :, cols],
            self.column.at[r - 1, :, cols],
            self.column_send.at[0],
            self.column_recv.at[r - 1, c],
            self.at(0),
        ).wait_recv()

    def ask_copy(self, r, c, k):
        cols = self.lanes(c)
        return self.remote(
            self.asked.at[r, pl.ds((k - 1) * self.share, self.share), cols],
            self.served.at[r, pl.ds((self.columns - k) * self.share, self.share), cols],
            self.ask_send.at[0],
            self.ask_recv.at[r],
            self.beside(k),
        )

    def give_copy(self, r, c, k):
        cols = self.cols(c)
        return self.remote(
            self.given.at[r, pl.ds((k - 1) * self.share, self.share), cols],
            self.answer.at[r, pl.ds((self.columns - k) * self.share, self.share), cols],
            self.give_send.at[0],
            self.give_recv.at[r, c],
            self.beside(k),
        )

    def ask(self, inner, r, c):
        cols = self.lanes(c)
        if r > 0:
            self.column_arrive(r, c)
            if inner == 1:
                self.column_copy(r, c).start()
        lines = self.normed[:, cols] if r == 0 else self.column[r - 1, :, cols]
        chosen = jnp.dot(self.pick[r], lines, preferred_element_type=F32).astype(BF16)
        self.served[r, 0 : self.share, cols] = chosen[0 : self.share]
        for k in range(1, self.columns):
            part = slice((k - 1) * self.share, k * self.share)
            self.asked[r, part, cols] = chosen[k * self.share : (k + 1) * self.share]
            self.ask_copy(r, c, k).start()

    def serve_up(self, r, first=False):
        block = self.asked.at[r]
        self.remote(
            block, block, self.ask_send.at[0], self.ask_recv.at[r], self.at(0)
        ).wait_recv()
        if first:
            self.loads[0].wait()
            self.loads[1].wait()

        pieces = self.served[r, :, self.model :].astype(F32)
        factor = jnp.sum(pieces, axis=-1, keepdims=True)
        mine = lax.axis_index("dp")
        size = self.model // self.dp
        for i in range(self.dp):
            row = (mine // 2 + self.dp // 2 - i // 2) % (self.dp // 2)
            block = row * 2 + (mine % 2 if i % 2 == 0 else 1 - mine % 2)
            cols = pl.ds(pl.multiple_of(block * size, size), size)
            lines = self.served[r, :, i * size : (i + 1) * size].astype(F32)
            self.ready[:, cols] = (lines * factor * self.norm[:, cols]).astype(BF16)

        def up_tile(t, carry):
            cols = pl.ds(pl.multiple_of(t * TILE, TILE), TILE)
            lines = self.ready[...]
            gate = jnp.dot(lines, self.gate[:, cols], preferred_element_type=F32)
            up = jnp.dot(lines, self.up[:, cols], preferred_element_type=F32)
            self.hidden[min(r, 1), :, cols] = (gate / (1.0 + jnp.exp(-gate)) * up).astype(BF16)
            return carry

        lax.fori_loop(0, self.gate.shape[1] // TILE, up_tile, 0)

    def serve_down(self, r, c, first=False):
        if first:
            self.loads[2].wait()

        def down_tile(t, carry):
            cols = pl.ds(pl.multiple_of(c * self.width + t * TILE, TILE), TILE)
            lines = jnp.dot(
                self.hidden[min(r, 1)], self.down[:, cols], preferred_element_type=F32
            ).astype(BF16)
            self.answer[r, 0 : self.share, cols] = lines[0 : self.share]
            self.given[r, :, cols] = lines[self.share :]
            return carry

        lax.fori_loop(0, self.width // TILE, down_tile, 0)
        for k in range(1, self.columns):
            self.give_copy(r, c, k).start()

    def combine(self, r, c):
        block = self.given.at[r, :, self.cols(c)]
        self.remote(
            block, block, self.give_send.at[0], self.give_recv.at[r, c], self.at(0)
        ).wait_recv()
        lines = self.answer[r, :, self.cols(c)]
        return jnp.dot(self.high[r], lines, preferred_element_type=F32) + jnp.dot(
            self.low[r], lines, preferred_element_type=F32
        )

    def part_copy(self, slot, place, step, c):
        cols = self.cols(c)
        return self.remote(
            self.partial.at[slot, :, cols],
            self.incoming.at[place, :, cols],
            self.part_send.at[0],
            self.part_recv.at[place, c],
            self.at(step * self.way),
        )

    def part_arrive(self, place, c):
        cols = self.cols(c)
        self.remote(
            self.partial.at[0, :, cols],
            self.incoming.at[place, :, cols],
            self.part_send.at[0],
            self.part_recv.at[place, c],
            self.at(0),
        ).wait_recv()
        return self.incoming[place, :, cols].astype(F32)

    def merge(self, r, c, slot, place, step, feed=None):
        total = self.combine(r, c)
        if feed is not None:
            total = total + self.part_arrive(feed, c)
        self.partial[slot, :, self.cols(c)] = total.astype(BF16)
        self.part_copy(slot, place, step, c).start()

    def own(self, c):
        cols = self.cols(c)
        self.hold[:, cols] = self.mixed[:, cols] + self.combine(0, c)

    def finish(self, c, places):
        cols = self.cols(c)
        total = self.hold[:, cols]
        for place in places:
            total = total + self.part_arrive(place, c)
        self.out[:, cols] = total.astype(BF16)

    def edge(self):
        chunks = range(CHUNKS)
        ask = functools.partial(self.ask, 0)

        def toward(r, c):
            self.merge(r, c, r - 1, r - 1, 1)

        def down(r, *cs):
            for c in cs:
                self.serve_down(r, c, r == 1 and c == 0)

        for c in range(CHUNKS // 2, CHUNKS):
            ask(1, c)
        for c in chunks:
            ask(0, c)
        self.serve_up(1, True)
        down(1, *chunks)
        ask(2, 0)
        toward(1, 0)
        ask(2, 1)
        toward(1, 1)
        toward(1, 2)
        ask(2, 2)
        toward(1, 3)
        ask(2, 3)
        ask(3, 0)
        ask(3, 1)
        self.serve_up(0)
        ask(3, 2)
        self.serve_up(2)
        down(2, *chunks)
        ask(3, 3)
        for c in chunks:
            toward(2, c)
        down(0, 0, 1)
        self.serve_up(3)
        down(3, *chunks)
        toward(3, 0)
        down(0, 2, 3)
        for c in range(1, CHUNKS):
            toward(3, c)
        for c in chunks:
            self.own(c)
        for c in chunks:
            self.finish(c, (5,))

    def inside(self):
        chunks = range(CHUNKS)
        ask = functools.partial(self.ask, 1)

        def down(r, *cs):
            for c in cs:
                self.serve_down(r, c, r == 1 and c == 0)

        for c in chunks:
            ask(0, c)
        ask(3, 0)
        ask(3, 1)
        ask(1, 0)
        ask(1, 1)
        ask(2, 0)
        ask(1, 2)
        ask(2, 1)
        ask(1, 3)
        ask(2, 2)
        ask(2, 3)
        ask(3, 2)
        ask(3, 3)
        for r in (1, 2, 3):
            self.serve_up(r, r == 1)
            down(r, *chunks)
        self.serve_up(0)

        def far(c):
            self.merge(2, c, 1, 3, 1, 1)

        def near(c):
            self.merge(1, c, 3, 5, -1, 3)

        for c in chunks:
            far(c)
        down(0, *chunks)
        for c in chunks:
            near(c)
        for c in chunks:
            self.own(c)
        for c in chunks:
            self.merge(3, c, 2, 4, 1, 2)
        for c in chunks:
            self.finish(c, (0, 4))

    def run(self):
        pl.when(self.role(0))(self.edge)
        pl.when(self.role(1))(self.inside)
        ends = [
            (self.normed, self.column_send.at[0]),
            (self.asked, self.ask_send.at[0]),
            (self.given, self.give_send.at[0]),
            (self.partial.at[pl.ds(0, 3)], self.part_send.at[0]),
        ]
        for block, sem in ends:
            self.remote(block, block, sem, self.part_recv.at[0, 0], self.at(0)).wait_send()

        @pl.when(self.role(1))
        def _():
            for block, way in ((self.normed, 1), (self.column, 2)):
                self.remote(
                    block, block, self.column_send.at[way], self.part_recv.at[0, 0], self.at(0)
                ).wait_send()

        self.tables_all().wait_send()


def layer_kernel(n, dp, capacity, *refs):
    inputs, refs = refs[:10], refs[10:]
    weights, out_ref, refs = refs[:3], refs[3], refs[4:]
    middle, refs = refs[:2], refs[2:]
    attention, refs = refs[:37], refs[37:]
    load_sem, stores = refs[0], refs[1:4]
    loads = [
        pltpu.make_async_copy(src.at[0], dst, load_sem.at[i])
        for i, (src, dst) in enumerate(zip(weights, stores))
    ]

    def start_loads():
        for load in loads:
            load.start()

    norm = attention[16]
    experts = Experts(n, dp, capacity, norm, *inputs[8:], middle, loads, out_ref, *refs[1:])
    drain = attention_part(n, dp, start_loads, *inputs[:8], *middle, experts, *attention)
    experts.run()
    drain()


def on_device(
    n,
    dp,
    queries,
    key_rows,
    values,
    query_gain,
    key_gain,
    out_weight,
    residual,
    norm_gain,
    expert_gate,
    expert_up,
    expert_down,
    routes,
    route_weight,
):
    _, rows, heads, width = queries.shape
    kv_heads = key_rows.shape[2]
    model = heads * width
    length = rows * n
    experts = expert_gate.shape[0] * n
    capacity = max(2, 4 * (rows // 2) // experts)
    across = max(x for x in range(1, n + 1) if n % x == 0 and x * x <= n)
    depth = n // across
    local_kv, local = kv_heads // across, heads // across
    units = across * local_kv
    slots = 2 * across * capacity
    aside = 2 * (across - 1) * capacity
    w_rows, w_cols = out_weight.shape
    dma = pltpu.SemaphoreType.DMA
    ny = dp // 2
    ff = expert_gate.shape[2]
    attention_scratch = [
        pltpu.VMEM((rows, heads, width), BF16),
        pltpu.VMEM((rows, kv_heads, width), BF16),
        pltpu.VMEM((rows, kv_heads, width), BF16),
        pltpu.VMEM((rows, heads, width), F32),
        pltpu.VMEM((across, 2 * local_kv, rows, width), BF16),
        pltpu.VMEM((across - 1, local, rows, width), BF16),
        pltpu.VMEM((local, across * rows, width), BF16),
        pltpu.VMEM((2 * local_kv, length, width), BF16),
        pltpu.VMEM((w_rows * n, w_cols), BF16),
        pltpu.VMEM((across - 1, rows, local * width), BF16),
        pltpu.VMEM((dp, rows, model), BF16),
        pltpu.VMEM((dp * rows, w_cols), F32),
        pltpu.VMEM((dp, rows, w_cols), BF16),
        pltpu.VMEM((dp, rows, w_cols), BF16),
        pltpu.VMEM((rows, model), BF16),
        pltpu.VMEM((2, 1, width), F32),
        pltpu.VMEM((1, model), F32),
        dma((8,)),
        dma((1,)),
        dma((across - 1, local_kv)),
        dma((2,)),
        dma((units, depth)),
        dma((1,)),
        dma((1,)),
        dma((2,)),
        dma((2, 2)),
        dma((3,)),
        dma((2,)),
        dma((4, depth)),
        dma((1,)),
        dma((across - 1, local_kv)),
        dma((1,)),
        dma((max(1, ny - 1), units)),
        dma((2,)),
        dma((2,)),
        dma((1,)),
        dma((dp,)),
    ]
    result = pl.pallas_call(
        functools.partial(layer_kernel, n, dp, capacity),
        out_shape=pltpu.VMEM((rows, model), BF16),
        in_specs=[ANY] * 8 + [VMEM] * 2 + [ANY] * 3,
        out_specs=VMEM,
        scratch_shapes=[
            pltpu.VMEM((rows, model), F32),
            pltpu.VMEM((rows, model + width), BF16),
            *attention_scratch,
            dma((3,)),
            pltpu.VMEM((model, ff), BF16),
            pltpu.VMEM((model, ff), BF16),
            pltpu.VMEM((ff, model), BF16),
            pltpu.VMEM((depth, 8, rows), F32),
            pltpu.VMEM((depth, slots, rows), BF16),
            pltpu.VMEM((depth, rows, slots), BF16),
            pltpu.VMEM((depth, rows, slots), BF16),
            pltpu.VMEM((depth - 1, rows, model + width), BF16),
            pltpu.VMEM((depth, aside, model + width), BF16),
            pltpu.VMEM((depth, slots, model + width), BF16),
            pltpu.VMEM((depth, slots, model), BF16),
            pltpu.VMEM((depth, aside, model), BF16),
            pltpu.VMEM((slots, model), BF16),
            pltpu.VMEM((2, slots, ff), BF16),
            pltpu.VMEM((4, rows, model), BF16),
            pltpu.VMEM((6, rows, model), BF16),
            pltpu.VMEM((rows, model), F32),
            dma((2,)),
            dma((3,)),
            dma((depth - 1, CHUNKS)),
            dma((1,)),
            dma((depth,)),
            dma((1,)),
            dma((depth, CHUNKS)),
            dma((1,)),
            dma((6, CHUNKS)),
        ],
        compiler_params=pltpu.CompilerParams(
            collective_id=0, has_side_effects=True, vmem_limit_bytes=56 * 1024 * 1024
        ),
        name="layer",
    )(
        queries[0],
        key_rows[0],
        values[0],
        query_gain[None],
        key_gain[None],
        out_weight,
        residual[0],
        norm_gain[None],
        routes[0].T,
        route_weight[0].T,
        expert_gate,
        expert_up,
        expert_down,
    )
    return result[None]


def solution(mesh):
    in_specs = (
        P("dp", "sp", None, None),
        P("dp", "sp", None, None),
        P("dp", "sp", None, None),
        P(),
        P(),
        P("sp", "dp"),
        P("dp", "sp", None),
        P(),
        P("sp", None, None),
        P("sp", None, None),
        P("sp", None, None),
        P("dp", "sp", None),
        P("dp", "sp", None),
    )
    out_specs = P("dp", "sp", None)
    return jax.shard_map(
        functools.partial(on_device, mesh.shape["sp"], mesh.shape["dp"]),
        mesh=mesh,
        in_specs=in_specs,
        out_specs=out_specs,
        check_vma=False,
    )
```

```python
import functools
import math

import jax
import jax.numpy as jnp
from jax import lax
from jax.experimental import pallas as pl
from jax.experimental.pallas import tpu as pltpu
from jax.sharding import PartitionSpec as P

GRID_W = 64
EPS = 1e-06
CHUNKS = 4
TILE = 256
THETA = 10000.0
MESH = pl.DeviceIdType.MESH
VMEM = pl.BlockSpec(memory_space=pltpu.VMEM)
ANY = pl.BlockSpec(memory_space=pl.ANY)
F32 = jnp.float32
BF16 = jnp.bfloat16


def rotation_tables(start, rows, width):
    quarter = width // 4
    lane = lax.broadcasted_iota(jnp.int32, (rows, width), 1)
    position = start + lax.broadcasted_iota(jnp.int32, (rows, width), 0)
    place = jnp.where(lane < 2 * quarter, position // GRID_W, position % GRID_W)
    part = lane % (2 * quarter)
    power = (part % quarter).astype(F32) * (-math.log(THETA) / quarter)
    angles = place.astype(F32) * jnp.exp(power)
    sign = jnp.where(part < quarter, -1.0, 1.0).astype(F32)
    return jnp.cos(angles), jnp.sin(angles) * sign


def turn(rows, gain, cosine, sine):
    width = rows.shape[-1]
    quarter = width // 4
    a = rows.astype(F32)
    a = a * lax.rsqrt(jnp.mean(a * a, axis=-1, keepdims=True) + EPS) * gain
    lane = lax.broadcasted_iota(jnp.int32, a.shape, 1) % (2 * quarter)
    partner = jnp.where(
        lane < quarter, pltpu.roll(a, width - quarter, 1), pltpu.roll(a, quarter, 1)
    )
    return (a * cosine + partner * sine).astype(BF16)


class Line:
    def __init__(self, depth, width, block, send, recv):
        self.depth, self.width, self.block = depth, width, block
        self.send, self.recv = send, recv
        me = lax.axis_index("sp")
        self.z, self.x = me // width, me % width

    def copy(self, unit, plane, way, target):
        return pltpu.make_async_remote_copy(
            src_ref=self.block(unit, plane * self.width + self.x),
            dst_ref=self.block(unit, plane * self.width + self.x),
            send_sem=self.send.at[way],
            recv_sem=self.recv.at[unit, plane],
            device_id={"sp": target * self.width + self.x},
            device_id_type=MESH,
        )

    def start(self, condition, unit, plane, way, target):
        @pl.when(condition)
        def _():
            self.copy(unit, plane, way, target).start()

    def up(self, condition, unit, plane):
        self.start(condition & (self.z < self.depth - 1), unit, plane, 0, self.z + 1)

    def down(self, condition, unit, plane):
        self.start(condition & (self.z > 0), unit, plane, 1, self.z - 1)

    def arrive(self, condition, unit, plane):
        @pl.when(condition)
        def _():
            self.copy(unit, plane, 0, plane).wait_recv()

    def step(self, t, unit, condition=True, then=None):
        below = (self.z - t >= 0) & condition
        above = (self.z + t < self.depth) & condition
        self.arrive(below, unit, self.z - t)
        self.up(below, unit, self.z - t)
        if then is not None:
            then(below, unit, self.z - t)
        self.arrive(above, unit, self.z + t)
        self.down(above, unit, self.z + t)
        if then is not None:
            then(above, unit, self.z + t)

    def drain(self, planes):
        for way in range(2):
            for count in range(1, self.depth):
                z = count - 1 if way == 0 else self.depth - count

                @pl.when(self.z == z)
                def _():
                    pltpu.make_async_remote_copy(
                        src_ref=planes(count),
                        dst_ref=planes(count),
                        send_sem=self.send.at[way],
                        recv_sem=self.recv.at[0, 0],
                        device_id={"sp": self.z * self.width + self.x},
                        device_id_type=MESH,
                    ).wait_send()


def selection(table, first_expert, column, columns, capacity):
    rows = table.shape[1]
    few = rows // 2
    slots = columns * 2 * capacity
    slot = lax.broadcasted_iota(jnp.int32, (slots, rows), 0)
    row = lax.broadcasted_iota(jnp.int32, (slots, rows), 1)
    side = (column + slot // (2 * capacity)) % columns
    expert = (first_expert + side).astype(F32)
    same = (slot // capacity) % 2 == row // few
    first = (table[0:1, :] == expert) & same
    second = (table[1:2, :] == expert) & same
    named = jnp.where(first | second, 1.0, 0.0).astype(BF16)
    before = lax.broadcasted_iota(jnp.int32, (rows, rows), 0)
    after = lax.broadcasted_iota(jnp.int32, (rows, rows), 1)
    earlier = jnp.where(before < after, 1.0, 0.0).astype(BF16)
    rank = jnp.dot(named, earlier, preferred_element_type=F32)
    here = rank == (slot % capacity).astype(F32)
    choice = jnp.where((first | second) & here, 1.0, 0.0)
    weight = jnp.where(first & here, table[2:3, :], 0.0)
    weight = weight + jnp.where(second & here, table[3:4, :], 0.0)
    weight = weight.T
    high = weight.astype(BF16)
    low = (weight - high.astype(F32)).astype(BF16)
    return choice.astype(BF16), high, low


def attention_part(
    n,
    dp,
    start_loads,
    q_ref,
    k_ref,
    v_ref,
    qg_ref,
    kg_ref,
    w_ref,
    res_ref,
    ng_ref,
    mixed_ref,
    normed_ref,
    experts,
    q_in,
    k_in,
    v_in,
    wide,
    stage,
    q_stage,
    q_all,
    kv,
    w_full,
    swap,
    att,
    total,
    proj,
    back,
    res_in,
    gains,
    norm_in,
    in_sem,
    kvx_send,
    kvx_recv,
    kvz_send,
    kvz_recv,
    qx_send,
    qx_recv,
    wx_send,
    wx_recv,
    wo_sem,
    wz_send,
    wz_recv,
    ax_send,
    ax_recv,
    y_send,
    y_recv,
    pair_sem,
    fwd_sem,
    back_send,
    back_recv,
):
    me = lax.axis_index("sp")
    mine = lax.axis_index("dp")
    rows, heads, width = q_ref.shape
    kv_heads = k_ref.shape[1]
    group = heads // kv_heads
    model = heads * width
    across = stage.shape[0]
    depth = n // across
    local_kv = kv_heads // across
    local = heads // across
    z, x = me // across, me % across
    always = me >= 0
    ny = dp // 2
    core = mine % 2
    row_y = mine // 2
    partner = row_y * 2 + 1 - core
    w_rows, w_cols = w_ref.shape

    def span(start, size):
        return pl.ds(pl.multiple_of(start * size, size), size)

    fetches = [
        pltpu.make_async_copy(src, dst, in_sem.at[i])
        for i, (src, dst) in enumerate(
            (
                (k_ref, k_in),
                (v_ref, v_in),
                (kg_ref, gains.at[0]),
                (q_ref, q_in),
                (qg_ref, gains.at[1]),
                (w_ref, w_full.at[span(me, w_rows)]),
                (res_ref, res_in),
                (ng_ref, norm_in),
            )
        )
    ]
    for fetch in fetches:
        fetch.start()
    barrier = pltpu.get_barrier_semaphore()
    for d in range(1, n):
        pl.semaphore_signal(
            barrier, inc=1, device_id={"sp": lax.rem(me + d, n)}, device_id_type=MESH
        )
    for d in range(1, dp):
        pl.semaphore_signal(
            barrier, inc=1, device_id={"dp": lax.rem(mine + d, dp)}, device_id_type=MESH
        )

    cosine, sine = rotation_tables(me * rows, rows, width)
    my_rows = span(me, rows)
    for fetch in fetches[:3]:
        fetch.wait()
    for part, source in ((0, k_in), (1, v_in)):
        wide[:, 0:kv_heads, :] = source[...].astype(F32)
        for g in range(kv_heads):
            lines = wide[:, g, :]
            slot = 2 * (g % local_kv) + part
            if part == 0:
                lines = turn(lines, gains[0], cosine, sine)
            stage[g // local_kv, slot] = lines.astype(BF16)
    for c in range(2 * local_kv):
        kv[c, my_rows, :] = stage[x, c]
    pl.semaphore_wait(barrier, n - 1 + dp - 1)

    def remote(src, dst, send, recv, **device):
        return pltpu.make_async_remote_copy(
            src_ref=src,
            dst_ref=dst,
            send_sem=send,
            recv_sem=recv,
            device_id=device,
            device_id_type=MESH,
        )

    def beside(k):
        return z * across + lax.rem(x + k, across)

    def kv_block(g, sp):
        return kv.at[pl.ds(2 * g, 2), span(sp, rows), :]

    kv_units = [(k, g) for g in range(local_kv) for k in range(across)]
    own_units = [u for u, (k, _) in enumerate(kv_units) if k == 0]

    def kv_unit(u, sp):
        k, g = kv_units[u]
        return kv_block(g, sp - sp % across + lax.rem(sp % across + k, across))

    halves = 2
    w_units = [(j, k) for j in range(halves) for k in range(2)]
    part_rows, part_cols = w_rows // 2, w_cols // halves

    def w_unit(u, sp):
        j, k = w_units[u]
        start = pl.multiple_of(sp * w_rows + k * part_rows, part_rows)
        return w_full.at[pl.ds(start, part_rows), pl.ds(j * part_cols, part_cols)]

    kv_line = Line(depth, across, kv_unit, kvz_send, kvz_recv)
    w_line = Line(depth, across, w_unit, wz_send, wz_recv)
    kvx, qx, ax = {}, {}, {}
    for g in range(local_kv):
        for k in range(1, across):
            kvx[k, g] = remote(
                stage.at[lax.rem(x + k, across), pl.ds(2 * g, 2)],
                kv_block(g, me),
                kvx_send.at[0],
                kvx_recv.at[across - k - 1, g],
                sp=beside(k),
            )
            kvx[k, g].start()
        kv_line.up(always, own_units[g], z)
        kv_line.down(always, own_units[g], z)

    start_loads()
    fetches[3].wait()
    fetches[4].wait()
    for h in range(0, heads, 8):
        wide[:, h : h + 8, :] = q_in[:, h : h + 8, :].astype(F32)
    for k in list(range(1, across)) + [0]:
        first = lax.rem(x + k, across) * local

        def turn_head(i, carry):
            lines = turn(wide[:, pl.ds(first + i, 1), :].reshape(rows, width), gains[1], cosine, sine)
            if k == 0:
                q_all[i, 0:rows] = lines
            else:
                q_stage[k - 1, i] = lines
            return carry

        lax.fori_loop(0, local, turn_head, 0)
        if k > 0:
            qx[k] = remote(
                q_stage.at[k - 1],
                q_all.at[:, pl.ds((across - k) * rows, rows), :],
                qx_send.at[0],
                qx_recv.at[0],
                sp=beside(k),
            )
            qx[k].start()
        if k == across - 1:
            for u, (kk, g) in enumerate(kv_units):
                if kk == 0:
                    continue
                remote(
                    stage.at[0, pl.ds(2 * g, 2)],
                    kv_block(g, beside(kk)),
                    kvx_send.at[0],
                    kvx_recv.at[kk - 1, g],
                    sp=me,
                ).wait_recv()
                kv_line.up(always, u, z)
                kv_line.down(always, u, z)
    fetches[5].wait()

    far = depth - 1 - z

    def is_far(plane):
        return jnp.where(plane == far, 1, 0)

    def w_across(condition, u, plane):
        for k in range(1, across):

            @pl.when(condition)
            def _():
                remote(
                    w_unit(u, plane * across + x),
                    w_unit(u, plane * across + x),
                    wx_send.at[w_units[u][0]],
                    wx_recv.at[w_units[u][0], is_far(plane)] if plane is not z else wo_sem.at[0],
                    sp=beside(k),
                ).start()

    upper = z // (depth // 2)
    way = 1 - 2 * upper

    def block_of(i, step):
        row = lax.rem(row_y + ny + step * (i // 2), ny)
        return row * 2 + (core if i % 2 == 0 else 1 - core)

    middle = (z > 0) & (z < depth - 1)
    edge = jnp.logical_not(middle)

    def w_half(sp, j):
        return w_full.at[span(sp, w_rows), pl.ds(j * part_cols, part_cols)]

    def w_along():
        block = w_full.at[pl.ds(0, (across - 1) * w_rows)]
        remote(block, block, wo_sem.at[1], wo_sem.at[0], sp=me).wait_recv()
        for j in range(halves):
            for k in range(1, across):
                block = w_half(beside(k), j)
                target = me + way * across
                inner = jnp.where(middle, 1, 0)
                remote(block, block, wo_sem.at[1], wx_recv.at[j, inner], sp=target).start()

    def w_back():
        @pl.when(middle)
        def _():
            for k in range(1, across):
                block = w_half(beside(k), 0)
                target = me - way * across
                remote(block, block, wo_sem.at[2], wx_recv.at[0, 0], sp=target).start()

    def w_aside(units):
        def then(condition, u, plane):
            if w_units[u][0] in units:
                w_across(condition, u, plane)

        return then

    def w_begin(t):
        for u in range(len(w_units)):
            w_line.up(z == t, u, z)
            w_line.down(depth - 1 - z == t, u, z)

    w_begin(0)
    experts.prepare(0)
    for u in range(len(w_units)):
        w_across(always, u, z)
    for t in range(1, depth - 1):
        for u in range(len(kv_units)):
            kv_line.step(t, u)
        w_begin(t)
    experts.prepare(1)
    remote(
        q_stage,
        q_all.at[:, pl.ds(rows, (across - 1) * rows), :],
        qx_send.at[0],
        qx_recv.at[0],
        sp=me,
    ).wait_recv()

    scale = width ** (-0.5)
    wide_group = group * width

    def att_cols(k, g):
        side = lax.rem(x + k, across)
        start = (side * local_kv + g) * wide_group
        return pl.ds(pl.multiple_of(start, wide_group), wide_group)

    def spread_att(u):
        k, g = kv_units[u]
        block = att.at[mine, :, att_cols(k, g)]
        for j in range(1, ny):
            target = lax.rem(row_y + j, ny) * 2 + core
            remote(block, block, y_send.at[0], y_recv.at[j - 1, u], dp=target).start()
        remote(block, block, pair_sem.at[0], pair_sem.at[1], dp=partner).start()

    def forward(u):
        for j in range(1, ny):
            source = lax.rem(row_y + ny - j, ny) * 2 + core
            remote(
                att.at[mine, :, att_cols(*kv_units[u])],
                att.at[mine, :, att_cols(*kv_units[u])],
                y_send.at[0],
                y_recv.at[j - 1, u],
                dp=mine,
            ).wait_recv()
            block = att.at[source, :, att_cols(*kv_units[u])]
            remote(block, block, fwd_sem.at[0], fwd_sem.at[1], dp=partner).start()

    for g in range(local_kv):
        for u, (_, gg) in enumerate(kv_units):
            if gg == g:
                kv_line.step(depth - 1, u)
        if g == local_kv - 1:
            for u in range(len(w_units)):
                w_line.step(1, u, middle)
            w_along()

        def one_head(i, carry):
            h = g * group + i
            scores = (
                lax.dot_general(
                    q_all[h], kv[2 * g], (((1,), (1,)), ((), ())), preferred_element_type=F32
                )
                * scale
            )
            exponent = jnp.exp(scores - jnp.max(scores, axis=-1, keepdims=True))
            weights = (exponent / jnp.sum(exponent, axis=-1, keepdims=True)).astype(BF16)
            out = jnp.dot(weights, kv[2 * g + 1], preferred_element_type=F32).astype(BF16)
            cols = pl.ds(pl.multiple_of((x * local + h) * width, width), width)
            att[mine, :, cols] = out[0:rows]
            cols = pl.ds(pl.multiple_of(h * width, width), width)
            for k in range(1, across):
                swap[k - 1, :, cols] = out[k * rows : (k + 1) * rows]
            return carry

        lax.fori_loop(0, group, one_head, 0)
        for k in range(1, across):
            ax[k, g] = remote(
                swap.at[k - 1, :, pl.ds(g * wide_group, wide_group)],
                att.at[mine, :, att_cols(0, g)],
                ax_send.at[0],
                ax_recv.at[across - k - 1, g],
                sp=beside(k),
            )
            ax[k, g].start()
        spread_att(own_units[g])
    for t in range(2, depth - 1):
        for u in range(len(w_units)):
            w_line.step(t, u, middle, w_across)
    w_back()
    for u in range(len(w_units)):
        w_line.step(1, u, edge, w_aside((1,)))
    for u, (k, g) in enumerate(kv_units):
        if k == 0:
            continue
        remote(
            swap.at[0, :, pl.ds(g * wide_group, wide_group)],
            att.at[mine, :, att_cols(k, g)],
            ax_send.at[0],
            ax_recv.at[k - 1, g],
            sp=me,
        ).wait_recv()
        spread_att(u)
    for t in range(2, depth - 1):
        for u in range(len(w_units)):
            w_line.step(t, u, edge, w_across)
    order = own_units + [u for u in range(len(kv_units)) if u not in own_units]
    for i in range(max(len(order), len(w_units))):
        if i < len(w_units):
            w_line.step(depth - 1, i, True, w_across)
        if i < len(order):
            forward(order[i])
    if ny > 1:
        remote(
            att.at[pl.ds(0, ny - 1)],
            att.at[pl.ds(0, ny - 1)],
            fwd_sem.at[0],
            fwd_sem.at[1],
            dp=mine,
        ).wait_recv()
    remote(att.at[mine], att.at[mine], pair_sem.at[0], pair_sem.at[1], dp=mine).wait_recv()

    deep = across * w_rows

    def project(place, cols):
        lines = pl.ds(pl.multiple_of(place * deep, deep), deep)
        return jnp.dot(
            att[:, :, lines].reshape(dp * rows, deep),
            w_full[lines, cols],
            preferred_element_type=F32,
        )

    def w_wait(j, planes, which):
        block = w_full.at[
            pl.ds(0, planes * (across - 1) * w_rows), pl.ds(j * part_cols, part_cols)
        ]
        remote(block, block, wx_send.at[0], wx_recv.at[j, which], sp=me).wait_recv()

    for j in range(halves):
        cols = slice(j * part_cols, (j + 1) * part_cols)
        w_wait(j, depth - 2, 0)
        total[:, cols] = project(lax.rem(far + 1, depth), cols)
        for step in range(2, depth):
            total[:, cols] += project(lax.rem(far + step, depth), cols)
    for j in range(halves):
        cols = slice(j * part_cols, (j + 1) * part_cols)
        w_wait(j, 1, 1)
        result = (total[:, cols] + project(far, cols)).astype(BF16)
        for s in range(dp):
            proj[s, :, cols] = result[s * rows : (s + 1) * rows]
        back[mine, :, cols] = proj[mine, :, cols]
        for i in list(range(2, dp)) + [1]:
            target = block_of(i, 1)
            remote(
                proj.at[target, :, cols],
                back.at[mine, :, cols],
                back_send.at[0],
                back_recv.at[i],
                dp=target,
            ).start()

    fetches[6].wait()
    fetches[7].wait()
    square = jnp.zeros((rows, 1), F32)
    each = dp // CHUNKS
    for i in range(dp):
        source = block_of(i, -1)
        if i > 0:
            remote(back.at[mine], back.at[source], back_send.at[0], back_recv.at[i], dp=mine).wait_recv()
        cols = span(source, w_cols)
        part = res_in[:, cols].astype(F32) + back[source].astype(F32)
        mixed_ref[:, cols] = part
        square = square + jnp.sum(part * part, axis=-1, keepdims=True)
        normed_ref[:, i * w_cols : (i + 1) * w_cols] = part.astype(BF16)
        if i == dp - 1:
            factor = lax.rsqrt(square / model + EPS)
            high = factor.astype(BF16).astype(F32)
            mid = (factor - high).astype(BF16).astype(F32)
            lane = lax.broadcasted_iota(jnp.int32, (rows, width), 1)
            pieces = jnp.where(lane == 0, high, jnp.where(lane == 1, mid, 0.0))
            pieces = jnp.where(lane == 2, factor - high - mid, pieces)
            normed_ref[:, model : model + width] = pieces.astype(BF16)
        if i % each == each - 1:
            experts.launch(i // each)
        if i == dp // 2 - 1:
            experts.early()

    def drain():
        kv_line.drain(lambda count: kv.at[:, pl.ds(0, count * across * rows), :])
        w_line.drain(lambda count: w_full.at[pl.ds(0, count * w_rows)])
        for role, counts in ((edge, (depth - 1, depth)), (middle, (2, 2))):

            @pl.when(role)
            def _():
                for j, count in enumerate(counts):
                    block = w_full.at[
                        pl.ds(0, count * (across - 1) * w_rows), pl.ds(0, part_cols)
                    ]
                    remote(block, block, wx_send.at[j], back_recv.at[0], sp=me).wait_send()

        @pl.when(middle)
        def _():
            block = w_full.at[pl.ds(0, (across - 1) * w_rows), pl.ds(0, part_cols)]
            remote(block, block, wo_sem.at[2], back_recv.at[0], sp=me).wait_send()

        whole = [
            (w_full.at[pl.ds(0, (across - 1) * w_rows)], wo_sem.at[1]),
            (stage.at[pl.ds(0, across - 1)], kvx_send.at[0]),
            (q_stage, qx_send.at[0]),
            (swap, ax_send.at[0]),
            (att.at[mine], pair_sem.at[0]),
            (proj.at[pl.ds(0, dp - 1)], back_send.at[0]),
        ]
        if ny > 1:
            whole.append((att.at[pl.ds(0, ny - 1)], y_send.at[0]))
            whole.append((att.at[pl.ds(0, ny - 1)], fwd_sem.at[0]))
        for block, sem in whole:
            remote(block, block, sem, back_recv.at[0], sp=me).wait_send()

    return drain


class Experts:
    def __init__(self, n, dp, capacity, norm, routes, gates, middle, loads, out, *refs):
        (
            self.gate,
            self.up,
            self.down,
            self.tables,
            self.pick,
            self.high,
            self.low,
            self.column,
            self.asked,
            self.served,
            self.answer,
            self.given,
            self.ready,
            self.hidden,
            self.partial,
            self.incoming,
            self.hold,
            self.table_sem,
            self.column_send,
            self.column_recv,
            self.ask_send,
            self.ask_recv,
            self.give_send,
            self.give_recv,
            self.part_send,
            self.part_recv,
        ) = refs
        self.mixed, self.normed = middle
        self.routes, self.gates = routes, gates
        self.loads, self.out = loads, out
        me = lax.axis_index("sp")
        self.columns = max(x for x in range(1, n + 1) if n % x == 0 and x * x <= n)
        self.depth = n // self.columns
        self.z, self.x = me // self.columns, me % self.columns
        self.upper = self.z // (self.depth // 2)
        self.way = 1 - 2 * self.upper
        self.inner = self.upper * (self.depth - 1) + self.way * self.z
        self.capacity = capacity
        self.norm, self.dp = norm, dp
        self.rows, self.model = self.mixed.shape
        self.width = self.model // CHUNKS
        self.share = 2 * capacity

    def role(self, inner):
        return self.inner == inner

    def plane(self, r):
        place = (self.inner, 1 - self.inner, self.depth - 1, self.depth - 2)[r]
        return self.upper * (self.depth - 1) + self.way * place

    def remote(self, src, dst, send, recv, target):
        return pltpu.make_async_remote_copy(
            src_ref=src,
            dst_ref=dst,
            send_sem=send,
            recv_sem=recv,
            device_id={"sp": target},
            device_id_type=MESH,
        )

    def at(self, step):
        return (self.z + step) * self.columns + self.x

    def beside(self, k):
        return self.z * self.columns + (self.x + k) % self.columns

    def lanes(self, c):
        end = (c + 1) * self.width if c < CHUNKS - 1 else self.normed.shape[1]
        return slice(c * self.width, end)

    def early(self):
        @pl.when(self.role(0))
        def _():
            for c in range(CHUNKS // 2):
                self.ask(0, 1, c)

    def launch(self, c):
        self.column_copy("forth", c).start()

        @pl.when(self.role(1))
        def _():
            self.column_copy("back", c).start()

    def cols(self, c):
        return slice(c * self.width, (c + 1) * self.width)

    def tables_all(self):
        block = self.tables.at[pl.ds(0, self.depth - 1)]
        return self.remote(block, block, self.table_sem.at[0], self.table_sem.at[1], self.at(0))

    def prepare(self, phase):
        planes = self.depth

        def table_copy(d):
            target = (self.z + d) % planes
            return self.remote(
                self.tables.at[self.z],
                self.tables.at[self.z],
                self.table_sem.at[0],
                self.table_sem.at[1],
                target * self.columns + self.x,
            )

        if phase == 0:
            rows = self.rows
            self.tables[self.z] = jnp.concatenate(
                [self.routes[...].astype(F32), self.gates[...], jnp.zeros((4, rows), F32)], axis=0
            )
            for d in range(1, planes):
                table_copy(d).start()
            return
        self.tables_all().wait_recv()
        for r in range(planes):
            choice, high, low = selection(
                self.tables[self.plane(r)],
                self.z * self.columns,
                self.x,
                self.columns,
                self.capacity,
            )
            self.pick[r] = choice
            self.high[r] = high
            self.low[r] = low

    def column_copy(self, kind, c):
        source, place, step = {
            "forth": (None, None, 1),
            "back": (None, 1, -1),
            1: (1, 2, 1),
            2: (2, 2, -1),
            3: (3, 3, -1),
        }[kind]
        cols = self.lanes(c)
        src = self.normed.at[:, cols] if source is None else self.column.at[source - 1, :, cols]
        if place is None:
            place = 1 + 2 * self.inner
        index = {"forth": 0, "back": 1}.get(kind, 2)
        return self.remote(
            src,
            self.column.at[place - 1, :, cols],
            self.column_send.at[index],
            self.column_recv.at[place - 1, c],
            self.at(step * self.way),
        )

    def column_arrive(self, r, c):
        cols = self.lanes(c)
        self.remote(
            self.column.at[r - 1, :, cols],
            self.column.at[r - 1, :, cols],
            self.column_send.at[0],
            self.column_recv.at[r - 1, c],
            self.at(0),
        ).wait_recv()

    def ask_copy(self, r, c, k):
        cols = self.lanes(c)
        return self.remote(
            self.asked.at[r, pl.ds((k - 1) * self.share, self.share), cols],
            self.served.at[r, pl.ds((self.columns - k) * self.share, self.share), cols],
            self.ask_send.at[0],
            self.ask_recv.at[r],
            self.beside(k),
        )

    def give_copy(self, r, c, k):
        cols = self.cols(c)
        return self.remote(
            self.given.at[r, pl.ds((k - 1) * self.share, self.share), cols],
            self.answer.at[r, pl.ds((self.columns - k) * self.share, self.share), cols],
            self.give_send.at[0],
            self.give_recv.at[r, c],
            self.beside(k),
        )

    def ask(self, inner, r, c):
        cols = self.lanes(c)
        if r > 0:
            self.column_arrive(r, c)
            if inner == 1:
                self.column_copy(r, c).start()
        lines = self.normed[:, cols] if r == 0 else self.column[r - 1, :, cols]
        chosen = jnp.dot(self.pick[r], lines, preferred_element_type=F32).astype(BF16)
        self.served[r, 0 : self.share, cols] = chosen[0 : self.share]
        for k in range(1, self.columns):
            part = slice((k - 1) * self.share, k * self.share)
            self.asked[r, part, cols] = chosen[k * self.share : (k + 1) * self.share]
            self.ask_copy(r, c, k).start()

    def serve_up(self, r, first=False):
        block = self.asked.at[r]
        self.remote(
            block, block, self.ask_send.at[0], self.ask_recv.at[r], self.at(0)
        ).wait_recv()
        if first:
            self.loads[0].wait()
            self.loads[1].wait()

        pieces = self.served[r, :, self.model :].astype(F32)
        factor = jnp.sum(pieces, axis=-1, keepdims=True)
        mine = lax.axis_index("dp")
        size = self.model // self.dp
        for i in range(self.dp):
            row = (mine // 2 + self.dp // 2 - i // 2) % (self.dp // 2)
            block = row * 2 + (mine % 2 if i % 2 == 0 else 1 - mine % 2)
            cols = pl.ds(pl.multiple_of(block * size, size), size)
            lines = self.served[r, :, i * size : (i + 1) * size].astype(F32)
            self.ready[:, cols] = (lines * factor * self.norm[:, cols]).astype(BF16)

        def up_tile(t, carry):
            cols = pl.ds(pl.multiple_of(t * TILE, TILE), TILE)
            lines = self.ready[...]
            gate = jnp.dot(lines, self.gate[:, cols], preferred_element_type=F32)
            up = jnp.dot(lines, self.up[:, cols], preferred_element_type=F32)
            self.hidden[min(r, 1), :, cols] = (gate / (1.0 + jnp.exp(-gate)) * up).astype(BF16)
            return carry

        lax.fori_loop(0, self.gate.shape[1] // TILE, up_tile, 0)

    def serve_down(self, r, c, first=False):
        if first:
            self.loads[2].wait()

        def down_tile(t, carry):
            cols = pl.ds(pl.multiple_of(c * self.width + t * TILE, TILE), TILE)
            lines = jnp.dot(
                self.hidden[min(r, 1)], self.down[:, cols], preferred_element_type=F32
            ).astype(BF16)
            self.answer[r, 0 : self.share, cols] = lines[0 : self.share]
            self.given[r, :, cols] = lines[self.share :]
            return carry

        lax.fori_loop(0, self.width // TILE, down_tile, 0)
        for k in range(1, self.columns):
            self.give_copy(r, c, k).start()

    def combine(self, r, c):
        block = self.given.at[r, :, self.cols(c)]
        self.remote(
            block, block, self.give_send.at[0], self.give_recv.at[r, c], self.at(0)
        ).wait_recv()
        lines = self.answer[r, :, self.cols(c)]
        return jnp.dot(self.high[r], lines, preferred_element_type=F32) + jnp.dot(
            self.low[r], lines, preferred_element_type=F32
        )

    def part_copy(self, slot, place, step, c):
        cols = self.cols(c)
        return self.remote(
            self.partial.at[slot, :, cols],
            self.incoming.at[place, :, cols],
            self.part_send.at[0],
            self.part_recv.at[place, c],
            self.at(step * self.way),
        )

    def part_arrive(self, place, c):
        cols = self.cols(c)
        self.remote(
            self.partial.at[0, :, cols],
            self.incoming.at[place, :, cols],
            self.part_send.at[0],
            self.part_recv.at[place, c],
            self.at(0),
        ).wait_recv()
        return self.incoming[place, :, cols].astype(F32)

    def merge(self, r, c, slot, place, step, feed=None):
        total = self.combine(r, c)
        if feed is not None:
            total = total + self.part_arrive(feed, c)
        self.partial[slot, :, self.cols(c)] = total.astype(BF16)
        self.part_copy(slot, place, step, c).start()

    def own(self, c):
        cols = self.cols(c)
        self.hold[:, cols] = self.mixed[:, cols] + self.combine(0, c)

    def finish(self, c, places):
        cols = self.cols(c)
        total = self.hold[:, cols]
        for place in places:
            total = total + self.part_arrive(place, c)
        self.out[:, cols] = total.astype(BF16)

    def edge(self):
        chunks = range(CHUNKS)
        ask = functools.partial(self.ask, 0)

        def toward(r, c):
            self.merge(r, c, r - 1, r - 1, 1)

        def down(r, *cs):
            for c in cs:
                self.serve_down(r, c, r == 1 and c == 0)

        for c in range(CHUNKS // 2, CHUNKS):
            ask(1, c)
        for c in chunks:
            ask(0, c)
        self.serve_up(1, True)
        down(1, *chunks)
        ask(2, 0)
        toward(1, 0)
        ask(2, 1)
        toward(1, 1)
        toward(1, 2)
        ask(2, 2)
        toward(1, 3)
        ask(2, 3)
        ask(3, 0)
        ask(3, 1)
        ask(3, 2)
        self.serve_up(2)
        down(2, *chunks)
        ask(3, 3)
        for c in chunks:
            toward(2, c)
        self.serve_up(3)
        down(3, *chunks)
        for c in chunks:
            toward(3, c)
        self.serve_up(0)
        down(0, *chunks)
        for c in chunks:
            self.own(c)
        for c in chunks:
            self.finish(c, (5,))

    def inside(self):
        chunks = range(CHUNKS)
        ask = functools.partial(self.ask, 1)

        def down(r, *cs):
            for c in cs:
                self.serve_down(r, c, r == 1 and c == 0)

        for c in chunks:
            ask(0, c)
        ask(3, 0)
        ask(3, 1)
        ask(1, 0)
        ask(1, 1)
        ask(2, 0)
        ask(1, 2)
        ask(2, 1)
        ask(1, 3)
        ask(2, 2)
        ask(2, 3)
        ask(3, 2)
        ask(3, 3)
        for r in (1, 2, 3):
            self.serve_up(r, r == 1)
            down(r, *chunks)
        self.serve_up(0)

        def far(c):
            self.merge(2, c, 1, 3, 1, 1)

        def near(c):
            self.merge(1, c, 3, 5, -1, 3)

        for c in chunks:
            far(c)
        down(0, *chunks)
        for c in chunks:
            near(c)
        for c in chunks:
            self.own(c)
        for c in chunks:
            self.merge(3, c, 2, 4, 1, 2)
        for c in chunks:
            self.finish(c, (0, 4))

    def run(self):
        pl.when(self.role(0))(self.edge)
        pl.when(self.role(1))(self.inside)
        ends = [
            (self.normed, self.column_send.at[0]),
            (self.asked, self.ask_send.at[0]),
            (self.given, self.give_send.at[0]),
            (self.partial.at[pl.ds(0, 3)], self.part_send.at[0]),
        ]
        for block, sem in ends:
            self.remote(block, block, sem, self.part_recv.at[0, 0], self.at(0)).wait_send()

        @pl.when(self.role(1))
        def _():
            for block, way in ((self.normed, 1), (self.column, 2)):
                self.remote(
                    block, block, self.column_send.at[way], self.part_recv.at[0, 0], self.at(0)
                ).wait_send()

        self.tables_all().wait_send()


def layer_kernel(n, dp, capacity, *refs):
    inputs, refs = refs[:10], refs[10:]
    weights, out_ref, refs = refs[:3], refs[3], refs[4:]
    middle, refs = refs[:2], refs[2:]
    attention, refs = refs[:37], refs[37:]
    load_sem, stores = refs[0], refs[1:4]
    loads = [
        pltpu.make_async_copy(src.at[0], dst, load_sem.at[i])
        for i, (src, dst) in enumerate(zip(weights, stores))
    ]

    def start_loads():
        for load in loads:
            load.start()

    norm = attention[16]
    experts = Experts(n, dp, capacity, norm, *inputs[8:], middle, loads, out_ref, *refs[1:])
    drain = attention_part(n, dp, start_loads, *inputs[:8], *middle, experts, *attention)
    experts.run()
    drain()


def on_device(
    n,
    dp,
    queries,
    key_rows,
    values,
    query_gain,
    key_gain,
    out_weight,
    residual,
    norm_gain,
    expert_gate,
    expert_up,
    expert_down,
    routes,
    route_weight,
):
    _, rows, heads, width = queries.shape
    kv_heads = key_rows.shape[2]
    model = heads * width
    length = rows * n
    experts = expert_gate.shape[0] * n
    capacity = max(2, 4 * (rows // 2) // experts)
    across = max(x for x in range(1, n + 1) if n % x == 0 and x * x <= n)
    depth = n // across
    local_kv, local = kv_heads // across, heads // across
    units = across * local_kv
    slots = 2 * across * capacity
    aside = 2 * (across - 1) * capacity
    w_rows, w_cols = out_weight.shape
    dma = pltpu.SemaphoreType.DMA
    ny = dp // 2
    ff = expert_gate.shape[2]
    attention_scratch = [
        pltpu.VMEM((rows, heads, width), BF16),
        pltpu.VMEM((rows, kv_heads, width), BF16),
        pltpu.VMEM((rows, kv_heads, width), BF16),
        pltpu.VMEM((rows, heads, width), F32),
        pltpu.VMEM((across, 2 * local_kv, rows, width), BF16),
        pltpu.VMEM((across - 1, local, rows, width), BF16),
        pltpu.VMEM((local, across * rows, width), BF16),
        pltpu.VMEM((2 * local_kv, length, width), BF16),
        pltpu.VMEM((w_rows * n, w_cols), BF16),
        pltpu.VMEM((across - 1, rows, local * width), BF16),
        pltpu.VMEM((dp, rows, model), BF16),
        pltpu.VMEM((dp * rows, w_cols), F32),
        pltpu.VMEM((dp, rows, w_cols), BF16),
        pltpu.VMEM((dp, rows, w_cols), BF16),
        pltpu.VMEM((rows, model), BF16),
        pltpu.VMEM((2, 1, width), F32),
        pltpu.VMEM((1, model), F32),
        dma((8,)),
        dma((1,)),
        dma((across - 1, local_kv)),
        dma((2,)),
        dma((units, depth)),
        dma((1,)),
        dma((1,)),
        dma((2,)),
        dma((2, 2)),
        dma((3,)),
        dma((2,)),
        dma((4, depth)),
        dma((1,)),
        dma((across - 1, local_kv)),
        dma((1,)),
        dma((max(1, ny - 1), units)),
        dma((2,)),
        dma((2,)),
        dma((1,)),
        dma((dp,)),
    ]
    result = pl.pallas_call(
        functools.partial(layer_kernel, n, dp, capacity),
        out_shape=pltpu.VMEM((rows, model), BF16),
        in_specs=[ANY] * 8 + [VMEM] * 2 + [ANY] * 3,
        out_specs=VMEM,
        scratch_shapes=[
            pltpu.VMEM((rows, model), F32),
            pltpu.VMEM((rows, model + width), BF16),
            *attention_scratch,
            dma((3,)),
            pltpu.VMEM((model, ff), BF16),
            pltpu.VMEM((model, ff), BF16),
            pltpu.VMEM((ff, model), BF16),
            pltpu.VMEM((depth, 8, rows), F32),
            pltpu.VMEM((depth, slots, rows), BF16),
            pltpu.VMEM((depth, rows, slots), BF16),
            pltpu.VMEM((depth, rows, slots), BF16),
            pltpu.VMEM((depth - 1, rows, model + width), BF16),
            pltpu.VMEM((depth, aside, model + width), BF16),
            pltpu.VMEM((depth, slots, model + width), BF16),
            pltpu.VMEM((depth, slots, model), BF16),
            pltpu.VMEM((depth, aside, model), BF16),
            pltpu.VMEM((slots, model), BF16),
            pltpu.VMEM((2, slots, ff), BF16),
            pltpu.VMEM((4, rows, model), BF16),
            pltpu.VMEM((6, rows, model), BF16),
            pltpu.VMEM((rows, model), F32),
            dma((2,)),
            dma((3,)),
            dma((depth - 1, CHUNKS)),
            dma((1,)),
            dma((depth,)),
            dma((1,)),
            dma((depth, CHUNKS)),
            dma((1,)),
            dma((6, CHUNKS)),
        ],
        compiler_params=pltpu.CompilerParams(
            collective_id=0, has_side_effects=True, vmem_limit_bytes=56 * 1024 * 1024
        ),
        name="layer",
    )(
        queries[0],
        key_rows[0],
        values[0],
        query_gain[None],
        key_gain[None],
        out_weight,
        residual[0],
        norm_gain[None],
        routes[0].T,
        route_weight[0].T,
        expert_gate,
        expert_up,
        expert_down,
    )
    return result[None]


def solution(mesh):
    in_specs = (
        P("dp", "sp", None, None),
        P("dp", "sp", None, None),
        P("dp", "sp", None, None),
        P(),
        P(),
        P("sp", "dp"),
        P("dp", "sp", None),
        P(),
        P("sp", None, None),
        P("sp", None, None),
        P("sp", None, None),
        P("dp", "sp", None),
        P("dp", "sp", None),
    )
    out_specs = P("dp", "sp", None)
    return jax.shard_map(
        functools.partial(on_device, mesh.shape["sp"], mesh.shape["dp"]),
        mesh=mesh,
        in_specs=in_specs,
        out_specs=out_specs,
        check_vma=False,
    )
```
